32 devices in a mesh: sp: 8 (over z, x), tp: 4 (over y, core).
Axes of the slice: x: 2, y: 2, z: 4, core: 2. Of those that a mesh axis runs over, the one named last changes fastest.
Arguments:
- stream_in: bfloat16 [1024, 2048], P('sp'), may hold values from -8 to 8
- out_cot: bfloat16 [1024, 2048], P('sp'), may hold values from -6 to 6
- route_experts: int32 [1024, 2], P('sp'), may hold values from 0 to 7, all different within a row; in each aligned block of 128 rows (0 to 127, 128 to 255, ...) at most 64 rows name the same one
- route_weights: float32 [1024, 2], P('sp'), may hold values from 0.1 to 1
- w_gate: bfloat16 [8, 2048, 2048], P('sp', None, 'tp'), may hold values from -0.125 to 0.125
- w_up: bfloat16 [8, 2048, 2048], P('sp', None, 'tp'), may hold values from -0.125 to 0.125
- w_down: bfloat16 [8, 2048, 2048], P('sp', 'tp'), may hold values from -0.125 to 0.125
- w_proj: bfloat16 [2048, 1024], P(None, 'tp'), may hold values from -0.1875 to 0.1875
- conv_value: bfloat16 [1024, 1024], P('tp', 'sp'), may hold values from -6 to 6
- conv_gate: bfloat16 [1024, 1024], P('tp', 'sp'), may hold values from -8 to 8
- conv_taps: float32 [31, 1024], P(None, 'tp'), may hold values from -1 to 1
- conv_result: bfloat16 [1024, 1024], P('tp', 'sp'), may hold values from -100 to 100
- channel_norm_gain: float32 [1024], P('tp'), may hold values from 0.1 to 1.9
Outputs:
- grad_gate: bfloat16 [8, 2048, 2048], P('sp', None, 'tp')
- grad_up: bfloat16 [8, 2048, 2048], P('sp', None, 'tp')
- grad_down: bfloat16 [8, 2048, 2048], P('sp', 'tp')
- grad_stream: bfloat16 [1024, 2048], P('sp')
- grad_proj: float32 [2048, 1024], P('sp', 'tp')
- grad_value: bfloat16 [1024, 1024], P('tp', 'sp')
- grad_gate_in: bfloat16 [1024, 1024], P('tp', 'sp')
The draws below stay inside these ranges and needn't reach their ends.
Inputs may be any that keep to these rules, and one draw needn't show every extreme that they name: `route_experts`: each row names 2 different experts; within each aligned block of 128 rows no expert is named by more than 64 rows, and at least one block reaches that bound for some expert.
All inputs are finite; a program needn't handle non-finite values.
Results may differ from the reference program's by a relative error of at most 0.025.
Values may be sent and summed in bfloat16 or wider, within the bound.
A program may use at most 64 MiB of HBM per device.

```python
import math
import jax
import jax.numpy as jnp
import numpy as np
from jax import lax

D = 2048
FF = 2048
CONV_CHANNELS = 1024
CONV_W = 31
TOP = 2
T_DEV = 128
EXPERTS = 8
TOKENS = 1024
CAP = 64
N_SP = 8
N_TP = 4


def draw_conv_result(key, part):
    first_key, second_key, third_key = jax.random.split(jax.random.fold_in(key, 17), 3)
    base = jnp.clip(jax.random.normal(first_key, (CONV_CHANNELS, TOKENS), jnp.float32), -6.0, 6.0)
    channel_pos = jnp.arange(CONV_CHANNELS, dtype=jnp.float32) / CONV_CHANNELS
    rough = jax.random.uniform(second_key, (CONV_CHANNELS, 1), jnp.float32, 0.5, 1.5)
    shift_noise = jnp.clip(jax.random.normal(third_key, (1, TOKENS), jnp.float32), -4.0, 4.0)
    scales = jnp.exp(jnp.log(3.0) * channel_pos)[:, None] * rough
    offset = shift_noise
    return (base * scales + offset).astype(jnp.bfloat16)


def spiked(values, rng, source, target, shards_of, factor):
    def block_of(dim):
        return (jnp.arange(values.shape[dim]) // (values.shape[dim] // shards_of)).reshape((-1,) + (1,) * (values.ndim - 1 - dim))

    near = jax.random.permutation(rng, shards_of)[block_of(target)]
    second = (block_of(target) + shards_of // 2) % shards_of
    return jnp.where((block_of(source) == near) | (block_of(source) == second), factor * values, values)


def steps_of(key, extent, cuts, smallest, top_value):
    def one(dim, parts):
        heights = jax.random.uniform(jax.random.fold_in(jax.random.fold_in(key, 6), dim), (parts,), jnp.float32, smallest / len(cuts), top_value / len(cuts))
        return jnp.repeat(jnp.exp(heights), extent[dim] // parts).reshape((-1,) + (1,) * (len(extent) - dim - 1))

    gain = one(*cuts[0])
    for cut in cuts[1:]:
        gain = gain * one(*cut)
    return gain


def deal_out(own_key, own, number, rows, count, top, reach, skew):
    ranking = jax.random.permutation(own_key, count)
    heavy_load, ordinary = load_shares(count, rows * top, reach, skew, True), load_shares(count, rows * top, reach, skew, False)
    places = jnp.arange(count)

    def named(sizes, turn):
        used = int((sizes > 0).sum())
        fixed = max(1, used // 4)
        moved = fixed + (places - fixed + turn * (used - fixed)) % max(1, count - fixed)
        return jnp.zeros((count,), jnp.int32).at[ranking[jnp.where(places < fixed, places, moved)]].set(jnp.asarray(sizes, jnp.int32))

    sizes = jnp.where(number % 4 == 0, named(heavy_load, number // 4), named(ordinary, number - number // 4 - 1))
    mixed = jax.random.permutation(jax.random.fold_in(own, 3), count)
    donor, sink = mixed[0:count // 2 * 2:2], mixed[1:count // 2 * 2:2]
    slack = jnp.minimum(sizes[donor] - 1, reach - sizes[sink]) // 2
    slack = jnp.where((donor == ranking[0]) | (sink == ranking[0]) | (sizes[sink] == 0), 0, jnp.maximum(slack, 0))
    moved = jax.random.randint(jax.random.fold_in(own, 4), (count // 2,), 0, 1 << 20) % (slack + 1)
    sizes = sizes.at[donor].add(-moved).at[sink].add(moved)
    labels = jnp.searchsorted(jnp.cumsum(sizes), jnp.arange(rows * top), side="right").astype(jnp.int32)
    listing = labels.reshape(top, rows).T
    listing = listing[jax.random.permutation(jax.random.fold_in(own, 1), rows)]
    turn = jax.random.randint(jax.random.fold_in(own, 2), (rows, 1), 0, top)
    return jnp.take_along_axis(listing, (jnp.arange(top)[None, :] + turn) % top, axis=1)


def load_shares(amount, total, most, lean, full):
    portions = [(1 << 20) // math.isqrt(grade ** lean) + 1 for grade in range(1, amount + 1)]
    largest = most if full else min(most, max(-(-total // amount), total * portions[0] // sum(portions)))
    least = 1 if total - largest >= amount - 1 else 0
    given, spare = [largest] + [least] * (amount - 1), total - largest - least * (amount - 1)
    while spare > 0:
        candidates = [i for i in range(1, amount) if given[i] < largest] or [i for i in range(1, amount) if given[i] < most]
        mass, budget = sum([portions[i] for i in candidates]), spare
        for i in candidates:
            more = min(most - given[i], max(1, budget * portions[i] // mass), spare)
            given[i] = given[i] + more
            spare = spare - more
    return np.array(given)


def centred(key, extent, width, most, cuts=(), kind=jnp.bfloat16):
    entries = jax.random.normal(key, extent, jnp.float32) * width
    if len(cuts) > 0:
        entries = steps_of(key, extent, cuts, -0.22, 0.18) * entries
    return jnp.clip(entries, min=-most, max=most).astype(kind)


def gaussian_with(rng, shape, deviation, most, cuts, heavy, kind=jnp.bfloat16):
    values = deviation * jax.random.normal(rng, shape, jnp.float32)
    if cuts:
        values = values * steps_of(rng, shape, cuts, -0.22, 0.18)
    return jnp.clip(spiked(values, jax.random.fold_in(rng, 3), *heavy), -most, most).astype(kind)


def setup_inputs(seed: int = 0) -> dict:
    key_list = jax.random.split(jax.random.key(seed), 14)
    stream_in = centred(key_list[0], (TOKENS, D), 1.25, 8.0, ((0, 8),))
    out_cot = gaussian_with(key_list[1], (TOKENS, D), 1.0, 6.0, ((0, 8),), (0, 1, 8, 2.0))
    route_experts_keys = jax.random.split(jax.random.fold_in(key_list[2], 1), TOKENS // T_DEV)
    route_experts_turns = jax.random.permutation(jax.random.fold_in(key_list[2], 3), TOKENS // T_DEV)
    route_experts = jax.vmap(lambda own, number: deal_out(jax.random.fold_in(key_list[2], 2), own, number, T_DEV, EXPERTS, TOP, CAP, 2))(route_experts_keys, route_experts_turns).reshape((TOKENS, TOP))
    route_weights = jnp.clip(0.1 + 0.9 * jax.random.uniform(key_list[3], (TOKENS, TOP), jnp.float32) ** steps_of(key_list[3], (TOKENS, TOP), ((0, 8),), -0.2, 0.2), 0.1, 1.0)
    w_gate = centred(key_list[4], (EXPERTS, D, FF), D ** -0.5, 0.125, ((0, 8), (2, 4)))
    w_up = centred(key_list[5], (EXPERTS, D, FF), D ** -0.5, 0.125, ((0, 8), (2, 4)))
    w_down = centred(key_list[6], (EXPERTS, FF, D), FF ** -0.5, 0.125, ((0, 8), (1, 4)))
    w_proj = centred(key_list[7], (D, CONV_CHANNELS), CONV_CHANNELS ** -0.5, 0.1875, ((1, 4),))
    conv_value = centred(key_list[8], (CONV_CHANNELS, TOKENS), 1.0, 6.0, ((0, 4), (1, 8)))
    conv_gate = centred(key_list[9], (CONV_CHANNELS, TOKENS), 1.5, 8.0, ((0, 4), (1, 8)))
    conv_taps = centred(key_list[10], (CONV_W, CONV_CHANNELS), CONV_W ** -0.5, 1.0, ((1, 4),), jnp.float32)
    conv_result = draw_conv_result(jax.random.fold_in(key_list[13], 71), 0)
    channel_norm_gain = jnp.clip(1.0 + 0.18 * jax.random.normal(key_list[12], (CONV_CHANNELS,), jnp.float32), 0.1, 1.9)
    return dict(stream_in=stream_in, out_cot=out_cot, route_experts=route_experts, route_weights=route_weights, w_gate=w_gate, w_up=w_up, w_down=w_down, w_proj=w_proj, conv_value=conv_value, conv_gate=conv_gate, conv_taps=conv_taps, conv_result=conv_result, channel_norm_gain=channel_norm_gain)


norm_eps = 1e-05
clamp_limit = 7.0
alpha_gate = 1.702

def slot_tables(block_routes, experts_all, capacity):
    flat_routes = block_routes.reshape(-1).astype(jnp.int32)
    assigns = flat_routes.shape[0]
    onehot = (flat_routes[:, None] == jnp.arange(experts_all, dtype=jnp.int32)[None, :]).astype(jnp.int32)
    before = jnp.cumsum(onehot, axis=0) - onehot
    rank_in = lax.optimization_barrier(jnp.sum(before * onehot, axis=1)).astype(jnp.int32)
    slot_of = (flat_routes * capacity + rank_in).astype(jnp.int32)
    source_of = jnp.full((experts_all * capacity,), -1, jnp.int32).at[slot_of].set(jnp.arange(assigns, dtype=jnp.int32))
    return (slot_of, source_of)

def one_expert(operands):
    rows_in, cot_in, gate_mat, up_mat, down_mat = operands
    pre_gate = jnp.dot(rows_in, gate_mat, preferred_element_type=jnp.float32)
    pre_up = jnp.dot(rows_in, up_mat, preferred_element_type=jnp.float32)
    glu_part = jnp.minimum(pre_gate, clamp_limit)
    lin_part = jnp.clip(pre_up, -clamp_limit, clamp_limit)
    sig_glu = jax.nn.sigmoid(alpha_gate * glu_part)
    activated = (glu_part * sig_glu * (lin_part + 1.0)).astype(jnp.bfloat16)
    grad_act = lax.dot_general(cot_in, down_mat, (((1,), (1,)), ((), ())), preferred_element_type=jnp.float32)
    slope = sig_glu + alpha_gate * glu_part * sig_glu * (1.0 - sig_glu)
    grad_pre_gate = jnp.where(pre_gate < clamp_limit, grad_act * (lin_part + 1.0) * slope, 0.0).astype(jnp.bfloat16)
    grad_pre_up = jnp.where(jnp.abs(pre_up) < clamp_limit, grad_act * glu_part * sig_glu, 0.0).astype(jnp.bfloat16)
    dims = (((0,), (0,)), ((), ()))
    grad_down = lax.dot_general(activated, cot_in, dims, preferred_element_type=jnp.float32).astype(jnp.bfloat16)
    grad_gate = lax.dot_general(rows_in, grad_pre_gate, dims, preferred_element_type=jnp.float32).astype(jnp.bfloat16)
    grad_up = lax.dot_general(rows_in, grad_pre_up, dims, preferred_element_type=jnp.float32).astype(jnp.bfloat16)
    row_count = rows_in.shape[0]
    group_width = FF // N_TP
    partial_sum = jnp.einsum('rpf,dpf->prd', grad_pre_gate.reshape(row_count, N_TP, group_width).astype(jnp.float32), gate_mat.reshape(D, N_TP, group_width).astype(jnp.float32))
    partial_sum = partial_sum + jnp.einsum('rpf,dpf->prd', grad_pre_up.reshape(row_count, N_TP, group_width).astype(jnp.float32), up_mat.reshape(D, N_TP, group_width).astype(jnp.float32))
    rounded = lax.optimization_barrier(partial_sum.astype(jnp.bfloat16))
    route_grad = lax.optimization_barrier(jnp.sum(rounded.astype(jnp.float32), axis=0)).astype(jnp.bfloat16)
    return (grad_gate, grad_up, grad_down, route_grad)

def reference(stream_in, out_cot, route_experts, route_weights, w_gate, w_up, w_down, w_proj, conv_value, conv_gate, conv_taps, conv_result, channel_norm_gain):
    block_routes = route_experts.reshape(N_SP, T_DEV, TOP)
    slot_of, source_of = jax.vmap(lambda routes_one: slot_tables(routes_one, EXPERTS, CAP))(block_routes)
    occupied = source_of >= 0
    source_safe = jnp.maximum(source_of, 0)
    offsets = (jnp.arange(N_SP, dtype=jnp.int32) * T_DEV)[:, None]
    token_of = (source_safe // TOP + offsets).astype(jnp.int32)
    weight_flat = route_weights.reshape(N_SP, T_DEV * TOP)
    slot_weight = jnp.where(occupied, jnp.take_along_axis(weight_flat, source_safe, axis=1), 0.0)
    row_buffer = jnp.where(occupied[..., None], stream_in[token_of], jnp.zeros((), jnp.bfloat16)).astype(jnp.bfloat16)
    cot_buffer = (slot_weight[..., None] * out_cot[token_of].astype(jnp.float32)).astype(jnp.bfloat16)
    row_buffer = row_buffer.reshape(N_SP, EXPERTS, CAP, D).transpose(1, 0, 2, 3).reshape(EXPERTS, N_SP * CAP, D)
    cot_buffer = cot_buffer.reshape(N_SP, EXPERTS, CAP, D).transpose(1, 0, 2, 3).reshape(EXPERTS, N_SP * CAP, D)
    grad_gate, grad_up, grad_down, route_grad = lax.map(one_expert, (row_buffer, cot_buffer, w_gate, w_up, w_down))
    returned = route_grad.reshape(EXPERTS, N_SP, CAP, D).transpose(1, 0, 2, 3).reshape(N_SP, EXPERTS * CAP, D)
    per_route = jnp.take_along_axis(returned, slot_of[..., None], axis=1).astype(jnp.float32)
    per_route = per_route.reshape(TOKENS, TOP, D)
    grad_stream = (out_cot.astype(jnp.float32) + lax.optimization_barrier(jnp.sum(per_route, axis=1))).astype(jnp.bfloat16)
    conv_float = conv_result.astype(jnp.float32)
    chan_mean = lax.optimization_barrier(jnp.sum(conv_float, axis=0)) / CONV_CHANNELS
    chan_var = lax.optimization_barrier(jnp.sum(conv_float * conv_float, axis=0)) / CONV_CHANNELS - chan_mean * chan_mean
    inverse_deviation = lax.rsqrt(chan_var + norm_eps)
    mean_removed = (conv_float - chan_mean) * inverse_deviation
    normalized_rows = mean_removed * channel_norm_gain[:, None]
    sigmoid_of_norm = jax.nn.sigmoid(normalized_rows)
    hidden = (normalized_rows * sigmoid_of_norm).astype(jnp.bfloat16)
    grad_proj = lax.dot_general(grad_stream, hidden, (((0,), (1,)), ((), ())), preferred_element_type=jnp.float32)
    hidden_gradient = lax.dot_general(w_proj, grad_stream, (((0,), (1,)), ((), ())), preferred_element_type=jnp.float32)
    normed_input_gradient = hidden_gradient * sigmoid_of_norm * (1.0 + normalized_rows * (1.0 - sigmoid_of_norm)) * channel_norm_gain[:, None]
    average_products = lax.optimization_barrier(jnp.sum(normed_input_gradient, axis=0)) / CONV_CHANNELS
    cross_products = lax.optimization_barrier(jnp.sum(normed_input_gradient * mean_removed, axis=0)) / CONV_CHANNELS
    conv_output_gradient = inverse_deviation * (normed_input_gradient - average_products - mean_removed * cross_products)
    extended = jnp.concatenate([conv_output_gradient, jnp.zeros((CONV_CHANNELS, CONV_W - 1), jnp.float32)], axis=1)
    grad_gated = jnp.zeros((CONV_CHANNELS, TOKENS), jnp.float32)
    for tap_index in range(CONV_W):
        grad_gated = grad_gated + conv_taps[tap_index][:, None] * extended[:, tap_index:tap_index + TOKENS]
    gate_sig = jax.nn.sigmoid(conv_gate.astype(jnp.float32))
    grad_value = (grad_gated * gate_sig).astype(jnp.bfloat16)
    grad_gate_in = (grad_gated * conv_value.astype(jnp.float32) * gate_sig * (1.0 - gate_sig)).astype(jnp.bfloat16)
    return (grad_gate, grad_up, grad_down, grad_stream, grad_proj, grad_value, grad_gate_in)
```

```python
import functools

import jax
import jax.numpy as jnp
from jax import lax
from jax.experimental import pallas as pl
from jax.experimental.pallas import tpu as pltpu
from jax.sharding import PartitionSpec as P

norm_eps = 1e-05
clamp_limit = 7.0
alpha_gate = 1.702
MESH = pl.DeviceIdType.MESH
f32 = jnp.float32
bf16 = jnp.bfloat16


def dot(a, b, ca=1, cb=0):
    return lax.dot_general(a, b, (((ca,), (cb,)), ((), ())), preferred_element_type=f32)


def aligned(start, size):
    return pl.ds(pl.multiple_of(start, size), size)


def greet(n, s, q, tp_peers):
    barrier = pltpu.get_barrier_semaphore()
    for d in range(1, n):
        pl.semaphore_signal(
            barrier, inc=1, device_id={"sp": lax.rem(s + d, n), "tp": q}, device_id_type=MESH
        )
    for peer in tp_peers:
        pl.semaphore_signal(barrier, inc=1, device_id={"sp": s, "tp": peer}, device_id_type=MESH)
    pl.semaphore_wait(barrier, n - 1 + len(tp_peers))


def remote(src, dst, send, recv, sp, tp):
    return pltpu.make_async_remote_copy(
        src_ref=src,
        dst_ref=dst,
        send_sem=send,
        recv_sem=recv,
        device_id={"sp": sp, "tp": tp},
        device_id_type=MESH,
    )


def partners(q):
    core, other = lax.rem(q, 2), q // 2
    return (2 * other + 1 - core, 2 * (1 - other) + core, 2 * (1 - other) + 1 - core)


def slot_pick(routes, weights, first, slots, cap):
    top, tokens = routes.shape
    local = routes - first
    expert_ids = lax.broadcasted_iota(jnp.int32, (8, tokens), 0)
    hits = [expert_ids == local[k : k + 1, :] for k in range(top)]
    count = sum(h.astype(f32) for h in hits)
    earlier = (
        lax.broadcasted_iota(jnp.int32, (tokens, tokens), 0)
        < lax.broadcasted_iota(jnp.int32, (tokens, tokens), 1)
    ).astype(f32)
    before = dot(count.astype(bf16), earlier.astype(bf16))
    slot_ids = lax.broadcasted_iota(jnp.int32, (slots, tokens), 0)
    pick = jnp.zeros((slots, tokens), f32)
    weighted = jnp.zeros((slots, tokens), f32)
    for k in range(top):
        rank = jnp.sum(jnp.where(hits[k], before, 0.0), axis=0, keepdims=True)
        here = slot_ids == local[k : k + 1, :] * cap + rank.astype(jnp.int32)
        pick = jnp.where(here, 1.0, pick)
        weighted = jnp.where(here, weights[k : k + 1, :], weighted)
    return pick.astype(bf16), jnp.sum(weighted, axis=1, keepdims=True)


def fused_kernel(n, cap, channel_total, names, *refs):
    r = dict(zip(names, refs))
    s, q = lax.axis_index("sp"), lax.axis_index("tp")
    q_core, q_y, q_far = partners(q)
    peers = (q_core, q_y, q_far)
    core, y = lax.rem(q, 2), q // 2
    z, x = s // 2, lax.rem(s, 2)
    sx = s + 1 - 2 * x
    nz = n // 2
    stream, cot = r["stream"], r["cot"]
    tokens, model_width = stream.shape
    width = r["ret"].shape[-1]
    top = r["routes"].shape[0]
    icols = r["gproj"].shape[0]
    pair = 2 * cap
    taps_count = r["taps"].shape[0]
    quarter, quarter_y = aligned(q * width, width), aligned(q_y * width, width)
    wg, wu, wd = r["wg"], r["wu"], r["wd"]
    full = (r["rows"], r["cots"])
    copies = []
    conditional = []

    loads = {}
    for i, name in enumerate(input_names):
        loads[name] = pltpu.make_async_copy(r[name + "_h"], r[name], r["load"].at[i])
        loads[name].start()

    def start(src, dst, key, index, sp, tp, recv=None):
        send, arrive = r["send_" + key], r["recv_" + key]
        copy = remote(src, dst, send.at[index], arrive.at[index if recv is None else recv], sp, tp)
        copy.start()
        copies.append(copy)
        return copy

    def start_if(cond, src, dst, key, index, sp, tp, recv):
        copy = remote(
            src, dst, r["send_" + key].at[index], r["recv_" + key].at[recv], sp, tp
        )
        pl.when(cond)(copy.start)
        conditional.append((cond, copy))

    def landed(dst, key, index):
        remote(dst, dst, r["send_" + key].at[index], r["recv_" + key].at[index], s, q).wait_recv()

    high = z // (nz // 2)
    folded = z + high * (nz - 1 - 2 * z)
    far_order = [1 - folded, 2 + 0 * z, 3 + 0 * z]
    source = [f + high * (nz - 1 - 2 * f) for f in far_order]
    chunk_z = [z] + source
    chunk_rows = [aligned(c * pair, pair) for c in chunk_z]

    def block_rows(block):
        return aligned(block * cap, cap)

    loads["routes"].wait()
    loads["weights"].wait()
    meta = r["meta"]
    routes_own, weights_own = r["routes"][...], r["weights"][...]
    meta[z] = jnp.concatenate(
        [routes_own.astype(f32), weights_own, jnp.zeros((8 - 2 * top, tokens), f32)], axis=0
    )
    greet(n, s, q, peers)
    meta_waits = [
        start(meta.at[z], meta.at[z], "m", d - 1, 2 * lax.rem(z + d, nz) + x, q)
        for d in range(1, nz)
    ]
    raw = r["raw"]
    values = (stream, cot)
    for a, name in enumerate(("stream", "cot")):
        loads[name].wait()
        src = values[a].at[:, quarter]
        start_if(z < nz - 1, src, raw.at[a, z], "zo", (a, 0), s + 2, q, (a, z))
        start_if(z > 0, src, raw.at[a, z], "zp", (a, 0), s - 2, q, (a, z))

    def landed_raw(a, j):
        dst = raw.at[a, source[j]]
        from_below = source[j] < z

        @pl.when(from_below)
        def _():
            landed(dst, "zo", (a, source[j]))

        @pl.when(source[j] > z)
        def _():
            landed(dst, "zp", (a, source[j]))

        start_if((source[j] < z) & (z < nz - 1), dst, dst, "zo", (a, j + 1), s + 2, q, (a, source[j]))
        start_if((source[j] > z) & (z > 0), dst, dst, "zp", (a, j + 1), s - 2, q, (a, source[j]))

    pick, slot_weight = slot_pick(routes_own, weights_own, 2 * z, pair, cap)
    ownbuf = r["ownbuf"]
    own_half, other_half = aligned(x * cap, cap), aligned((1 - x) * cap, cap)
    for a in range(2):
        got = dot(pick, values[a][...])
        ownbuf[a] = (got * slot_weight if a else got).astype(bf16)
        for i, cols in enumerate((quarter, quarter_y)):
            start(
                ownbuf.at[a, other_half, cols], full[a].at[block_rows(s), cols],
                "xo", (a, i), sx, q,
            )
    for a in range(2):
        full[a][block_rows(s), :] = ownbuf[a, own_half, :]
    r["pick"][...] = slot_pick(routes_own, weights_own, 0, n * cap, cap)[0]

    def exchange_stats(buffer, first, second, which):
        lanes = lax.broadcasted_iota(jnp.int32, (tokens, tokens), 1)
        packed = jnp.where(lanes == 0, first, jnp.where(lanes == 1, second, 0.0))
        buffer[3] = packed.T[0:8, :]
        return [
            start(buffer.at[3], buffer.at[p], "s", (which, p), s, peer)
            for p, peer in enumerate(peers)
        ]

    def summed_stats(buffer, waits):
        for w in waits:
            w.wait_recv()
        total = (buffer[3] + buffer[0]) + (buffer[1] + buffer[2])
        wide = jnp.concatenate([total, jnp.zeros((tokens - 8, tokens), f32)], axis=0).T
        return wide[:, 0:1], wide[:, 1:2]

    loads["conv"].wait()
    loads["gain"].wait()
    conv = r["conv"][...].astype(f32).T
    stat_waits = exchange_stats(
        r["stat"],
        jnp.sum(conv, axis=1, keepdims=True),
        jnp.sum(conv * conv, axis=1, keepdims=True),
        0,
    )
    for copy in meta_waits:
        copy.wait_recv()
    picks = []
    for j in range(nz - 1):
        there = meta[source[j]]
        picks.append(
            slot_pick(there[0:top].astype(jnp.int32), there[top : 2 * top], 2 * z, pair, cap)
        )
    pickbuf = r["pickbuf"]

    def arrive_raw(j, a):
        landed_raw(a, j)
        pick_j, weight_j = picks[j]
        got = dot(pick_j, raw[a, source[j]])
        pickbuf[a, j] = (got * weight_j if a else got).astype(bf16)
        rows = block_rows(2 * source[j] + x)
        mine, other = pickbuf.at[a, j, own_half], pickbuf.at[a, j, other_half]
        here = full[a].at[rows, quarter]
        start(other, here, "x", (a, j), sx, q)
        start(mine, here, "y", (a, j, 0), s, q_y)
        start(mine, here, "c", (a, j, 0), s, q_core)
        full[a][rows, quarter] = pickbuf[a, j, own_half]

    def arrive_x(j, a):
        here = full[a].at[block_rows(2 * source[j] + 1 - x), quarter]
        landed(here, "x", (a, j))
        start(here, here, "y", (a, j, 1), s, q_y)
        start(here, here, "c", (a, j, 1), s, q_core)

    def arrive_y(j, a):
        for i in range(2):
            here = full[a].at[block_rows(2 * source[j] + (x if i == 0 else 1 - x)), quarter_y]
            landed(here, "y", (a, j, i))
            start(here, here, "d", (a, j, i), s, q_core)

    def complete(j, a):
        for i in range(2):
            rows = block_rows(2 * source[j] + (x if i == 0 else 1 - x))
            for key, owner in (("c", q_core), ("d", q_far)):
                landed(full[a].at[rows, aligned(owner * width, width)], key, (a, j, i))

    def arrive_own(a):
        for i, cols in enumerate((quarter, quarter_y)):
            here = full[a].at[block_rows(sx), cols]
            landed(here, "xo", (a, i))
            start(here, here, "xc", (a, i), s, q_core)

    def complete_own(a):
        for i, owner in enumerate((q_core, q_far)):
            landed(full[a].at[block_rows(sx), aligned(owner * width, width)], "xc", (a, i))

    act_all, dg_all, du_all, part = r["act"], r["dg"], r["du"], r["part"]
    pre_gate_ref, pre_up_ref = r["pre_gate"], r["pre_up"]

    def first_half(k):
        rows = chunk_rows[k]
        if k:
            complete(k - 1, 0)
        else:
            complete_own(0)
            loads["wg"].wait()
            loads["wu"].wait()
        rows_in = full[0][rows, :]
        pre_gate_ref[...] = dot(rows_in, wg[...])
        pre_up_ref[...] = dot(rows_in, wu[...])

    def second_half(k):
        rows = chunk_rows[k]
        if k:
            complete(k - 1, 1)
        else:
            complete_own(1)
            loads["wd"].wait()
        grad_act = dot(full[1][rows, :], wd[...], 1, 1)
        pre_gate, pre_up = pre_gate_ref[...], pre_up_ref[...]
        glu_part = jnp.minimum(pre_gate, clamp_limit)
        lin_part = jnp.clip(pre_up, -clamp_limit, clamp_limit)
        sig_glu = jax.nn.sigmoid(alpha_gate * glu_part)
        act_all[rows, :] = (glu_part * sig_glu * (lin_part + 1.0)).astype(bf16)
        slope = sig_glu + alpha_gate * glu_part * sig_glu * (1.0 - sig_glu)
        dg = jnp.where(
            pre_gate < clamp_limit, grad_act * (lin_part + 1.0) * slope, 0.0
        ).astype(bf16)
        du = jnp.where(
            jnp.abs(pre_up) < clamp_limit, grad_act * glu_part * sig_glu, 0.0
        ).astype(bf16)
        dg_all[rows, :] = dg
        du_all[rows, :] = du
        part[rows, :] = (dot(dg, wg[...], 1, 1) + dot(du, wu[...], 1, 1)).astype(bf16)
        for h, half in ((0, 1 - y), (1, y)):
            start(
                part.at[rows, aligned((2 * half + 1 - core) * width, width)],
                r["from_core"].at[h, rows], "rc", (k, h), s, q_core,
            )

    def reduce_core(k):
        rows = chunk_rows[k]
        landed(r["from_core"].at[0, rows], "rc", (k, 0))
        r["to_y"][rows, :] = (
            part[rows, quarter_y].astype(f32) + r["from_core"][0, rows, :].astype(f32)
        ).astype(bf16)
        start(r["to_y"].at[rows], r["from_y"].at[rows], "ry", k, s, q_y)
        landed(r["from_core"].at[1, rows], "rc", (k, 1))
        r["own"][rows, :] = part[rows, quarter].astype(f32) + r["from_core"][
            1, rows, :
        ].astype(f32)

    ret = r["ret"]
    mine_slots = block_rows(s)

    def reduce_y(k):
        rows = chunk_rows[k]
        landed(r["from_y"].at[rows], "ry", k)
        r["to_xz"][rows, :] = (
            r["own"][rows, :] + r["from_y"][rows, :].astype(f32)
        ).astype(bf16)
        if k:
            for i in range(2):
                home = 2 * chunk_z[k] + i
                start(r["to_xz"].at[block_rows(home)], ret.at[mine_slots], "r", (k, i), home, q, (s, 0))
        else:
            start(r["to_xz"].at[block_rows(sx)], ret.at[mine_slots], "r", (0, 0), sx, q, (s, 0))
            ret[mine_slots, :] = r["to_xz"][mine_slots, :]

    hid_all = r["hid"]

    def hid_rows(block):
        return aligned(block * tokens, tokens)

    def relay_hidden(j):
        if j < 0:
            here = hid_all.at[hid_rows(s)]
            start_if(z < nz - 1, here, here, "ho", 0, s + 2, q, z)
            start_if(z > 0, here, here, "hp", 0, s - 2, q, z)
        else:
            here = hid_all.at[hid_rows(2 * source[j] + x)]

            @pl.when(source[j] < z)
            def _():
                landed(here, "ho", source[j])

            @pl.when(source[j] > z)
            def _():
                landed(here, "hp", source[j])

            start_if((source[j] < z) & (z < nz - 1), here, here, "ho", j + 1, s + 2, q, source[j])
            start_if((source[j] > z) & (z > 0), here, here, "hp", j + 1, s - 2, q, source[j])
        start(here, here, "hx", j + 1, sx, q)

    def weight_grad(left, right, out, by_left):
        tile = right.shape[1] if by_left else left.shape[1]

        def step(i, carry):
            there = aligned(i * tile, tile)
            if by_left:
                out[there, :] = dot(left[:, there], right[...], 0, 0).astype(bf16)
            else:
                out[:, there] = dot(left[...], right[:, there], 0, 0).astype(bf16)
            return carry

        lax.fori_loop(0, model_width // tile, step, 0)

    arrive_raw(0, 0)
    arrive_own(0)
    chan_sum, chan_sq = summed_stats(r["stat"], stat_waits)
    chan_mean = chan_sum / channel_total
    chan_var = chan_sq / channel_total - chan_mean * chan_mean
    inverse_deviation = lax.rsqrt(chan_var + norm_eps)
    mean_removed = (conv - chan_mean) * inverse_deviation
    gain = r["gain"][...]
    normed = mean_removed * gain
    sig = jax.nn.sigmoid(normed)
    hid_all[hid_rows(s), :] = (normed * sig).astype(bf16)
    r["slope"][...] = sig * (1.0 + normed * (1.0 - sig)) * gain
    r["removed"][...] = mean_removed
    r["inverse"][...] = jnp.broadcast_to(inverse_deviation, r["inverse"].shape)
    arrive_raw(0, 1)
    arrive_own(1)
    arrive_x(0, 0)
    first_half(0)
    arrive_raw(1, 0)
    arrive_y(0, 0)
    arrive_x(0, 1)
    second_half(0)
    arrive_raw(1, 1)
    arrive_y(0, 1)
    arrive_x(1, 0)
    first_half(1)
    arrive_raw(2, 0)
    arrive_y(1, 0)
    arrive_x(1, 1)
    second_half(1)
    arrive_raw(2, 1)
    relay_hidden(-1)
    arrive_y(1, 1)
    arrive_x(2, 0)
    reduce_core(0)
    first_half(2)
    arrive_x(2, 1)
    arrive_y(2, 0)
    second_half(2)
    reduce_core(1)
    arrive_y(2, 1)
    first_half(3)
    second_half(3)
    reduce_y(0)
    reduce_core(2)
    reduce_core(3)
    relay_hidden(0)
    reduce_y(1)
    weight_grad(r["act"], r["cots"], r["gdown"], False)
    reduce_y(2)
    relay_hidden(1)
    reduce_y(3)
    relay_hidden(2)
    weight_grad(r["rows"], r["dg"], r["ggate"], True)
    weight_grad(r["rows"], r["du"], r["gup"], True)

    for d in range(1, n):
        e = lax.rem(s + d, n)
        landed(ret.at[block_rows(e)], "r", (e, 0))
    gs_ref = r["gs"]
    combined = dot(r["pick"][...], ret[...], 0, 0) + cot[:, quarter].astype(f32)
    gs_ref[:, quarter] = combined.astype(bf16)
    mine_cols = gs_ref.at[:, quarter]
    by_core = start(mine_cols, mine_cols, "g", 0, s, q_core)
    by_y = start(mine_cols, mine_cols, "g", 1, s, q_y)
    loads["proj"].wait()
    proj = r["proj"]

    def partial_of(owner):
        cols = aligned(owner * width, width)
        return dot(gs_ref[:, cols], proj[cols, :])

    grad_hidden = partial_of(q)
    by_y.wait_recv()
    y_cols = gs_ref.at[:, quarter_y]
    by_far = start(y_cols, y_cols, "g", 2, s, q_core)
    grad_hidden = grad_hidden + partial_of(q_y)
    by_core.wait_recv()
    grad_hidden = grad_hidden + partial_of(q_core)
    by_far.wait_recv()
    grad_hidden = grad_hidden + partial_of(q_far)
    half_rows = tokens // 2
    part_rows = aligned(core * half_rows, half_rows)
    land = aligned(s * tokens + core * half_rows, half_rows)
    order = [lax.rem(s + d, n) for d in range(1, n)]
    col_all = r["col"]
    col_waits = [
        start(
            gs_ref.at[part_rows, aligned(order[j] * icols, icols)], col_all.at[land],
            "k", j, order[j], q,
        )
        for j in range(n - 1)
    ]
    col_all[hid_rows(s), :] = gs_ref[:, aligned(s * icols, icols)]
    mean_removed = r["removed"][...]
    inverse_deviation = r["inverse"][:, 0:1]
    norm_grad = grad_hidden * r["slope"][...]
    stat_waits = exchange_stats(
        r["stat2"],
        jnp.sum(norm_grad, axis=1, keepdims=True),
        jnp.sum(norm_grad * mean_removed, axis=1, keepdims=True),
        1,
    )
    avg, cross = summed_stats(r["stat2"], stat_waits)
    conv_grad = inverse_deviation * (
        norm_grad - avg / channel_total - mean_removed * (cross / channel_total)
    )
    ext = r["ext"]
    rim = ext.shape[0] - tokens
    ext[0:tokens, :] = conv_grad
    halo = remote(
        ext.at[0:rim], ext.at[tokens : tokens + rim], r["send_e"].at[0], r["recv_e"].at[0],
        lax.rem(s + n - 1, n), q,
    )
    halo.start()
    forwards = []
    for j in range(n - 1):
        col_waits[j].wait_recv()
        origin = lax.rem(s + n - (j + 1), n)
        there = col_all.at[aligned(origin * tokens + core * half_rows, half_rows)]
        forwards.append(start(there, there, "f", j, s, q_core))
    loads["taps"].wait()
    loads["gate"].wait()
    loads["value"].wait()
    halo.wait_recv()
    edge = ext[tokens : tokens + rim, :]
    halo.wait_send()
    ext[tokens : tokens + rim, :] = jnp.where(s == n - 1, 0.0, edge)
    acc = jnp.zeros((tokens, ext.shape[1]), f32)
    for tap in range(taps_count):
        acc = acc + r["taps"][tap : tap + 1, :] * ext[tap : tap + tokens, :]
    gated = acc.T
    gate_sig = jax.nn.sigmoid(r["gate"][...].astype(f32))
    r["gvalue"][...] = (gated * gate_sig).astype(bf16)
    r["ggin"][...] = (
        gated * r["value"][...].astype(f32) * gate_sig * (1.0 - gate_sig)
    ).astype(bf16)
    for copy in forwards:
        copy.wait_recv()
    for k in range(nz):
        landed(hid_all.at[hid_rows(2 * chunk_z[k] + 1 - x)], "hx", k)
    r["gproj"][...] = dot(col_all[...], hid_all[...], 0, 0)
    for copy in copies:
        copy.wait_send()
    for cond, copy in conditional:
        pl.when(cond)(copy.wait_send)


input_names = (
    "routes", "weights", "stream", "cot", "conv", "gain", "wg", "wu", "wd", "proj", "value",
    "gate", "taps",
)


def fused(
    routes, weights, stream, cot, wg, wu, wd, proj, value, gate, taps, conv, gain, n, cap, tp_count
):
    tokens, model_width = stream.shape
    hidden_width = wg.shape[1]
    width = model_width // tp_count
    channels = value.shape[0]
    icols = model_width // n
    slots = n * cap
    rim = -(-(taps.shape[0] - 1) // 8) * 8
    nz = n // 2
    V, dma = pltpu.VMEM, pltpu.SemaphoreType.DMA
    given = dict(
        routes=routes, weights=weights, stream=stream, cot=cot, conv=conv, gain=gain, wg=wg, wu=wu,
        wd=wd, proj=proj, value=value, gate=gate, taps=taps,
    )
    outs = dict(
        ggate=((model_width, hidden_width), bf16),
        gup=((model_width, hidden_width), bf16),
        gdown=((hidden_width, model_width), bf16),
        gs=((tokens, model_width), bf16),
        gproj=((icols, channels), f32),
        gvalue=((channels, tokens), bf16),
        ggin=((channels, tokens), bf16),
    )
    scratch = {name: V(given[name].shape, given[name].dtype) for name in input_names}
    scratch.update(
        meta=V((nz, 8, tokens), f32),
        raw=V((2, nz, tokens, width), bf16),
        ownbuf=V((2, 2 * cap, model_width), bf16),
        pickbuf=V((2, nz - 1, 2 * cap, width), bf16),
        pick=V((slots, tokens), bf16),
        rows=V((slots, model_width), bf16),
        cots=V((slots, model_width), bf16),
        act=V((slots, hidden_width), bf16),
        dg=V((slots, hidden_width), bf16),
        du=V((slots, hidden_width), bf16),
        part=V((slots, model_width), bf16),
        pre_gate=V((2 * cap, hidden_width), f32),
        pre_up=V((2 * cap, hidden_width), f32),
        from_core=V((2, slots, width), bf16),
        own=V((slots, width), f32),
        to_y=V((slots, width), bf16),
        from_y=V((slots, width), bf16),
        to_xz=V((slots, width), bf16),
        ret=V((slots, width), bf16),
        hid=V((n * tokens, channels), bf16),
        col=V((n * tokens, icols), bf16),
        slope=V((tokens, channels), f32),
        removed=V((tokens, channels), f32),
        inverse=V((tokens, tokens), f32),
        stat=V((4, 8, tokens), f32),
        stat2=V((4, 8, tokens), f32),
        ext=V((tokens + rim, channels), f32),
        load=dma((len(input_names),)),
    )
    sems = dict(
        m=(nz - 1,), zo=(2, nz), zp=(2, nz), xo=(2, 2), xc=(2, 2), x=(2, nz - 1), y=(2, nz - 1, 2),
        c=(2, nz - 1, 2), d=(2, nz - 1, 2), s=(2, 3), rc=(nz, 2), ry=(nz,), ho=(nz,), hp=(nz,),
        hx=(nz,), g=(3,), k=(n - 1,), f=(n - 1,), e=(1,), r=(n, 2),
    )
    for key, shape in sems.items():
        scratch["send_" + key] = dma(shape)
        scratch["recv_" + key] = dma(shape)
    names = [name + "_h" for name in input_names] + list(outs) + list(scratch)
    return pl.pallas_call(
        functools.partial(fused_kernel, n, cap, channels * tp_count, tuple(names)),
        out_shape=tuple(jax.ShapeDtypeStruct(*o) for o in outs.values()),
        in_specs=[pl.BlockSpec(memory_space=pltpu.HBM)] * len(input_names),
        out_specs=[pl.BlockSpec(memory_space=V)] * len(outs),
        scratch_shapes=list(scratch.values()),
        compiler_params=pltpu.CompilerParams(
            collective_id=0, has_side_effects=True, vmem_limit_bytes=48 << 20
        ),
        name="fused",
    )(*[given[name] for name in input_names])


def flush_kernel(*refs):
    count = len(refs) // 2
    copies = [
        pltpu.make_async_copy(refs[i], refs[count + i], refs[-1].at[i]) for i in range(count)
    ]
    for copy in copies:
        copy.start()
    for copy in copies:
        copy.wait()


def flush(*arrays):
    return pl.pallas_call(
        flush_kernel,
        out_shape=tuple(jax.ShapeDtypeStruct(a.shape, a.dtype) for a in arrays),
        in_specs=[pl.BlockSpec(memory_space=pltpu.VMEM)] * len(arrays),
        out_specs=[pl.BlockSpec(memory_space=pltpu.HBM)] * len(arrays),
        scratch_shapes=[pltpu.SemaphoreType.DMA((len(arrays),))],
        compiler_params=pltpu.CompilerParams(vmem_limit_bytes=4 << 20),
        name="flush",
    )(*arrays)


def body(
    stream_in, out_cot, route_experts, route_weights, w_gate, w_up, w_down, w_proj,
    conv_value, conv_gate, conv_taps, conv_result, channel_norm_gain,
):
    n = lax.axis_size("sp")
    tp_count = lax.axis_size("tp")
    experts = w_gate.shape[0] * n
    tokens, model_width = stream_in.shape
    cap = 2 * route_experts.shape[1] * tokens // experts
    outs = flush(
        *fused(
            route_experts.T, route_weights.T, stream_in, out_cot, w_gate[0], w_up[0], w_down[0],
            w_proj, conv_value, conv_gate, conv_taps, conv_result, channel_norm_gain[None, :],
            n, cap, tp_count,
        )
    )
    return (outs[0][None], outs[1][None], outs[2][None]) + tuple(outs[3:])


def from_behind(value, axis, steps):
    count = lax.axis_size(axis)
    leading, last = (max(0, -steps), min(count, count - steps))
    return lax.ppermute(value, axis, [(source, source + steps) for source in range(leading, last)])


def slot_tables(block_routes, experts_all, capacity):
    flat_routes = block_routes.reshape(-1)
    assigns = flat_routes.shape[0]
    onehot = (flat_routes[:, None] == jnp.arange(experts_all, dtype=jnp.int32)[None, :]).astype(
        jnp.int32
    )
    before = jnp.cumsum(onehot, axis=0) - onehot
    rank_in = jnp.sum(before * onehot, axis=1)
    slot_of = flat_routes * capacity + rank_in
    source_of = (
        jnp.full((experts_all * capacity,), -1, jnp.int32)
        .at[slot_of]
        .set(jnp.arange(assigns, dtype=jnp.int32))
    )
    return (slot_of, source_of)


def combine_routes(returned, slot_of, cot_cols, token_rows, top_count):
    feature_count = returned.shape[-1]
    flat_back = returned.reshape(-1, feature_count)
    per_route = flat_back[slot_of].astype(jnp.float32).reshape(token_rows, top_count, feature_count)
    return (cot_cols.astype(jnp.float32) + jnp.sum(per_route, axis=1)).astype(jnp.bfloat16)


def expert_terms_plain(rows_in, cot_in, w_gate, w_up, w_down):
    pre_gate = jnp.einsum("secd,edf->secf", rows_in, w_gate, preferred_element_type=jnp.float32)
    pre_up = jnp.einsum("secd,edf->secf", rows_in, w_up, preferred_element_type=jnp.float32)
    glu_part = jnp.minimum(pre_gate, clamp_limit)
    lin_part = jnp.clip(pre_up, -clamp_limit, clamp_limit)
    sig_glu = jax.nn.sigmoid(alpha_gate * glu_part)
    activated = (glu_part * sig_glu * (lin_part + 1.0)).astype(jnp.bfloat16)
    grad_act = jnp.einsum("secd,efd->secf", cot_in, w_down, preferred_element_type=jnp.float32)
    slope = sig_glu + alpha_gate * glu_part * sig_glu * (1.0 - sig_glu)
    grad_pre_gate = jnp.where(
        pre_gate < clamp_limit, grad_act * (lin_part + 1.0) * slope, 0.0
    ).astype(jnp.bfloat16)
    grad_pre_up = jnp.where(
        jnp.abs(pre_up) < clamp_limit, grad_act * glu_part * sig_glu, 0.0
    ).astype(jnp.bfloat16)
    grad_down = jnp.einsum(
        "secf,secd->efd", activated, cot_in, preferred_element_type=jnp.float32
    ).astype(jnp.bfloat16)
    grad_gate = jnp.einsum(
        "secd,secf->edf", rows_in, grad_pre_gate, preferred_element_type=jnp.float32
    ).astype(jnp.bfloat16)
    grad_up = jnp.einsum(
        "secd,secf->edf", rows_in, grad_pre_up, preferred_element_type=jnp.float32
    ).astype(jnp.bfloat16)
    input_part = jnp.einsum(
        "secf,edf->secd", grad_pre_gate, w_gate, preferred_element_type=jnp.float32
    )
    input_part = input_part + jnp.einsum(
        "secf,edf->secd", grad_pre_up, w_up, preferred_element_type=jnp.float32
    )
    return (grad_gate, grad_up, grad_down, input_part)


def body_plain(
    stream_in,
    out_cot,
    route_experts,
    route_weights,
    w_gate,
    w_up,
    w_down,
    w_proj,
    conv_value,
    conv_gate,
    conv_taps,
    conv_result,
    channel_norm_gain,
):
    sp_count = lax.axis_size("sp")
    tp_count = lax.axis_size("tp")
    local_experts = w_gate.shape[0]
    experts_all = local_experts * sp_count
    token_rows, model_width = stream_in.shape
    top_count = route_experts.shape[1]
    capacity = 2 * top_count * token_rows // experts_all
    slot_of, source_of = slot_tables(route_experts, experts_all, capacity)
    occupied = source_of >= 0
    source_safe = jnp.maximum(source_of, 0)
    token_of = source_safe // top_count
    slot_weight = jnp.where(occupied, route_weights.reshape(-1)[source_safe], 0.0)
    row_buffer = jnp.where(occupied[:, None], stream_in[token_of], jnp.zeros((), jnp.bfloat16))
    cot_buffer = (slot_weight[:, None] * out_cot[token_of].astype(jnp.float32)).astype(jnp.bfloat16)
    row_buffer = row_buffer.reshape(experts_all, capacity, model_width)
    cot_buffer = cot_buffer.reshape(experts_all, capacity, model_width)
    slice_width = model_width // tp_count
    slice_start = lax.axis_index("tp") * slice_width
    row_slice = lax.dynamic_slice_in_dim(row_buffer, slice_start, slice_width, 2)
    cot_slice = lax.dynamic_slice_in_dim(cot_buffer, slice_start, slice_width, 2)
    row_slice, cot_slice = (
        lax.all_to_all(row_slice, "sp", split_axis=0, concat_axis=0, tiled=True),
        lax.all_to_all(cot_slice, "sp", split_axis=0, concat_axis=0, tiled=True),
    )
    rows_in, cot_in = (
        lax.all_gather(row_slice, "tp", axis=2, tiled=True),
        lax.all_gather(cot_slice, "tp", axis=2, tiled=True),
    )
    rows_in = rows_in.reshape(sp_count, local_experts, capacity, model_width)
    cot_in = cot_in.reshape(sp_count, local_experts, capacity, model_width)
    grad_gate, grad_up, grad_down, input_part = expert_terms_plain(rows_in, cot_in, w_gate, w_up, w_down)
    shared = lax.psum_scatter(
        input_part.astype(jnp.bfloat16), "tp", scatter_dimension=3, tiled=True
    )
    returned = shared.reshape(experts_all, capacity, slice_width)
    returned = lax.all_to_all(returned, "sp", split_axis=0, concat_axis=0, tiled=True)
    cot_cols = lax.dynamic_slice_in_dim(out_cot, slice_start, slice_width, 1)
    stream_part = combine_routes(returned, slot_of, cot_cols, token_rows, top_count)
    grad_stream = lax.all_gather(stream_part, "tp", axis=1, tiled=True)
    channel_total = conv_result.shape[0] * tp_count
    positions = conv_result.shape[1]
    conv_float = conv_result.astype(jnp.float32)
    chan_sum, chan_sq = lax.psum(
        (jnp.sum(conv_float, axis=0), jnp.sum(conv_float * conv_float, axis=0)), "tp"
    )
    chan_mean = chan_sum / channel_total
    chan_var = chan_sq / channel_total - chan_mean * chan_mean
    inverse_deviation = lax.rsqrt(chan_var + norm_eps)
    mean_removed = (conv_float - chan_mean) * inverse_deviation
    normalized_rows = mean_removed * channel_norm_gain[:, None]
    sigmoid_of_norm = jax.nn.sigmoid(normalized_rows)
    hidden = (normalized_rows * sigmoid_of_norm).astype(jnp.bfloat16)
    grad_proj = lax.psum_scatter(
        lax.dot_general(
            grad_stream, hidden, (((0,), (1,)), ((), ())), preferred_element_type=jnp.float32
        ),
        "sp",
        scatter_dimension=0,
        tiled=True,
    )
    hidden_gradient = lax.dot_general(
        w_proj, grad_stream, (((0,), (1,)), ((), ())), preferred_element_type=jnp.float32
    )
    normed_input_gradient = (
        hidden_gradient
        * sigmoid_of_norm
        * (1.0 + normalized_rows * (1.0 - sigmoid_of_norm))
        * channel_norm_gain[:, None]
    )
    average_products, cross_products = lax.psum(
        (
            jnp.sum(normed_input_gradient, axis=0),
            jnp.sum(normed_input_gradient * mean_removed, axis=0),
        ),
        "tp",
    )
    conv_output_gradient = inverse_deviation * (
        normed_input_gradient
        - average_products / channel_total
        - mean_removed * (cross_products / channel_total)
    )
    taps_count = conv_taps.shape[0]
    next_rim = from_behind(conv_output_gradient[:, : taps_count - 1], "sp", -1)
    extended = jnp.concatenate([conv_output_gradient, next_rim], axis=1)
    grad_gated = jnp.zeros_like(conv_output_gradient)
    for tap_index in range(taps_count):
        grad_gated = (
            grad_gated
            + conv_taps[tap_index][:, None] * extended[:, tap_index : tap_index + positions]
        )
    gate_sig = jax.nn.sigmoid(conv_gate.astype(jnp.float32))
    grad_value = (grad_gated * gate_sig).astype(jnp.bfloat16)
    grad_gate_in = (
        grad_gated * conv_value.astype(jnp.float32) * gate_sig * (1.0 - gate_sig)
    ).astype(jnp.bfloat16)
    return (grad_gate, grad_up, grad_down, grad_stream, grad_proj, grad_value, grad_gate_in)


def solution(mesh):
    return jax.shard_map(
        body if (mesh.shape["sp"], mesh.shape["tp"]) == (8, 4) else body_plain,
        mesh=mesh,
        in_specs=(
            P("sp", None),
            P("sp", None),
            P("sp", None),
            P("sp", None),
            P("sp", None, "tp"),
            P("sp", None, "tp"),
            P("sp", "tp", None),
            P(None, "tp"),
            P("tp", "sp"),
            P("tp", "sp"),
            P(None, "tp"),
            P("tp", "sp"),
            P("tp"),
        ),
        out_specs=(
            P("sp", None, "tp"),
            P("sp", None, "tp"),
            P("sp", "tp", None),
            P("sp", None),
            P("sp", "tp"),
            P("tp", "sp"),
            P("tp", "sp"),
        ),
        check_vma=False,
    )
```

```python
import functools

import jax
import jax.numpy as jnp
from jax import lax
from jax.experimental import pallas as pl
from jax.experimental.pallas import tpu as pltpu
from jax.sharding import PartitionSpec as P

norm_eps = 1e-05
clamp_limit = 7.0
alpha_gate = 1.702
MESH = pl.DeviceIdType.MESH
f32 = jnp.float32
bf16 = jnp.bfloat16


def dot(a, b, ca=1, cb=0):
    return lax.dot_general(a, b, (((ca,), (cb,)), ((), ())), preferred_element_type=f32)


def aligned(start, size):
    return pl.ds(pl.multiple_of(start, size), size)


def greet(n, s, q, tp_peers):
    barrier = pltpu.get_barrier_semaphore()
    for d in range(1, n):
        pl.semaphore_signal(
            barrier, inc=1, device_id={"sp": lax.rem(s + d, n), "tp": q}, device_id_type=MESH
        )
    for peer in tp_peers:
        pl.semaphore_signal(barrier, inc=1, device_id={"sp": s, "tp": peer}, device_id_type=MESH)
    pl.semaphore_wait(barrier, n - 1 + len(tp_peers))


def remote(src, dst, send, recv, sp, tp):
    return pltpu.make_async_remote_copy(
        src_ref=src,
        dst_ref=dst,
        send_sem=send,
        recv_sem=recv,
        device_id={"sp": sp, "tp": tp},
        device_id_type=MESH,
    )


def partners(q):
    core, other = lax.rem(q, 2), q // 2
    return (2 * other + 1 - core, 2 * (1 - other) + core, 2 * (1 - other) + 1 - core)


def slot_pick(routes, weights, first, slots, cap):
    top, tokens = routes.shape
    local = routes - first
    expert_ids = lax.broadcasted_iota(jnp.int32, (8, tokens), 0)
    hits = [expert_ids == local[k : k + 1, :] for k in range(top)]
    count = sum(h.astype(f32) for h in hits)
    earlier = (
        lax.broadcasted_iota(jnp.int32, (tokens, tokens), 0)
        < lax.broadcasted_iota(jnp.int32, (tokens, tokens), 1)
    ).astype(f32)
    before = dot(count.astype(bf16), earlier.astype(bf16))
    slot_ids = lax.broadcasted_iota(jnp.int32, (slots, tokens), 0)
    pick = jnp.zeros((slots, tokens), f32)
    weighted = jnp.zeros((slots, tokens), f32)
    for k in range(top):
        rank = jnp.sum(jnp.where(hits[k], before, 0.0), axis=0, keepdims=True)
        here = slot_ids == local[k : k + 1, :] * cap + rank.astype(jnp.int32)
        pick = jnp.where(here, 1.0, pick)
        weighted = jnp.where(here, weights[k : k + 1, :], weighted)
    return pick.astype(bf16), jnp.sum(weighted, axis=1, keepdims=True)


def fused_kernel(n, cap, channel_total, names, *refs):
    r = dict(zip(names, refs))
    s, q = lax.axis_index("sp"), lax.axis_index("tp")
    q_core, q_y, q_far = partners(q)
    peers = (q_core, q_y, q_far)
    core, y = lax.rem(q, 2), q // 2
    z, x = s // 2, lax.rem(s, 2)
    sx = s + 1 - 2 * x
    nz = n // 2
    stream, cot = r["stream"], r["cot"]
    tokens, model_width = stream.shape
    width = r["ret"].shape[-1]
    top = r["routes"].shape[0]
    icols = r["gproj"].shape[0]
    pair = 2 * cap
    taps_count = r["taps"].shape[0]
    quarter, quarter_y = aligned(q * width, width), aligned(q_y * width, width)
    wg, wu, wd = r["wg"], r["wu"], r["wd"]
    full = (r["rows"], r["cots"])
    copies = []
    conditional = []

    loads = {}
    for i, name in enumerate(input_names):
        loads[name] = pltpu.make_async_copy(r[name + "_h"], r[name], r["load"].at[i])
        loads[name].start()

    def start(src, dst, key, index, sp, tp, recv=None):
        send, arrive = r["send_" + key], r["recv_" + key]
        copy = remote(src, dst, send.at[index], arrive.at[index if recv is None else recv], sp, tp)
        copy.start()
        copies.append(copy)
        return copy

    def start_if(cond, src, dst, key, index, sp, tp, recv):
        copy = remote(
            src, dst, r["send_" + key].at[index], r["recv_" + key].at[recv], sp, tp
        )
        pl.when(cond)(copy.start)
        conditional.append((cond, copy))

    def landed(dst, key, index):
        remote(dst, dst, r["send_" + key].at[index], r["recv_" + key].at[index], s, q).wait_recv()

    high = z // (nz // 2)
    folded = z + high * (nz - 1 - 2 * z)
    far_order = [1 - folded, 2 + 0 * z, 3 + 0 * z]
    source = [f + high * (nz - 1 - 2 * f) for f in far_order]
    chunk_z = [z] + source
    chunk_rows = [aligned(c * pair, pair) for c in chunk_z]

    def block_rows(block):
        return aligned(block * cap, cap)

    loads["routes"].wait()
    loads["weights"].wait()
    meta = r["meta"]
    routes_own, weights_own = r["routes"][...], r["weights"][...]
    meta[z] = jnp.concatenate(
        [routes_own.astype(f32), weights_own, jnp.zeros((8 - 2 * top, tokens), f32)], axis=0
    )
    greet(n, s, q, peers)
    meta_waits = [
        start(meta.at[z], meta.at[z], "m", d - 1, 2 * lax.rem(z + d, nz) + x, q)
        for d in range(1, nz)
    ]
    raw = r["raw"]
    values = (stream, cot)
    for a, name in enumerate(("stream", "cot")):
        loads[name].wait()
        src = values[a].at[:, quarter]
        start_if(z < nz - 1, src, raw.at[a, z], "zo", (a, 0), s + 2, q, (a, z))
        start_if(z > 0, src, raw.at[a, z], "zp", (a, 0), s - 2, q, (a, z))

    def landed_raw(a, j):
        dst = raw.at[a, source[j]]
        from_below = source[j] < z

        @pl.when(from_below)
        def _():
            landed(dst, "zo", (a, source[j]))

        @pl.when(source[j] > z)
        def _():
            landed(dst, "zp", (a, source[j]))

        start_if((source[j] < z) & (z < nz - 1), dst, dst, "zo", (a, j + 1), s + 2, q, (a, source[j]))
        start_if((source[j] > z) & (z > 0), dst, dst, "zp", (a, j + 1), s - 2, q, (a, source[j]))

    pick, slot_weight = slot_pick(routes_own, weights_own, 2 * z, pair, cap)
    ownbuf = r["ownbuf"]
    own_half, other_half = aligned(x * cap, cap), aligned((1 - x) * cap, cap)
    for a in range(2):
        got = dot(pick, values[a][...])
        ownbuf[a] = (got * slot_weight if a else got).astype(bf16)
        for i, cols in enumerate((quarter, quarter_y)):
            start(
                ownbuf.at[a, other_half, cols], full[a].at[block_rows(s), cols],
                "xo", (a, i), sx, q,
            )
    for a in range(2):
        full[a][block_rows(s), :] = ownbuf[a, own_half, :]
    r["pick"][...] = slot_pick(routes_own, weights_own, 0, n * cap, cap)[0]

    def exchange_stats(buffer, first, second, which):
        lanes = lax.broadcasted_iota(jnp.int32, (tokens, tokens), 1)
        packed = jnp.where(lanes == 0, first, jnp.where(lanes == 1, second, 0.0))
        buffer[3] = packed.T[0:8, :]
        return [
            start(buffer.at[3], buffer.at[p], "s", (which, p), s, peer)
            for p, peer in enumerate(peers)
        ]

    def summed_stats(buffer, waits):
        for w in waits:
            w.wait_recv()
        total = (buffer[3] + buffer[0]) + (buffer[1] + buffer[2])
        wide = jnp.concatenate([total, jnp.zeros((tokens - 8, tokens), f32)], axis=0).T
        return wide[:, 0:1], wide[:, 1:2]

    loads["conv"].wait()
    loads["gain"].wait()
    conv = r["conv"][...].astype(f32).T
    stat_waits = exchange_stats(
        r["stat"],
        jnp.sum(conv, axis=1, keepdims=True),
        jnp.sum(conv * conv, axis=1, keepdims=True),
        0,
    )
    for copy in meta_waits:
        copy.wait_recv()
    picks = []
    for j in range(nz - 1):
        there = meta[source[j]]
        picks.append(
            slot_pick(there[0:top].astype(jnp.int32), there[top : 2 * top], 2 * z, pair, cap)
        )
    pickbuf = r["pickbuf"]

    def arrive_raw(j, a):
        landed_raw(a, j)
        pick_j, weight_j = picks[j]
        got = dot(pick_j, raw[a, source[j]])
        pickbuf[a, j] = (got * weight_j if a else got).astype(bf16)
        rows = block_rows(2 * source[j] + x)
        mine, other = pickbuf.at[a, j, own_half], pickbuf.at[a, j, other_half]
        here = full[a].at[rows, quarter]
        start(other, here, "x", (a, j), sx, q)
        start(mine, here, "y", (a, j, 0), s, q_y)
        start(mine, here, "c", (a, j, 0), s, q_core)
        full[a][rows, quarter] = pickbuf[a, j, own_half]

    def arrive_x(j, a):
        here = full[a].at[block_rows(2 * source[j] + 1 - x), quarter]
        landed(here, "x", (a, j))
        start(here, here, "y", (a, j, 1), s, q_y)
        start(here, here, "c", (a, j, 1), s, q_core)

    def arrive_y(j, a):
        for i in range(2):
            here = full[a].at[block_rows(2 * source[j] + (x if i == 0 else 1 - x)), quarter_y]
            landed(here, "y", (a, j, i))
            start(here, here, "d", (a, j, i), s, q_core)

    def complete(j, a):
        for i in range(2):
            rows = block_rows(2 * source[j] + (x if i == 0 else 1 - x))
            for key, owner in (("c", q_core), ("d", q_far)):
                landed(full[a].at[rows, aligned(owner * width, width)], key, (a, j, i))

    def arrive_own(a):
        for i, cols in enumerate((quarter, quarter_y)):
            here = full[a].at[block_rows(sx), cols]
            landed(here, "xo", (a, i))
            start(here, here, "xc", (a, i), s, q_core)

    def complete_own(a):
        for i, owner in enumerate((q_core, q_far)):
            landed(full[a].at[block_rows(sx), aligned(owner * width, width)], "xc", (a, i))

    act_all, dg_all, du_all, part = r["act"], r["dg"], r["du"], r["part"]
    pre_gate_ref, pre_up_ref = r["pre_gate"], r["pre_up"]

    def first_half(k):
        rows = chunk_rows[k]
        if k:
            complete(k - 1, 0)
        else:
            complete_own(0)
            loads["wg"].wait()
            loads["wu"].wait()
        rows_in = full[0][rows, :]
        pre_gate_ref[...] = dot(rows_in, wg[...])
        pre_up_ref[...] = dot(rows_in, wu[...])

    def second_half(k):
        rows = chunk_rows[k]
        if k:
            complete(k - 1, 1)
        else:
            complete_own(1)
            loads["wd"].wait()
        grad_act = dot(full[1][rows, :], wd[...], 1, 1)
        pre_gate, pre_up = pre_gate_ref[...], pre_up_ref[...]
        glu_part = jnp.minimum(pre_gate, clamp_limit)
        lin_part = jnp.clip(pre_up, -clamp_limit, clamp_limit)
        sig_glu = jax.nn.sigmoid(alpha_gate * glu_part)
        act_all[rows, :] = (glu_part * sig_glu * (lin_part + 1.0)).astype(bf16)
        slope = sig_glu + alpha_gate * glu_part * sig_glu * (1.0 - sig_glu)
        dg = jnp.where(
            pre_gate < clamp_limit, grad_act * (lin_part + 1.0) * slope, 0.0
        ).astype(bf16)
        du = jnp.where(
            jnp.abs(pre_up) < clamp_limit, grad_act * glu_part * sig_glu, 0.0
        ).astype(bf16)
        dg_all[rows, :] = dg
        du_all[rows, :] = du
        part[rows, :] = (dot(dg, wg[...], 1, 1) + dot(du, wu[...], 1, 1)).astype(bf16)
        for h, half in ((0, 1 - y), (1, y)):
            start(
                part.at[rows, aligned((2 * half + 1 - core) * width, width)],
                r["from_core"].at[h, rows], "rc", (k, h), s, q_core,
            )

    def reduce_core(k):
        rows = chunk_rows[k]
        landed(r["from_core"].at[0, rows], "rc", (k, 0))
        r["to_y"][rows, :] = (
            part[rows, quarter_y].astype(f32) + r["from_core"][0, rows, :].astype(f32)
        ).astype(bf16)
        start(r["to_y"].at[rows], r["from_y"].at[rows], "ry", k, s, q_y)
        landed(r["from_core"].at[1, rows], "rc", (k, 1))
        r["own"][rows, :] = part[rows, quarter].astype(f32) + r["from_core"][
            1, rows, :
        ].astype(f32)

    ret = r["ret"]
    mine_slots = block_rows(s)

    def reduce_y(k):
        rows = chunk_rows[k]
        landed(r["from_y"].at[rows], "ry", k)
        r["to_xz"][rows, :] = (
            r["own"][rows, :] + r["from_y"][rows, :].astype(f32)
        ).astype(bf16)
        if k:
            for i in range(2):
                home = 2 * chunk_z[k] + i
                start(r["to_xz"].at[block_rows(home)], ret.at[mine_slots], "r", (k, i), home, q, (s, 0))
        else:
            start(r["to_xz"].at[block_rows(sx)], ret.at[mine_slots], "r", (0, 0), sx, q, (s, 0))
            ret[mine_slots, :] = r["to_xz"][mine_slots, :]

    hid_all = r["hid"]

    def hid_rows(block):
        return aligned(block * tokens, tokens)

    def relay_hidden(j):
        if j < 0:
            here = hid_all.at[hid_rows(s)]
            start_if(z < nz - 1, here, here, "ho", 0, s + 2, q, z)
            start_if(z > 0, here, here, "hp", 0, s - 2, q, z)
        else:
            here = hid_all.at[hid_rows(2 * source[j] + x)]

            @pl.when(source[j] < z)
            def _():
                landed(here, "ho", source[j])

            @pl.when(source[j] > z)
            def _():
                landed(here, "hp", source[j])

            start_if((source[j] < z) & (z < nz - 1), here, here, "ho", j + 1, s + 2, q, source[j])
            start_if((source[j] > z) & (z > 0), here, here, "hp", j + 1, s - 2, q, source[j])
        start(here, here, "hx", j + 1, sx, q)

    def weight_grad(left, right, out, by_left):
        tile = right.shape[1] if by_left else left.shape[1]

        def step(i, carry):
            there = aligned(i * tile, tile)
            if by_left:
                out[there, :] = dot(left[:, there], right[...], 0, 0).astype(bf16)
            else:
                out[:, there] = dot(left[...], right[:, there], 0, 0).astype(bf16)
            return carry

        lax.fori_loop(0, model_width // tile, step, 0)

    arrive_raw(0, 0)
    arrive_own(0)
    chan_sum, chan_sq = summed_stats(r["stat"], stat_waits)
    chan_mean = chan_sum / channel_total
    chan_var = chan_sq / channel_total - chan_mean * chan_mean
    inverse_deviation = lax.rsqrt(chan_var + norm_eps)
    mean_removed = (conv - chan_mean) * inverse_deviation
    gain = r["gain"][...]
    normed = mean_removed * gain
    sig = jax.nn.sigmoid(normed)
    hid_all[hid_rows(s), :] = (normed * sig).astype(bf16)
    r["slope"][...] = sig * (1.0 + normed * (1.0 - sig)) * gain
    r["removed"][...] = mean_removed
    r["inverse"][...] = jnp.broadcast_to(inverse_deviation, r["inverse"].shape)
    arrive_raw(0, 1)
    arrive_own(1)
    arrive_x(0, 0)
    first_half(0)
    arrive_raw(1, 0)
    arrive_y(0, 0)
    arrive_x(0, 1)
    second_half(0)
    arrive_raw(1, 1)
    arrive_y(0, 1)
    arrive_x(1, 0)
    first_half(1)
    arrive_raw(2, 0)
    arrive_y(1, 0)
    arrive_x(1, 1)
    second_half(1)
    arrive_raw(2, 1)
    relay_hidden(-1)
    arrive_y(1, 1)
    arrive_x(2, 0)
    reduce_core(0)
    first_half(2)
    arrive_x(2, 1)
    arrive_y(2, 0)
    second_half(2)
    reduce_core(1)
    arrive_y(2, 1)
    first_half(3)
    second_half(3)
    reduce_y(0)
    reduce_core(2)
    reduce_core(3)
    relay_hidden(0)
    reduce_y(1)
    weight_grad(r["act"], r["cots"], r["gdown"], False)
    reduce_y(2)
    relay_hidden(1)
    reduce_y(3)
    relay_hidden(2)
    weight_grad(r["rows"], r["dg"], r["ggate"], True)
    weight_grad(r["rows"], r["du"], r["gup"], True)

    for d in range(1, n):
        e = lax.rem(s + d, n)
        landed(ret.at[block_rows(e)], "r", (e, 0))
    gs_ref = r["gs"]
    combined = dot(r["pick"][...], ret[...], 0, 0) + cot[:, quarter].astype(f32)
    gs_ref[:, quarter] = combined.astype(bf16)
    mine_cols = gs_ref.at[:, quarter]
    by_core = start(mine_cols, mine_cols, "g", 0, s, q_core)
    by_y = start(mine_cols, mine_cols, "g", 1, s, q_y)
    loads["proj"].wait()
    proj = r["proj"]

    def partial_of(owner):
        cols = aligned(owner * width, width)
        return dot(gs_ref[:, cols], proj[cols, :])

    grad_hidden = partial_of(q)
    by_y.wait_recv()
    y_cols = gs_ref.at[:, quarter_y]
    by_far = start(y_cols, y_cols, "g", 2, s, q_core)
    grad_hidden = grad_hidden + partial_of(q_y)
    by_core.wait_recv()
    grad_hidden = grad_hidden + partial_of(q_core)
    by_far.wait_recv()
    grad_hidden = grad_hidden + partial_of(q_far)
    half_rows = tokens // 2
    part_rows = aligned(core * half_rows, half_rows)
    land = aligned(s * tokens + core * half_rows, half_rows)
    order = [lax.rem(s + d, n) for d in range(1, n)]
    col_all = r["col"]
    col_waits = [
        start(
            gs_ref.at[part_rows, aligned(order[j] * icols, icols)], col_all.at[land],
            "k", j, order[j], q,
        )
        for j in range(n - 1)
    ]
    col_all[hid_rows(s), :] = gs_ref[:, aligned(s * icols, icols)]
    mean_removed = r["removed"][...]
    inverse_deviation = r["inverse"][:, 0:1]
    norm_grad = grad_hidden * r["slope"][...]
    stat_waits = exchange_stats(
        r["stat2"],
        jnp.sum(norm_grad, axis=1, keepdims=True),
        jnp.sum(norm_grad * mean_removed, axis=1, keepdims=True),
        1,
    )
    avg, cross = summed_stats(r["stat2"], stat_waits)
    conv_grad = inverse_deviation * (
        norm_grad - avg / channel_total - mean_removed * (cross / channel_total)
    )
    ext = r["ext"]
    rim = ext.shape[0] - tokens
    ext[0:tokens, :] = conv_grad
    halo = remote(
        ext.at[0:rim], ext.at[tokens : tokens + rim], r["send_e"].at[0], r["recv_e"].at[0],
        lax.rem(s + n - 1, n), q,
    )
    halo.start()
    forwards = []
    for j in range(n - 1):
        col_waits[j].wait_recv()
        origin = lax.rem(s + n - (j + 1), n)
        there = col_all.at[aligned(origin * tokens + core * half_rows, half_rows)]
        forwards.append(start(there, there, "f", j, s, q_core))
    loads["taps"].wait()
    loads["gate"].wait()
    loads["value"].wait()
    halo.wait_recv()
    edge = ext[tokens : tokens + rim, :]
    halo.wait_send()
    ext[tokens : tokens + rim, :] = jnp.where(s == n - 1, 0.0, edge)
    acc = jnp.zeros((tokens, ext.shape[1]), f32)
    for tap in range(taps_count):
        acc = acc + r["taps"][tap : tap + 1, :] * ext[tap : tap + tokens, :]
    gated = acc.T
    gate_sig = jax.nn.sigmoid(r["gate"][...].astype(f32))
    r["gvalue"][...] = (gated * gate_sig).astype(bf16)
    r["ggin"][...] = (
        gated * r["value"][...].astype(f32) * gate_sig * (1.0 - gate_sig)
    ).astype(bf16)
    for copy in forwards:
        copy.wait_recv()
    for k in range(nz):
        landed(hid_all.at[hid_rows(2 * chunk_z[k] + 1 - x)], "hx", k)
    r["gproj"][...] = dot(col_all[...], hid_all[...], 0, 0)
    for copy in copies:
        copy.wait_send()
    for cond, copy in conditional:
        pl.when(cond)(copy.wait_send)


input_names = (
    "routes", "weights", "stream", "cot", "conv", "gain", "wg", "wu", "wd", "proj", "value",
    "gate", "taps",
)


def fused(
    routes, weights, stream, cot, wg, wu, wd, proj, value, gate, taps, conv, gain, n, cap, tp_count
):
    tokens, model_width = stream.shape
    hidden_width = wg.shape[1]
    width = model_width // tp_count
    channels = value.shape[0]
    icols = model_width // n
    slots = n * cap
    rim = -(-(taps.shape[0] - 1) // 8) * 8
    nz = n // 2
    V, dma = pltpu.VMEM, pltpu.SemaphoreType.DMA
    given = dict(
        routes=routes, weights=weights, stream=stream, cot=cot, conv=conv, gain=gain, wg=wg, wu=wu,
        wd=wd, proj=proj, value=value, gate=gate, taps=taps,
    )
    outs = dict(
        ggate=((model_width, hidden_width), bf16),
        gup=((model_width, hidden_width), bf16),
        gdown=((hidden_width, model_width), bf16),
        gs=((tokens, model_width), bf16),
        gproj=((icols, channels), f32),
        gvalue=((channels, tokens), bf16),
        ggin=((channels, tokens), bf16),
    )
    scratch = {name: V(given[name].shape, given[name].dtype) for name in input_names}
    scratch.update(
        meta=V((nz, 8, tokens), f32),
        raw=V((2, nz, tokens, width), bf16),
        ownbuf=V((2, 2 * cap, model_width), bf16),
        pickbuf=V((2, nz - 1, 2 * cap, width), bf16),
        pick=V((slots, tokens), bf16),
        rows=V((slots, model_width), bf16),
        cots=V((slots, model_width), bf16),
        act=V((slots, hidden_width), bf16),
        dg=V((slots, hidden_width), bf16),
        du=V((slots, hidden_width), bf16),
        part=V((slots, model_width), bf16),
        pre_gate=V((2 * cap, hidden_width), f32),
        pre_up=V((2 * cap, hidden_width), f32),
        from_core=V((2, slots, width), bf16),
        own=V((slots, width), f32),
        to_y=V((slots, width), bf16),
        from_y=V((slots, width), bf16),
        to_xz=V((slots, width), bf16),
        ret=V((slots, width), bf16),
        hid=V((n * tokens, channels), bf16),
        col=V((n * tokens, icols), bf16),
        slope=V((tokens, channels), f32),
        removed=V((tokens, channels), f32),
        inverse=V((tokens, tokens), f32),
        stat=V((4, 8, tokens), f32),
        stat2=V((4, 8, tokens), f32),
        ext=V((tokens + rim, channels), f32),
        load=dma((len(input_names),)),
    )
    sems = dict(
        m=(nz - 1,), zo=(2, nz), zp=(2, nz), xo=(2, 2), xc=(2, 2), x=(2, nz - 1), y=(2, nz - 1, 2),
        c=(2, nz - 1, 2), d=(2, nz - 1, 2), s=(2, 3), rc=(nz, 2), ry=(nz,), ho=(nz,), hp=(nz,),
        hx=(nz,), g=(3,), k=(n - 1,), f=(n - 1,), e=(1,), r=(n, 2),
    )
    for key, shape in sems.items():
        scratch["send_" + key] = dma(shape)
        scratch["recv_" + key] = dma(shape)
    names = [name + "_h" for name in input_names] + list(outs) + list(scratch)
    return pl.pallas_call(
        functools.partial(fused_kernel, n, cap, channels * tp_count, tuple(names)),
        out_shape=tuple(V(*o) for o in outs.values()),
        in_specs=[pl.BlockSpec(memory_space=pltpu.HBM)] * len(input_names),
        out_specs=[pl.BlockSpec(memory_space=V)] * len(outs),
        scratch_shapes=list(scratch.values()),
        compiler_params=pltpu.CompilerParams(
            collective_id=0, has_side_effects=True, vmem_limit_bytes=48 << 20
        ),
        name="fused",
    )(*[pltpu.with_memory_space_constraint(given[name], pltpu.HBM) for name in input_names])


def flush_kernel(*refs):
    count = len(refs) // 2
    copies = [
        pltpu.make_async_copy(refs[i], refs[count + i], refs[-1].at[i]) for i in range(count)
    ]
    for copy in copies:
        copy.start()
    for copy in copies:
        copy.wait()


def flush(*arrays):
    return pl.pallas_call(
        flush_kernel,
        out_shape=tuple(jax.ShapeDtypeStruct(a.shape, a.dtype) for a in arrays),
        in_specs=[pl.BlockSpec(memory_space=pltpu.VMEM)] * len(arrays),
        out_specs=[pl.BlockSpec(memory_space=pltpu.HBM)] * len(arrays),
        scratch_shapes=[pltpu.SemaphoreType.DMA((len(arrays),))],
        compiler_params=pltpu.CompilerParams(vmem_limit_bytes=4 << 20),
        name="flush",
    )(*arrays)


def body(
    stream_in, out_cot, route_experts, route_weights, w_gate, w_up, w_down, w_proj,
    conv_value, conv_gate, conv_taps, conv_result, channel_norm_gain,
):
    n = lax.axis_size("sp")
    tp_count = lax.axis_size("tp")
    experts = w_gate.shape[0] * n
    tokens, model_width = stream_in.shape
    cap = 2 * route_experts.shape[1] * tokens // experts
    outs = flush(
        *fused(
            route_experts.T, route_weights.T, stream_in, out_cot, w_gate[0], w_up[0], w_down[0],
            w_proj, conv_value, conv_gate, conv_taps, conv_result, channel_norm_gain[None, :],
            n, cap, tp_count,
        )
    )
    return (outs[0][None], outs[1][None], outs[2][None]) + tuple(outs[3:])


def from_behind(value, axis, steps):
    count = lax.axis_size(axis)
    leading, last = (max(0, -steps), min(count, count - steps))
    return lax.ppermute(value, axis, [(source, source + steps) for source in range(leading, last)])


def slot_tables(block_routes, experts_all, capacity):
    flat_routes = block_routes.reshape(-1)
    assigns = flat_routes.shape[0]
    onehot = (flat_routes[:, None] == jnp.arange(experts_all, dtype=jnp.int32)[None, :]).astype(
        jnp.int32
    )
    before = jnp.cumsum(onehot, axis=0) - onehot
    rank_in = jnp.sum(before * onehot, axis=1)
    slot_of = flat_routes * capacity + rank_in
    source_of = (
        jnp.full((experts_all * capacity,), -1, jnp.int32)
        .at[slot_of]
        .set(jnp.arange(assigns, dtype=jnp.int32))
    )
    return (slot_of, source_of)


def combine_routes(returned, slot_of, cot_cols, token_rows, top_count):
    feature_count = returned.shape[-1]
    flat_back = returned.reshape(-1, feature_count)
    per_route = flat_back[slot_of].astype(jnp.float32).reshape(token_rows, top_count, feature_count)
    return (cot_cols.astype(jnp.float32) + jnp.sum(per_route, axis=1)).astype(jnp.bfloat16)


def expert_terms_plain(rows_in, cot_in, w_gate, w_up, w_down):
    pre_gate = jnp.einsum("secd,edf->secf", rows_in, w_gate, preferred_element_type=jnp.float32)
    pre_up = jnp.einsum("secd,edf->secf", rows_in, w_up, preferred_element_type=jnp.float32)
    glu_part = jnp.minimum(pre_gate, clamp_limit)
    lin_part = jnp.clip(pre_up, -clamp_limit, clamp_limit)
    sig_glu = jax.nn.sigmoid(alpha_gate * glu_part)
    activated = (glu_part * sig_glu * (lin_part + 1.0)).astype(jnp.bfloat16)
    grad_act = jnp.einsum("secd,efd->secf", cot_in, w_down, preferred_element_type=jnp.float32)
    slope = sig_glu + alpha_gate * glu_part * sig_glu * (1.0 - sig_glu)
    grad_pre_gate = jnp.where(
        pre_gate < clamp_limit, grad_act * (lin_part + 1.0) * slope, 0.0
    ).astype(jnp.bfloat16)
    grad_pre_up = jnp.where(
        jnp.abs(pre_up) < clamp_limit, grad_act * glu_part * sig_glu, 0.0
    ).astype(jnp.bfloat16)
    grad_down = jnp.einsum(
        "secf,secd->efd", activated, cot_in, preferred_element_type=jnp.float32
    ).astype(jnp.bfloat16)
    grad_gate = jnp.einsum(
        "secd,secf->edf", rows_in, grad_pre_gate, preferred_element_type=jnp.float32
    ).astype(jnp.bfloat16)
    grad_up = jnp.einsum(
        "secd,secf->edf", rows_in, grad_pre_up, preferred_element_type=jnp.float32
    ).astype(jnp.bfloat16)
    input_part = jnp.einsum(
        "secf,edf->secd", grad_pre_gate, w_gate, preferred_element_type=jnp.float32
    )
    input_part = input_part + jnp.einsum(
        "secf,edf->secd", grad_pre_up, w_up, preferred_element_type=jnp.float32
    )
    return (grad_gate, grad_up, grad_down, input_part)


def body_plain(
    stream_in,
    out_cot,
    route_experts,
    route_weights,
    w_gate,
    w_up,
    w_down,
    w_proj,
    conv_value,
    conv_gate,
    conv_taps,
    conv_result,
    channel_norm_gain,
):
    sp_count = lax.axis_size("sp")
    tp_count = lax.axis_size("tp")
    local_experts = w_gate.shape[0]
    experts_all = local_experts * sp_count
    token_rows, model_width = stream_in.shape
    top_count = route_experts.shape[1]
    capacity = 2 * top_count * token_rows // experts_all
    slot_of, source_of = slot_tables(route_experts, experts_all, capacity)
    occupied = source_of >= 0
    source_safe = jnp.maximum(source_of, 0)
    token_of = source_safe // top_count
    slot_weight = jnp.where(occupied, route_weights.reshape(-1)[source_safe], 0.0)
    row_buffer = jnp.where(occupied[:, None], stream_in[token_of], jnp.zeros((), jnp.bfloat16))
    cot_buffer = (slot_weight[:, None] * out_cot[token_of].astype(jnp.float32)).astype(jnp.bfloat16)
    row_buffer = row_buffer.reshape(experts_all, capacity, model_width)
    cot_buffer = cot_buffer.reshape(experts_all, capacity, model_width)
    slice_width = model_width // tp_count
    slice_start = lax.axis_index("tp") * slice_width
    row_slice = lax.dynamic_slice_in_dim(row_buffer, slice_start, slice_width, 2)
    cot_slice = lax.dynamic_slice_in_dim(cot_buffer, slice_start, slice_width, 2)
    row_slice, cot_slice = (
        lax.all_to_all(row_slice, "sp", split_axis=0, concat_axis=0, tiled=True),
        lax.all_to_all(cot_slice, "sp", split_axis=0, concat_axis=0, tiled=True),
    )
    rows_in, cot_in = (
        lax.all_gather(row_slice, "tp", axis=2, tiled=True),
        lax.all_gather(cot_slice, "tp", axis=2, tiled=True),
    )
    rows_in = rows_in.reshape(sp_count, local_experts, capacity, model_width)
    cot_in = cot_in.reshape(sp_count, local_experts, capacity, model_width)
    grad_gate, grad_up, grad_down, input_part = expert_terms_plain(rows_in, cot_in, w_gate, w_up, w_down)
    shared = lax.psum_scatter(
        input_part.astype(jnp.bfloat16), "tp", scatter_dimension=3, tiled=True
    )
    returned = shared.reshape(experts_all, capacity, slice_width)
    returned = lax.all_to_all(returned, "sp", split_axis=0, concat_axis=0, tiled=True)
    cot_cols = lax.dynamic_slice_in_dim(out_cot, slice_start, slice_width, 1)
    stream_part = combine_routes(returned, slot_of, cot_cols, token_rows, top_count)
    grad_stream = lax.all_gather(stream_part, "tp", axis=1, tiled=True)
    channel_total = conv_result.shape[0] * tp_count
    positions = conv_result.shape[1]
    conv_float = conv_result.astype(jnp.float32)
    chan_sum, chan_sq = lax.psum(
        (jnp.sum(conv_float, axis=0), jnp.sum(conv_float * conv_float, axis=0)), "tp"
    )
    chan_mean = chan_sum / channel_total
    chan_var = chan_sq / channel_total - chan_mean * chan_mean
    inverse_deviation = lax.rsqrt(chan_var + norm_eps)
    mean_removed = (conv_float - chan_mean) * inverse_deviation
    normalized_rows = mean_removed * channel_norm_gain[:, None]
    sigmoid_of_norm = jax.nn.sigmoid(normalized_rows)
    hidden = (normalized_rows * sigmoid_of_norm).astype(jnp.bfloat16)
    grad_proj = lax.psum_scatter(
        lax.dot_general(
            grad_stream, hidden, (((0,), (1,)), ((), ())), preferred_element_type=jnp.float32
        ),
        "sp",
        scatter_dimension=0,
        tiled=True,
    )
    hidden_gradient = lax.dot_general(
        w_proj, grad_stream, (((0,), (1,)), ((), ())), preferred_element_type=jnp.float32
    )
    normed_input_gradient = (
        hidden_gradient
        * sigmoid_of_norm
        * (1.0 + normalized_rows * (1.0 - sigmoid_of_norm))
        * channel_norm_gain[:, None]
    )
    average_products, cross_products = lax.psum(
        (
            jnp.sum(normed_input_gradient, axis=0),
            jnp.sum(normed_input_gradient * mean_removed, axis=0),
        ),
        "tp",
    )
    conv_output_gradient = inverse_deviation * (
        normed_input_gradient
        - average_products / channel_total
        - mean_removed * (cross_products / channel_total)
    )
    taps_count = conv_taps.shape[0]
    next_rim = from_behind(conv_output_gradient[:, : taps_count - 1], "sp", -1)
    extended = jnp.concatenate([conv_output_gradient, next_rim], axis=1)
    grad_gated = jnp.zeros_like(conv_output_gradient)
    for tap_index in range(taps_count):
        grad_gated = (
            grad_gated
            + conv_taps[tap_index][:, None] * extended[:, tap_index : tap_index + positions]
        )
    gate_sig = jax.nn.sigmoid(conv_gate.astype(jnp.float32))
    grad_value = (grad_gated * gate_sig).astype(jnp.bfloat16)
    grad_gate_in = (
        grad_gated * conv_value.astype(jnp.float32) * gate_sig * (1.0 - gate_sig)
    ).astype(jnp.bfloat16)
    return (grad_gate, grad_up, grad_down, grad_stream, grad_proj, grad_value, grad_gate_in)


def solution(mesh):
    return jax.shard_map(
        body if (mesh.shape["sp"], mesh.shape["tp"]) == (8, 4) else body_plain,
        mesh=mesh,
        in_specs=(
            P("sp", None),
            P("sp", None),
            P("sp", None),
            P("sp", None),
            P("sp", None, "tp"),
            P("sp", None, "tp"),
            P("sp", "tp", None),
            P(None, "tp"),
            P("tp", "sp"),
            P("tp", "sp"),
            P(None, "tp"),
            P("tp", "sp"),
            P("tp"),
        ),
        out_specs=(
            P("sp", None, "tp"),
            P("sp", None, "tp"),
            P("sp", "tp", None),
            P("sp", None),
            P("sp", "tp"),
            P("tp", "sp"),
            P("tp", "sp"),
        ),
        check_vma=False,
    )
```

```python
import functools

import jax
import jax.numpy as jnp
from jax import lax
from jax.experimental import pallas as pl
from jax.experimental.pallas import tpu as pltpu
from jax.sharding import PartitionSpec as P

norm_eps = 1e-05
clamp_limit = 7.0
alpha_gate = 1.702
MESH = pl.DeviceIdType.MESH
f32 = jnp.float32
bf16 = jnp.bfloat16


def dot(a, b, ca=1, cb=0):
    return lax.dot_general(a, b, (((ca,), (cb,)), ((), ())), preferred_element_type=f32)


def aligned(start, size):
    return pl.ds(pl.multiple_of(start, size), size)


def greet(n, s, q, tp_peers, ahead):
    barrier = pltpu.get_barrier_semaphore()
    for d in range(1, n):
        pl.semaphore_signal(
            barrier, inc=1, device_id={"sp": lax.rem(s + d, n), "tp": q}, device_id_type=MESH
        )
    for peer in tp_peers:
        for sp in (s, ahead):
            pl.semaphore_signal(
                barrier, inc=1, device_id={"sp": sp, "tp": peer}, device_id_type=MESH
            )
    pl.semaphore_wait(barrier, n - 1 + 2 * len(tp_peers))


def remote(src, dst, send, recv, sp, tp):
    return pltpu.make_async_remote_copy(
        src_ref=src,
        dst_ref=dst,
        send_sem=send,
        recv_sem=recv,
        device_id={"sp": sp, "tp": tp},
        device_id_type=MESH,
    )


def partners(q):
    core, other = lax.rem(q, 2), q // 2
    return (2 * other + 1 - core, 2 * (1 - other) + core, 2 * (1 - other) + 1 - core)


def slot_pick(routes, weights, first, slots, cap):
    top, tokens = routes.shape
    local = routes - first
    expert_ids = lax.broadcasted_iota(jnp.int32, (8, tokens), 0)
    hits = [expert_ids == local[k : k + 1, :] for k in range(top)]
    count = sum(h.astype(f32) for h in hits)
    earlier = (
        lax.broadcasted_iota(jnp.int32, (tokens, tokens), 0)
        < lax.broadcasted_iota(jnp.int32, (tokens, tokens), 1)
    ).astype(f32)
    before = dot(count.astype(bf16), earlier.astype(bf16))
    slot_ids = lax.broadcasted_iota(jnp.int32, (slots, tokens), 0)
    pick = jnp.zeros((slots, tokens), f32)
    weighted = jnp.zeros((slots, tokens), f32)
    for k in range(top):
        rank = jnp.sum(jnp.where(hits[k], before, 0.0), axis=0, keepdims=True)
        here = slot_ids == local[k : k + 1, :] * cap + rank.astype(jnp.int32)
        pick = jnp.where(here, 1.0, pick)
        weighted = jnp.where(here, weights[k : k + 1, :], weighted)
    return pick.astype(bf16), jnp.sum(weighted, axis=1, keepdims=True)


def fused_kernel(n, cap, channel_total, names, *refs):
    r = dict(zip(names, refs))
    s, q = lax.axis_index("sp"), lax.axis_index("tp")
    q_core, q_y, q_far = partners(q)
    peers = (q_core, q_y, q_far)
    core, y = lax.rem(q, 2), q // 2
    z, x = s // 2, lax.rem(s, 2)
    sx = s + 1 - 2 * x
    nz = n // 2
    stream, cot = r["stream"], r["cot"]
    tokens, model_width = stream.shape
    width = r["ret"].shape[-1]
    top = r["routes"].shape[0]
    icols = r["gproj"].shape[0]
    pair = 2 * cap
    taps_count = r["taps"].shape[0]
    quarter, quarter_y = aligned(q * width, width), aligned(q_y * width, width)
    wg, wu, wd = r["wg"], r["wu"], r["wd"]
    full = (r["rows"], r["cots"])
    copies = []
    conditional = []

    loads = {}
    for i, name in enumerate(input_names):
        loads[name] = pltpu.make_async_copy(r[name + "_h"], r[name], r["load"].at[i])
        loads[name].start()

    def start(src, dst, key, index, sp, tp, recv=None, keep=True):
        send, arrive = r["send_" + key], r["recv_" + key]
        copy = remote(src, dst, send.at[index], arrive.at[index if recv is None else recv], sp, tp)
        copy.start()
        if keep:
            copies.append(copy)
        return copy

    def sent(like, key, index):
        remote(like, like, r["send_" + key].at[index], r["recv_" + key].at[index], s, q).wait_send()

    def start_if(cond, src, dst, key, index, sp, tp, recv):
        copy = remote(
            src, dst, r["send_" + key].at[index], r["recv_" + key].at[recv], sp, tp
        )
        pl.when(cond)(copy.start)
        conditional.append((cond, copy))

    def landed(dst, key, index):
        remote(dst, dst, r["send_" + key].at[index], r["recv_" + key].at[index], s, q).wait_recv()

    high = z // (nz // 2)
    folded = z + high * (nz - 1 - 2 * z)
    middle, at_end = folded == 1, folded == 0

    def unfold(f):
        return f + high * (nz - 1 - 2 * f)

    source = [
        unfold((1 - folded) * (j + 1) + folded * mid) for j, mid in enumerate((2, 0, 3))
    ]
    chunks_end = [z] + source
    chunks_mid = source + [z]

    def block_rows(block):
        return aligned(block * cap, cap)

    loads["routes"].wait()
    loads["weights"].wait()
    meta = r["meta"]
    routes_own, weights_own = r["routes"][...], r["weights"][...]
    meta[z] = jnp.concatenate(
        [routes_own.astype(f32), weights_own, jnp.zeros((8 - 2 * top, tokens), f32)], axis=0
    )
    behind, ahead = lax.rem(s + n - 1, n), lax.rem(s + 1, n)
    greet(n, s, q, peers, ahead)
    for d in range(1, nz):
        start(meta.at[z], meta.at[z], "m", d - 1, 2 * lax.rem(z + d, nz) + x, q, z)
    raw = r["raw"]
    values = (stream, cot)
    for a, name in enumerate(("stream", "cot")):
        loads[name].wait()
        src = values[a].at[:, quarter]
        start_if(z < nz - 1, src, raw.at[a, z], "z", (a, 0), s + 2, q, (a, z))
        start_if(z > 0, src, raw.at[a, z], "z", (a, 1), s - 2, q, (a, z))

    middle = (z > 0) & (z < nz - 1)

    def onward(j):
        return 2 * z - source[1] if j == 1 else source[1]

    def relay_raw(j, a):
        dst = raw.at[a, source[j]]
        landed(dst, "z", (a, source[j]))
        start(dst, dst, "z", (a, j + 2), 2 * onward(j) + x, q, (a, source[j]), keep=False)

    pick, slot_weight = slot_pick(routes_own, weights_own, 2 * z, pair, cap)
    ownbuf = r["ownbuf"]
    own_half, other_half = aligned(x * cap, cap), aligned((1 - x) * cap, cap)

    def send_own(a):
        got = dot(pick, values[a][...])
        ownbuf[a] = (got * slot_weight if a else got).astype(bf16)
        for i, cols in enumerate((quarter, quarter_y)):
            start(
                ownbuf.at[a, other_half, cols], full[a].at[block_rows(s), cols],
                "xo", (a, i), sx, q, keep=False,
            )
        full[a][block_rows(s), :] = ownbuf[a, own_half, :]

    send_own(0)
    r["pick"][...] = slot_pick(routes_own, weights_own, 0, n * cap, cap)[0]

    def exchange_stats(buffer, first, second, which):
        lanes = lax.broadcasted_iota(jnp.int32, (tokens, tokens), 1)
        packed = jnp.where(lanes == 0, first, jnp.where(lanes == 1, second, 0.0))
        buffer[3] = packed.T[0:8, :]
        return [
            start(buffer.at[3], buffer.at[p], "s", (which, p), s, peer)
            for p, peer in enumerate(peers)
        ]

    def totals(total):
        wide = jnp.concatenate([total, jnp.zeros((tokens - 8, tokens), f32)], axis=0).T
        return wide[:, 0:1], wide[:, 1:2]

    def summed_stats(buffer, waits):
        for w in waits:
            w.wait_recv()
        return totals((buffer[3] + buffer[0]) + (buffer[1] + buffer[2]))

    loads["conv"].wait()
    loads["gain"].wait()
    conv = r["conv"][...].astype(f32).T
    stat_waits = exchange_stats(
        r["stat"],
        jnp.sum(conv, axis=1, keepdims=True),
        jnp.sum(conv * conv, axis=1, keepdims=True),
        0,
    )
    pick_all, weight_all = r["picks"], r["slot_weights"]

    def pick_for(j):
        landed(meta.at[source[j]], "m", source[j])
        there = meta[source[j]]
        pick_j, weight_j = slot_pick(
            there[0:top].astype(jnp.int32), there[top : 2 * top], 2 * z, pair, cap
        )
        pick_all[j] = pick_j
        weight_all[j] = jnp.broadcast_to(weight_j, weight_all.shape[1:])

    pickbuf = r["pickbuf"]

    def take_raw(j, a):
        got = dot(pick_all[j], raw[a, source[j]])
        pickbuf[a, j] = (got * weight_all[j][:, 0:1] if a else got).astype(bf16)
        rows = block_rows(2 * source[j] + x)
        mine, other = pickbuf.at[a, j, own_half], pickbuf.at[a, j, other_half]
        here = full[a].at[rows, quarter]
        start(other, here, "x", (a, j), sx, q, keep=False)
        start(mine, here, "y", (a, j, 0), s, q_y, keep=False)
        start(mine, here, "c", (a, j, 0), s, q_core, keep=False)
        full[a][rows, quarter] = pickbuf[a, j, own_half]

    def arrive_raw(j, a):
        landed(raw.at[a, source[j]], "z", (a, source[j]))
        take_raw(j, a)

    def arrive_x(j, a):
        here = full[a].at[block_rows(2 * source[j] + 1 - x), quarter]
        landed(here, "x", (a, j))
        start(here, here, "y", (a, j, 1), s, q_y, keep=False)
        start(here, here, "c", (a, j, 1), s, q_core, keep=False)

    def arrive_y(j, a, i):
        here = full[a].at[block_rows(2 * source[j] + (x if i == 0 else 1 - x)), quarter_y]
        landed(here, "y", (a, j, i))
        start(here, here, "d", (a, j, i), s, q_core, keep=False)

    def complete(j, a):
        for i in range(2):
            rows = block_rows(2 * source[j] + (x if i == 0 else 1 - x))
            for key, owner in (("c", q_core), ("d", q_far)):
                landed(full[a].at[rows, aligned(owner * width, width)], key, (a, j, i))

    def arrive_own(a):
        for i, cols in enumerate((quarter, quarter_y)):
            here = full[a].at[block_rows(sx), cols]
            landed(here, "xo", (a, i))
            start(here, here, "xc", (a, i), s, q_core, keep=False)

    def complete_own(a):
        for i, owner in enumerate((q_core, q_far)):
            landed(full[a].at[block_rows(sx), aligned(owner * width, width)], "xc", (a, i))

    act_all, dg_all, du_all, part = r["act"], r["dg"], r["du"], r["part"]
    pre_gate_ref, pre_up_ref = r["pre_gate"], r["pre_up"]

    chunks = chunks_end

    def block_of(k, i):
        if chunks[k] is z:
            return s if i else sx
        return 2 * chunks[k] + i

    def chunk_of(k):
        return aligned(chunks[k] * pair, pair)

    def ready(k, a):
        if chunks[k] is z:
            complete_own(a)
        else:
            complete(k - 1 if chunks is chunks_end else k, a)

    def first_half(k):
        ready(k, 0)
        rows_in = full[0][chunk_of(k), :]
        pre_gate_ref[k] = dot(rows_in, wg[...])
        pre_up_ref[k] = dot(rows_in, wu[...])

    def second_half(k):
        ready(k, 1)
        rows = chunk_of(k)
        grad_act = dot(full[1][rows, :], wd[...], 1, 1)
        pre_gate, pre_up = pre_gate_ref[k], pre_up_ref[k]
        glu_part = jnp.minimum(pre_gate, clamp_limit)
        lin_part = jnp.clip(pre_up, -clamp_limit, clamp_limit)
        sig_glu = jax.nn.sigmoid(alpha_gate * glu_part)
        act_all[rows, :] = (glu_part * sig_glu * (lin_part + 1.0)).astype(bf16)
        slope = sig_glu + alpha_gate * glu_part * sig_glu * (1.0 - sig_glu)
        dg = jnp.where(
            pre_gate < clamp_limit, grad_act * (lin_part + 1.0) * slope, 0.0
        ).astype(bf16)
        du = jnp.where(
            jnp.abs(pre_up) < clamp_limit, grad_act * glu_part * sig_glu, 0.0
        ).astype(bf16)
        dg_all[rows, :] = dg
        du_all[rows, :] = du

    def input_grad(k, h):
        rows = chunk_of(k)
        half = y if h else 1 - y
        there = aligned(half * 2 * width, 2 * width)
        part[rows, there] = (
            dot(dg_all[rows, :], wg[there, :], 1, 1) + dot(du_all[rows, :], wu[there, :], 1, 1)
        ).astype(bf16)
        start(
            part.at[rows, aligned((2 * half + 1 - core) * width, width)],
            r["from_core"].at[h, rows], "rc", (k, h), s, q_core, keep=False,
        )

    def reduce_core(k, *parts):
        if 1 not in parts:
            landed(r["from_core"].at[0, chunk_of(k)], "rc", (k, 0))
        for i in parts or (0, 1):
            some = block_rows(block_of(k, i))
            r["to_y"][some, :] = (
                part[some, quarter_y].astype(f32) + r["from_core"][0, some, :].astype(f32)
            ).astype(bf16)
            start(
                r["to_y"].at[some], r["from_y"].at[some], "ry", (k, i), s, q_y, keep=False
            )

    ret = r["ret"]
    mine_slots = block_rows(s)

    def reduce_y(k):
        landed(r["from_core"].at[1, chunk_of(k)], "rc", (k, 1))
        for i in range(2):
            home = block_of(k, i)
            some = block_rows(home)
            landed(r["from_y"].at[some], "ry", (k, i))
            r["to_xz"][some, :] = (
                part[some, quarter].astype(f32)
                + r["from_core"][1, some, :].astype(f32)
                + r["from_y"][some, :].astype(f32)
            ).astype(bf16)
            if chunks[k] is z and i:
                ret[mine_slots, :] = r["to_xz"][mine_slots, :]
            else:
                send_home(home)

    def send_home(home):
        start(
            r["to_xz"].at[block_rows(home)], ret.at[mine_slots], "r", home, home, q, s, keep=False
        )

    hid_all = r["hid"]

    def hid_rows(block):
        return aligned(block * tokens, tokens)

    def send_hidden():
        here = hid_all.at[hid_rows(s)]
        start_if(z < nz - 1, here, here, "h", 0, s + 2, q, z)
        start_if(z > 0, here, here, "h", 1, s - 2, q, z)

    rim = r["rim_grad"].shape[0]

    def send_rim():
        for i, name in enumerate(("removed", "inverse")):
            start(r[name].at[0:rim], r["rim_" + name], "e", i, behind, q, keep=False)

    def relay_hidden(j):
        here = hid_all.at[hid_rows(2 * source[j] + x)]
        landed(here, "h", source[j])
        start(here, here, "h", j + 2, 2 * onward(j) + x, q, source[j], keep=False)

    def cross_hidden(k):
        here = hid_all.at[hid_rows(2 * chunks_end[k] + x)]
        start(here, here, "hx", k, sx, q, keep=False)

    def arrive_hidden(j):
        landed(hid_all.at[hid_rows(2 * source[j] + x)], "h", source[j])
        cross_hidden(j + 1)

    def weight_grad(left, right, out, by_left, part_of):
        tile = right.shape[1] if by_left else left.shape[1]
        steps = model_width // tile // 2

        def step(i, carry):
            there = aligned((part_of * steps + i) * tile, tile)
            if by_left:
                out[there, :] = dot(left[:, there], right[...], 0, 0).astype(bf16)
            else:
                out[:, there] = dot(left[...], right[:, there], 0, 0).astype(bf16)
            return carry

        lax.fori_loop(0, steps, step, 0)

    def grad_of(which, part_of):
        if which == "down":
            weight_grad(r["act"], r["cots"], r["gdown"], False, part_of)
        else:
            weight_grad(r["rows"], r["dg" if which == "gate" else "du"], r["g" + which], True, part_of)

    chan_sum, chan_sq = summed_stats(r["stat"], stat_waits)
    chan_mean = chan_sum / channel_total
    chan_var = chan_sq / channel_total - chan_mean * chan_mean
    inverse_deviation = lax.rsqrt(chan_var + norm_eps)
    mean_removed = (conv - chan_mean) * inverse_deviation
    gain = r["gain"][...]
    normed = mean_removed * gain
    sig = jax.nn.sigmoid(normed)
    hid_all[hid_rows(s), :] = (normed * sig).astype(bf16)
    r["slope"][...] = sig * (1.0 + normed * (1.0 - sig)) * gain
    r["removed"][...] = mean_removed
    r["inverse"][...] = jnp.broadcast_to(inverse_deviation, r["inverse"].shape)
    send_hidden()
    for name in ("wg", "wu", "wd"):
        loads[name].wait()

    def end_sequence():
        pick_for(0)
        arrive_raw(0, 0)
        send_own(1)
        arrive_own(0)
        pick_for(1)
        pick_for(2)
        arrive_raw(0, 1)
        arrive_x(0, 0)
        arrive_y(0, 0, 0)
        first_half(0)
        arrive_raw(1, 0)
        arrive_own(1)
        arrive_y(0, 1, 0)
        arrive_x(0, 1)
        arrive_y(0, 0, 1)
        arrive_raw(1, 1)
        second_half(0)
        arrive_x(1, 0)
        arrive_y(1, 0, 0)
        input_grad(0, 0)
        send_rim()
        arrive_y(0, 1, 1)
        arrive_raw(2, 0)
        first_half(1)
        arrive_x(1, 1)
        arrive_y(1, 1, 0)
        arrive_y(1, 0, 1)
        arrive_raw(2, 1)
        second_half(1)
        cross_hidden(0)
        arrive_x(2, 0)
        arrive_y(2, 0, 0)
        input_grad(1, 0)
        arrive_hidden(0)
        arrive_y(1, 1, 1)
        arrive_x(2, 1)
        first_half(2)
        arrive_y(2, 0, 1)
        arrive_y(2, 1, 0)
        reduce_core(1)
        second_half(2)
        input_grad(2, 0)
        input_grad(1, 1)
        reduce_core(2)
        reduce_core(0, 0)
        first_half(3)
        arrive_y(2, 1, 1)
        arrive_hidden(1)
        reduce_y(1)
        second_half(3)
        input_grad(3, 0)
        input_grad(2, 1)
        reduce_core(3)
        reduce_core(0, 1)
        reduce_y(2)
        input_grad(3, 1)
        grad_of("down", 0)
        input_grad(0, 1)
        grad_of("down", 1)
        reduce_y(3)
        reduce_y(0)
        arrive_hidden(2)

    def mid_sequence():
        pick_for(0)
        pick_for(1)
        relay_raw(0, 0)
        relay_raw(1, 0)
        take_raw(0, 0)
        take_raw(1, 0)
        pick_for(2)
        relay_raw(0, 1)
        relay_raw(1, 1)
        take_raw(0, 1)
        take_raw(1, 1)
        send_own(1)
        arrive_own(0)
        arrive_x(0, 0)
        arrive_x(1, 0)
        arrive_y(0, 0, 0)
        relay_raw(2, 0)
        take_raw(2, 0)
        arrive_y(1, 0, 0)
        arrive_x(0, 1)
        arrive_x(1, 1)
        arrive_y(0, 1, 0)
        relay_raw(2, 1)
        take_raw(2, 1)
        send_rim()
        arrive_y(1, 1, 0)
        arrive_y(0, 0, 1)
        relay_hidden(0)
        relay_hidden(1)
        arrive_own(1)
        arrive_y(1, 0, 1)
        arrive_x(2, 0)
        first_half(0)
        arrive_y(2, 0, 0)
        arrive_x(2, 1)
        first_half(1)
        arrive_y(0, 1, 1)
        cross_hidden(0)
        cross_hidden(1)
        cross_hidden(2)
        second_half(0)
        arrive_y(1, 1, 1)
        arrive_y(2, 1, 0)
        input_grad(0, 0)
        relay_hidden(2)
        cross_hidden(3)
        second_half(1)
        reduce_core(0)
        input_grad(1, 0)
        input_grad(0, 1)
        arrive_y(2, 0, 1)
        first_half(2)
        reduce_core(1)
        arrive_y(2, 1, 1)
        input_grad(1, 1)
        second_half(2)
        input_grad(2, 0)
        reduce_y(0)
        input_grad(2, 1)
        reduce_core(2)
        first_half(3)
        second_half(3)
        reduce_y(1)
        input_grad(3, 0)
        input_grad(3, 1)
        reduce_core(3)
        reduce_y(2)
        grad_of("down", 0)
        grad_of("down", 1)
        reduce_y(3)

    chunks = chunks_end
    pl.when(at_end)(end_sequence)
    chunks = chunks_mid
    pl.when(middle)(mid_sequence)
    grad_of("gate", 0)
    grad_of("gate", 1)

    for d in range(1, n):
        e = lax.rem(s + d, n)
        landed(ret.at[block_rows(e)], "r", e)
    gs_ref = r["gs"]
    combined = dot(r["pick"][...], ret[...], 0, 0) + cot[:, quarter].astype(f32)
    gs_ref[:, quarter] = combined.astype(bf16)
    mine_cols = gs_ref.at[:, quarter]
    by_core = start(mine_cols, mine_cols, "g", 0, s, q_core)
    by_y = start(mine_cols, mine_cols, "g", 1, s, q_y)
    col_all = r["col"]
    holder, relay = q == z, q_y == z
    for i in range(2):
        target = 2 * q + i
        start_if(
            target != s, gs_ref.at[:, aligned(target * icols, icols)], col_all.at[hid_rows(s)],
            "k", i, target, q, s,
        )
    blocks = [sx]
    for j in range(nz - 1):
        blocks += [2 * source[j] + x, 2 * source[j] + 1 - x]

    def pass_cols(block):
        there = col_all.at[hid_rows(block)]

        @pl.when(holder)
        def _():
            landed(there, "k", block)
            start(there, there, "fy", block, s, q_y, keep=False)
            start(there, there, "fc", block, s, q_core, keep=False)

    def relay_cols(block):
        there = col_all.at[hid_rows(block)]

        @pl.when(relay)
        def _():
            landed(there, "fy", block)
            start(there, there, "fc", block, s, q_core, keep=False)

    loads["proj"].wait()
    proj = r["proj"]

    def partial_of(owner):
        cols = aligned(owner * width, width)
        return dot(gs_ref[:, cols], proj[cols, :])

    grad_of("up", 0)
    grad_of("up", 1)
    grad_hidden = partial_of(q)
    by_y.wait_recv()
    y_cols = gs_ref.at[:, quarter_y]
    by_far = start(y_cols, y_cols, "g", 2, s, q_core)
    grad_hidden = grad_hidden + partial_of(q_y)
    pass_cols(blocks[0])
    pass_cols(blocks[1])
    by_core.wait_recv()
    grad_hidden = grad_hidden + partial_of(q_core)
    pass_cols(blocks[2])
    by_far.wait_recv()
    grad_hidden = grad_hidden + partial_of(q_far)
    norm_grad = grad_hidden * r["slope"][...]
    mean_removed = r["removed"][...]
    inverse_deviation = r["inverse"][:, 0:1]
    norm_grad_ref = r["norm_grad"]
    norm_grad_ref[...] = norm_grad
    start(norm_grad_ref.at[0:rim], r["rim_grad"], "e", 2, behind, q)
    stat_waits = exchange_stats(
        r["stat2"],
        jnp.sum(norm_grad, axis=1, keepdims=True),
        jnp.sum(norm_grad * mean_removed, axis=1, keepdims=True),
        1,
    )
    rim_stat = r["rim_stat"]
    for p, peer in enumerate((q,) + peers):
        start(r["stat2"].at[3], rim_stat.at[q], "t", p, behind, peer, q)
    col_all[hid_rows(s), :] = gs_ref[:, aligned(s * icols, icols)]
    for block in blocks[3:5]:
        pass_cols(block)
    for block in blocks[:2]:
        relay_cols(block)
    avg, cross = summed_stats(r["stat2"], stat_waits)
    ext = r["ext"]

    def conv_grad_of(inverse, grad, removed, avg, cross):
        return inverse * (grad - avg / channel_total - removed * (cross / channel_total))

    ext[0:tokens, :] = conv_grad_of(inverse_deviation, norm_grad, mean_removed, avg, cross)
    for block in blocks[5:]:
        pass_cols(block)
    for block in blocks[2:4]:
        relay_cols(block)
    for i, name in enumerate(("removed", "inverse", "grad")):
        landed(r["rim_" + name], "e", i)
    for owner in range(1 + len(peers)):
        landed(rim_stat.at[owner], "t", owner)
    avg, cross = totals((rim_stat[0] + rim_stat[1]) + (rim_stat[2] + rim_stat[3]))
    edge = conv_grad_of(
        r["rim_inverse"][:, 0:1], r["rim_grad"][...], r["rim_removed"][...], avg[0:rim],
        cross[0:rim],
    )
    ext[tokens : tokens + rim, :] = jnp.where(s == n - 1, 0.0, edge)
    relay_cols(blocks[4])
    loads["taps"].wait()
    loads["gate"].wait()
    loads["value"].wait()
    acc = jnp.zeros((tokens, ext.shape[1]), f32)
    for tap in range(taps_count):
        acc = acc + r["taps"][tap : tap + 1, :] * ext[tap : tap + tokens, :]
    gated = acc.T
    gate_sig = jax.nn.sigmoid(r["gate"][...].astype(f32))
    r["gvalue"][...] = (gated * gate_sig).astype(bf16)
    r["ggin"][...] = (
        gated * r["value"][...].astype(f32) * gate_sig * (1.0 - gate_sig)
    ).astype(bf16)
    for block in blocks[5:]:
        relay_cols(block)

    @pl.when(jnp.logical_not(holder | relay))
    def _():
        for block in blocks:
            landed(col_all.at[hid_rows(block)], "fc", block)

    for k in range(nz):
        landed(hid_all.at[hid_rows(2 * chunks_end[k] + 1 - x)], "hx", k)
    r["gproj"][...] = dot(col_all[...], hid_all[...], 0, 0)
    for copy in copies:
        copy.wait_send()
    piece, half_chunk = full[0].at[0:cap, 0:width], part.at[0:pair, 0:width]
    raw_piece, hid_piece = raw.at[0, 0], hid_all.at[hid_rows(0)]
    for a in range(2):
        for i in range(2):
            sent(piece, "xo", (a, i))
            sent(piece, "xc", (a, i))
        for j in range(nz - 1):
            sent(piece, "x", (a, j))
            for key in ("y", "c", "d"):
                for i in range(2):
                    sent(piece, key, (a, j, i))
    for k in range(nz):
        sent(hid_piece, "hx", k)
        for i in range(2):
            sent(half_chunk, "rc", (k, i))
            sent(piece, "ry", (k, i))
    for d in range(1, n):
        sent(piece, "r", lax.rem(s + d, n))
    for i, name in enumerate(("removed", "inverse")):
        sent(r["rim_" + name], "e", i)

    @pl.when(middle)
    def _():
        for j in range(nz - 1):
            sent(hid_piece, "h", j + 2)
            for a in range(2):
                sent(raw_piece, "z", (a, j + 2))

    for cond, copy in conditional:
        pl.when(cond)(copy.wait_send)
    block_cols = col_all.at[hid_rows(0)]
    for block in blocks:

        @pl.when(holder)
        def _():
            sent(block_cols, "fy", block)

        @pl.when(holder | relay)
        def _():
            sent(block_cols, "fc", block)


input_names = (
    "routes", "weights", "stream", "cot", "conv", "gain", "wg", "wu", "wd", "proj", "value",
    "gate", "taps",
)


def fused(
    routes, weights, stream, cot, wg, wu, wd, proj, value, gate, taps, conv, gain, n, cap, tp_count
):
    tokens, model_width = stream.shape
    hidden_width = wg.shape[1]
    width = model_width // tp_count
    channels = value.shape[0]
    icols = model_width // n
    slots = n * cap
    rim = -(-(taps.shape[0] - 1) // 8) * 8
    nz = n // 2
    V, dma = pltpu.VMEM, pltpu.SemaphoreType.DMA
    given = dict(
        routes=routes, weights=weights, stream=stream, cot=cot, conv=conv, gain=gain, wg=wg, wu=wu,
        wd=wd, proj=proj, value=value, gate=gate, taps=taps,
    )
    outs = dict(
        ggate=((model_width, hidden_width), bf16),
        gup=((model_width, hidden_width), bf16),
        gdown=((hidden_width, model_width), bf16),
        gs=((tokens, model_width), bf16),
        gproj=((icols, channels), f32),
        gvalue=((channels, tokens), bf16),
        ggin=((channels, tokens), bf16),
    )
    scratch = {name: V(given[name].shape, given[name].dtype) for name in input_names}
    scratch.update(
        meta=V((nz, 8, tokens), f32),
        raw=V((2, nz, tokens, width), bf16),
        ownbuf=V((2, 2 * cap, model_width), bf16),
        pickbuf=V((2, nz - 1, 2 * cap, width), bf16),
        pick=V((slots, tokens), bf16),
        picks=V((nz - 1, 2 * cap, tokens), bf16),
        slot_weights=V((nz - 1, 2 * cap, tokens), f32),
        rows=V((slots, model_width), bf16),
        cots=V((slots, model_width), bf16),
        act=V((slots, hidden_width), bf16),
        dg=V((slots, hidden_width), bf16),
        du=V((slots, hidden_width), bf16),
        part=V((slots, model_width), bf16),
        pre_gate=V((nz, 2 * cap, hidden_width), f32),
        pre_up=V((nz, 2 * cap, hidden_width), f32),
        from_core=V((2, slots, width), bf16),
        to_y=V((slots, width), bf16),
        from_y=V((slots, width), bf16),
        to_xz=V((slots, width), bf16),
        ret=V((slots, width), bf16),
        hid=V((n * tokens, channels), bf16),
        col=V((n * tokens, icols), bf16),
        slope=V((tokens, channels), f32),
        removed=V((tokens, channels), f32),
        inverse=V((tokens, tokens), f32),
        stat=V((4, 8, tokens), f32),
        stat2=V((4, 8, tokens), f32),
        norm_grad=V((tokens, channels), f32),
        rim_removed=V((rim, channels), f32),
        rim_inverse=V((rim, tokens), f32),
        rim_grad=V((rim, channels), f32),
        rim_stat=V((tp_count, 8, tokens), f32),
        ext=V((tokens + rim, channels), f32),
        load=dma((len(input_names),)),
    )
    sems = dict(
        m=(nz,), z=(2, nz + 1), xo=(2, 2), xc=(2, 2), x=(2, nz - 1), y=(2, nz - 1, 2),
        c=(2, nz - 1, 2), d=(2, nz - 1, 2), s=(2, 3), rc=(nz, 2), ry=(nz, 2), h=(nz + 1,),
        hx=(nz,), g=(3,), k=(n,), fy=(n,), fc=(n,), e=(3,), t=(tp_count,), r=(n,),
    )
    for key, shape in sems.items():
        scratch["send_" + key] = dma(shape)
        scratch["recv_" + key] = dma(shape)
    names = [name + "_h" for name in input_names] + list(outs) + list(scratch)
    return pl.pallas_call(
        functools.partial(fused_kernel, n, cap, channels * tp_count, tuple(names)),
        out_shape=tuple(V(*o) for o in outs.values()),
        in_specs=[pl.BlockSpec(memory_space=pltpu.HBM)] * len(input_names),
        out_specs=[pl.BlockSpec(memory_space=V)] * len(outs),
        scratch_shapes=list(scratch.values()),
        compiler_params=pltpu.CompilerParams(
            collective_id=0, has_side_effects=True, vmem_limit_bytes=48 << 20
        ),
        name="fused",
    )(*[pltpu.with_memory_space_constraint(given[name], pltpu.HBM) for name in input_names])


def flush_kernel(*refs):
    count = len(refs) // 2
    copies = [
        pltpu.make_async_copy(refs[i], refs[count + i], refs[-1].at[i]) for i in range(count)
    ]
    for copy in copies:
        copy.start()
    for copy in copies:
        copy.wait()


def flush(*arrays):
    return pl.pallas_call(
        flush_kernel,
        out_shape=tuple(jax.ShapeDtypeStruct(a.shape, a.dtype) for a in arrays),
        in_specs=[pl.BlockSpec(memory_space=pltpu.VMEM)] * len(arrays),
        out_specs=[pl.BlockSpec(memory_space=pltpu.HBM)] * len(arrays),
        scratch_shapes=[pltpu.SemaphoreType.DMA((len(arrays),))],
        compiler_params=pltpu.CompilerParams(vmem_limit_bytes=4 << 20),
        name="flush",
    )(*arrays)


def body(
    stream_in, out_cot, route_experts, route_weights, w_gate, w_up, w_down, w_proj,
    conv_value, conv_gate, conv_taps, conv_result, channel_norm_gain,
):
    n = lax.axis_size("sp")
    tp_count = lax.axis_size("tp")
    experts = w_gate.shape[0] * n
    tokens, model_width = stream_in.shape
    cap = 2 * route_experts.shape[1] * tokens // experts
    outs = flush(
        *fused(
            route_experts.T, route_weights.T, stream_in, out_cot, w_gate[0], w_up[0], w_down[0],
            w_proj, conv_value, conv_gate, conv_taps, conv_result, channel_norm_gain[None, :],
            n, cap, tp_count,
        )
    )
    return (outs[0][None], outs[1][None], outs[2][None]) + tuple(outs[3:])


def from_behind(value, axis, steps):
    count = lax.axis_size(axis)
    leading, last = (max(0, -steps), min(count, count - steps))
    return lax.ppermute(value, axis, [(source, source + steps) for source in range(leading, last)])


def slot_tables(block_routes, experts_all, capacity):
    flat_routes = block_routes.reshape(-1)
    assigns = flat_routes.shape[0]
    onehot = (flat_routes[:, None] == jnp.arange(experts_all, dtype=jnp.int32)[None, :]).astype(
        jnp.int32
    )
    before = jnp.cumsum(onehot, axis=0) - onehot
    rank_in = jnp.sum(before * onehot, axis=1)
    slot_of = flat_routes * capacity + rank_in
    source_of = (
        jnp.full((experts_all * capacity,), -1, jnp.int32)
        .at[slot_of]
        .set(jnp.arange(assigns, dtype=jnp.int32))
    )
    return (slot_of, source_of)


def combine_routes(returned, slot_of, cot_cols, token_rows, top_count):
    feature_count = returned.shape[-1]
    flat_back = returned.reshape(-1, feature_count)
    per_route = flat_back[slot_of].astype(jnp.float32).reshape(token_rows, top_count, feature_count)
    return (cot_cols.astype(jnp.float32) + jnp.sum(per_route, axis=1)).astype(jnp.bfloat16)


def expert_terms_plain(rows_in, cot_in, w_gate, w_up, w_down):
    pre_gate = jnp.einsum("secd,edf->secf", rows_in, w_gate, preferred_element_type=jnp.float32)
    pre_up = jnp.einsum("secd,edf->secf", rows_in, w_up, preferred_element_type=jnp.float32)
    glu_part = jnp.minimum(pre_gate, clamp_limit)
    lin_part = jnp.clip(pre_up, -clamp_limit, clamp_limit)
    sig_glu = jax.nn.sigmoid(alpha_gate * glu_part)
    activated = (glu_part * sig_glu * (lin_part + 1.0)).astype(jnp.bfloat16)
    grad_act = jnp.einsum("secd,efd->secf", cot_in, w_down, preferred_element_type=jnp.float32)
    slope = sig_glu + alpha_gate * glu_part * sig_glu * (1.0 - sig_glu)
    grad_pre_gate = jnp.where(
        pre_gate < clamp_limit, grad_act * (lin_part + 1.0) * slope, 0.0
    ).astype(jnp.bfloat16)
    grad_pre_up = jnp.where(
        jnp.abs(pre_up) < clamp_limit, grad_act * glu_part * sig_glu, 0.0
    ).astype(jnp.bfloat16)
    grad_down = jnp.einsum(
        "secf,secd->efd", activated, cot_in, preferred_element_type=jnp.float32
    ).astype(jnp.bfloat16)
    grad_gate = jnp.einsum(
        "secd,secf->edf", rows_in, grad_pre_gate, preferred_element_type=jnp.float32
    ).astype(jnp.bfloat16)
    grad_up = jnp.einsum(
        "secd,secf->edf", rows_in, grad_pre_up, preferred_element_type=jnp.float32
    ).astype(jnp.bfloat16)
    input_part = jnp.einsum(
        "secf,edf->secd", grad_pre_gate, w_gate, preferred_element_type=jnp.float32
    )
    input_part = input_part + jnp.einsum(
        "secf,edf->secd", grad_pre_up, w_up, preferred_element_type=jnp.float32
    )
    return (grad_gate, grad_up, grad_down, input_part)


def body_plain(
    stream_in,
    out_cot,
    route_experts,
    route_weights,
    w_gate,
    w_up,
    w_down,
    w_proj,
    conv_value,
    conv_gate,
    conv_taps,
    conv_result,
    channel_norm_gain,
):
    sp_count = lax.axis_size("sp")
    tp_count = lax.axis_size("tp")
    local_experts = w_gate.shape[0]
    experts_all = local_experts * sp_count
    token_rows, model_width = stream_in.shape
    top_count = route_experts.shape[1]
    capacity = 2 * top_count * token_rows // experts_all
    slot_of, source_of = slot_tables(route_experts, experts_all, capacity)
    occupied = source_of >= 0
    source_safe = jnp.maximum(source_of, 0)
    token_of = source_safe // top_count
    slot_weight = jnp.where(occupied, route_weights.reshape(-1)[source_safe], 0.0)
    row_buffer = jnp.where(occupied[:, None], stream_in[token_of], jnp.zeros((), jnp.bfloat16))
    cot_buffer = (slot_weight[:, None] * out_cot[token_of].astype(jnp.float32)).astype(jnp.bfloat16)
    row_buffer = row_buffer.reshape(experts_all, capacity, model_width)
    cot_buffer = cot_buffer.reshape(experts_all, capacity, model_width)
    slice_width = model_width // tp_count
    slice_start = lax.axis_index("tp") * slice_width
    row_slice = lax.dynamic_slice_in_dim(row_buffer, slice_start, slice_width, 2)
    cot_slice = lax.dynamic_slice_in_dim(cot_buffer, slice_start, slice_width, 2)
    row_slice, cot_slice = (
        lax.all_to_all(row_slice, "sp", split_axis=0, concat_axis=0, tiled=True),
        lax.all_to_all(cot_slice, "sp", split_axis=0, concat_axis=0, tiled=True),
    )
    rows_in, cot_in = (
        lax.all_gather(row_slice, "tp", axis=2, tiled=True),
        lax.all_gather(cot_slice, "tp", axis=2, tiled=True),
    )
    rows_in = rows_in.reshape(sp_count, local_experts, capacity, model_width)
    cot_in = cot_in.reshape(sp_count, local_experts, capacity, model_width)
    grad_gate, grad_up, grad_down, input_part = expert_terms_plain(rows_in, cot_in, w_gate, w_up, w_down)
    shared = lax.psum_scatter(
        input_part.astype(jnp.bfloat16), "tp", scatter_dimension=3, tiled=True
    )
    returned = shared.reshape(experts_all, capacity, slice_width)
    returned = lax.all_to_all(returned, "sp", split_axis=0, concat_axis=0, tiled=True)
    cot_cols = lax.dynamic_slice_in_dim(out_cot, slice_start, slice_width, 1)
    stream_part = combine_routes(returned, slot_of, cot_cols, token_rows, top_count)
    grad_stream = lax.all_gather(stream_part, "tp", axis=1, tiled=True)
    channel_total = conv_result.shape[0] * tp_count
    positions = conv_result.shape[1]
    conv_float = conv_result.astype(jnp.float32)
    chan_sum, chan_sq = lax.psum(
        (jnp.sum(conv_float, axis=0), jnp.sum(conv_float * conv_float, axis=0)), "tp"
    )
    chan_mean = chan_sum / channel_total
    chan_var = chan_sq / channel_total - chan_mean * chan_mean
    inverse_deviation = lax.rsqrt(chan_var + norm_eps)
    mean_removed = (conv_float - chan_mean) * inverse_deviation
    normalized_rows = mean_removed * channel_norm_gain[:, None]
    sigmoid_of_norm = jax.nn.sigmoid(normalized_rows)
    hidden = (normalized_rows * sigmoid_of_norm).astype(jnp.bfloat16)
    grad_proj = lax.psum_scatter(
        lax.dot_general(
            grad_stream, hidden, (((0,), (1,)), ((), ())), preferred_element_type=jnp.float32
        ),
        "sp",
        scatter_dimension=0,
        tiled=True,
    )
    hidden_gradient = lax.dot_general(
        w_proj, grad_stream, (((0,), (1,)), ((), ())), preferred_element_type=jnp.float32
    )
    normed_input_gradient = (
        hidden_gradient
        * sigmoid_of_norm
        * (1.0 + normalized_rows * (1.0 - sigmoid_of_norm))
        * channel_norm_gain[:, None]
    )
    average_products, cross_products = lax.psum(
        (
            jnp.sum(normed_input_gradient, axis=0),
            jnp.sum(normed_input_gradient * mean_removed, axis=0),
        ),
        "tp",
    )
    conv_output_gradient = inverse_deviation * (
        normed_input_gradient
        - average_products / channel_total
        - mean_removed * (cross_products / channel_total)
    )
    taps_count = conv_taps.shape[0]
    next_rim = from_behind(conv_output_gradient[:, : taps_count - 1], "sp", -1)
    extended = jnp.concatenate([conv_output_gradient, next_rim], axis=1)
    grad_gated = jnp.zeros_like(conv_output_gradient)
    for tap_index in range(taps_count):
        grad_gated = (
            grad_gated
            + conv_taps[tap_index][:, None] * extended[:, tap_index : tap_index + positions]
        )
    gate_sig = jax.nn.sigmoid(conv_gate.astype(jnp.float32))
    grad_value = (grad_gated * gate_sig).astype(jnp.bfloat16)
    grad_gate_in = (
        grad_gated * conv_value.astype(jnp.float32) * gate_sig * (1.0 - gate_sig)
    ).astype(jnp.bfloat16)
    return (grad_gate, grad_up, grad_down, grad_stream, grad_proj, grad_value, grad_gate_in)


def solution(mesh):
    return jax.shard_map(
        body if (mesh.shape["sp"], mesh.shape["tp"]) == (8, 4) else body_plain,
        mesh=mesh,
        in_specs=(
            P("sp", None),
            P("sp", None),
            P("sp", None),
            P("sp", None),
            P("sp", None, "tp"),
            P("sp", None, "tp"),
            P("sp", "tp", None),
            P(None, "tp"),
            P("tp", "sp"),
            P("tp", "sp"),
            P(None, "tp"),
            P("tp", "sp"),
            P("tp"),
        ),
        out_specs=(
            P("sp", None, "tp"),
            P("sp", None, "tp"),
            P("sp", "tp", None),
            P("sp", None),
            P("sp", "tp"),
            P("tp", "sp"),
            P("tp", "sp"),
        ),
        check_vma=False,
    )
```

```python
import functools

import jax
import jax.numpy as jnp
from jax import lax
from jax.experimental import pallas as pl
from jax.experimental.pallas import tpu as pltpu
from jax.sharding import PartitionSpec as P

norm_eps = 1e-05
clamp_limit = 7.0
alpha_gate = 1.702
MESH = pl.DeviceIdType.MESH
f32 = jnp.float32
bf16 = jnp.bfloat16


def dot(a, b, ca=1, cb=0):
    return lax.dot_general(a, b, (((ca,), (cb,)), ((), ())), preferred_element_type=f32)


def aligned(start, size):
    return pl.ds(pl.multiple_of(start, size), size)


def greet(n, s, q, tp_peers, ahead):
    barrier = pltpu.get_barrier_semaphore()
    for d in range(1, n):
        pl.semaphore_signal(
            barrier, inc=1, device_id={"sp": lax.rem(s + d, n), "tp": q}, device_id_type=MESH
        )
    for peer in tp_peers:
        for sp in (s, ahead):
            pl.semaphore_signal(
                barrier, inc=1, device_id={"sp": sp, "tp": peer}, device_id_type=MESH
            )
    pl.semaphore_wait(barrier, n - 1 + 2 * len(tp_peers))


def remote(src, dst, send, recv, sp, tp):
    return pltpu.make_async_remote_copy(
        src_ref=src,
        dst_ref=dst,
        send_sem=send,
        recv_sem=recv,
        device_id={"sp": sp, "tp": tp},
        device_id_type=MESH,
    )


def partners(q):
    core, other = lax.rem(q, 2), q // 2
    return (2 * other + 1 - core, 2 * (1 - other) + core, 2 * (1 - other) + 1 - core)


def slot_pick(routes, weights, first, slots, cap):
    top, tokens = routes.shape
    local = routes - first
    expert_ids = lax.broadcasted_iota(jnp.int32, (8, tokens), 0)
    hits = [expert_ids == local[k : k + 1, :] for k in range(top)]
    count = sum(h.astype(f32) for h in hits)
    earlier = (
        lax.broadcasted_iota(jnp.int32, (tokens, tokens), 0)
        < lax.broadcasted_iota(jnp.int32, (tokens, tokens), 1)
    ).astype(f32)
    before = dot(count.astype(bf16), earlier.astype(bf16))
    slot_ids = lax.broadcasted_iota(jnp.int32, (slots, tokens), 0)
    pick = jnp.zeros((slots, tokens), f32)
    weighted = jnp.zeros((slots, tokens), f32)
    for k in range(top):
        rank = jnp.sum(jnp.where(hits[k], before, 0.0), axis=0, keepdims=True)
        here = slot_ids == local[k : k + 1, :] * cap + rank.astype(jnp.int32)
        pick = jnp.where(here, 1.0, pick)
        weighted = jnp.where(here, weights[k : k + 1, :], weighted)
    return pick.astype(bf16), jnp.sum(weighted, axis=1, keepdims=True)


def fused_kernel(n, cap, channel_total, names, *refs):
    r = dict(zip(names, refs))
    s, q = lax.axis_index("sp"), lax.axis_index("tp")
    q_core, q_y, q_far = partners(q)
    peers = (q_core, q_y, q_far)
    core, y = lax.rem(q, 2), q // 2
    z, x = s // 2, lax.rem(s, 2)
    sx = s + 1 - 2 * x
    nz = n // 2
    stream, cot = r["stream"], r["cot"]
    tokens, model_width = stream.shape
    width = r["ret"].shape[-1]
    top = r["routes"].shape[0]
    icols = r["col"].shape[1]
    pair = 2 * cap
    quarter, quarter_y = aligned(q * width, width), aligned(q_y * width, width)
    wg, wu, wd = r["wg"], r["wu"], r["wd"]
    full = (r["rows"], r["cots"])
    copies = []
    conditional = []

    loads = {}
    for i, name in enumerate(input_names):
        loads[name] = pltpu.make_async_copy(r[name + "_h"], r[name], r["load"].at[i])
        loads[name].start()

    def start(src, dst, key, index, sp, tp, recv=None, keep=True):
        send, arrive = r["send_" + key], r["recv_" + key]
        copy = remote(src, dst, send.at[index], arrive.at[index if recv is None else recv], sp, tp)
        copy.start()
        if keep:
            copies.append(copy)
        return copy

    def sent(like, key, index):
        remote(like, like, r["send_" + key].at[index], r["recv_" + key].at[index], s, q).wait_send()

    def start_if(cond, src, dst, key, index, sp, tp, recv):
        copy = remote(
            src, dst, r["send_" + key].at[index], r["recv_" + key].at[recv], sp, tp
        )
        pl.when(cond)(copy.start)
        conditional.append((cond, copy))

    def landed(dst, key, index):
        remote(dst, dst, r["send_" + key].at[index], r["recv_" + key].at[index], s, q).wait_recv()

    high = z // (nz // 2)
    folded = z + high * (nz - 1 - 2 * z)
    middle, at_end = folded == 1, folded == 0

    def unfold(f):
        return f + high * (nz - 1 - 2 * f)

    source = [
        unfold((1 - folded) * (j + 1) + folded * mid) for j, mid in enumerate((2, 0, 3))
    ]
    chunks_end = [z] + source
    chunks_mid = source + [z]

    def block_rows(block):
        return aligned(block * cap, cap)

    loads["routes"].wait()
    loads["weights"].wait()
    meta = r["meta"]
    routes_own, weights_own = r["routes"][...], r["weights"][...]
    meta[z] = jnp.concatenate(
        [routes_own.astype(f32), weights_own, jnp.zeros((8 - 2 * top, tokens), f32)], axis=0
    )
    behind, ahead = lax.rem(s + n - 1, n), lax.rem(s + 1, n)
    greet(n, s, q, peers, ahead)
    for d in range(1, nz):
        start(meta.at[z], meta.at[z], "m", d - 1, 2 * lax.rem(z + d, nz) + x, q, z)
    raw = r["raw"]
    values = (stream, cot)
    for a, name in enumerate(("stream", "cot")):
        loads[name].wait()
        src = values[a].at[:, quarter]
        start_if(z < nz - 1, src, raw.at[a, z], "z", (a, 0), s + 2, q, (a, z))
        start_if(z > 0, src, raw.at[a, z], "z", (a, 1), s - 2, q, (a, z))

    middle = (z > 0) & (z < nz - 1)

    def onward(j):
        return 2 * z - source[1] if j == 1 else source[1]

    def relay_raw(j, a):
        dst = raw.at[a, source[j]]
        landed(dst, "z", (a, source[j]))
        start(dst, dst, "z", (a, j + 2), 2 * onward(j) + x, q, (a, source[j]), keep=False)

    pick, slot_weight = slot_pick(routes_own, weights_own, 2 * z, pair, cap)
    ownbuf = r["ownbuf"]
    own_half, other_half = aligned(x * cap, cap), aligned((1 - x) * cap, cap)

    def send_own(a):
        got = dot(pick, values[a][...])
        ownbuf[a] = (got * slot_weight if a else got).astype(bf16)
        for i, cols in enumerate((quarter, quarter_y)):
            start(
                ownbuf.at[a, other_half, cols], full[a].at[block_rows(s), cols],
                "xo", (a, i), sx, q, keep=False,
            )
        full[a][block_rows(s), :] = ownbuf[a, own_half, :]

    send_own(0)
    r["pick"][...] = slot_pick(routes_own, weights_own, 0, n * cap, cap)[0]

    def exchange_stats(buffer, first, second, which):
        lanes = lax.broadcasted_iota(jnp.int32, (tokens, tokens), 1)
        packed = jnp.where(lanes == 0, first, jnp.where(lanes == 1, second, 0.0))
        buffer[3] = packed.T[0:8, :]
        return [
            start(buffer.at[3], buffer.at[p], "s", (which, p), s, peer)
            for p, peer in enumerate(peers)
        ]

    def totals(total):
        wide = jnp.concatenate([total, jnp.zeros((tokens - 8, tokens), f32)], axis=0).T
        return wide[:, 0:1], wide[:, 1:2]

    def summed_stats(buffer, waits):
        for w in waits:
            w.wait_recv()
        return totals((buffer[3] + buffer[0]) + (buffer[1] + buffer[2]))

    loads["conv"].wait()
    loads["gain"].wait()
    conv = r["conv"][...].astype(f32).T
    stat_waits = exchange_stats(
        r["stat"],
        jnp.sum(conv, axis=1, keepdims=True),
        jnp.sum(conv * conv, axis=1, keepdims=True),
        0,
    )
    pick_all, weight_all = r["picks"], r["slot_weights"]

    def pick_for(j):
        landed(meta.at[source[j]], "m", source[j])
        there = meta[source[j]]
        pick_j, weight_j = slot_pick(
            there[0:top].astype(jnp.int32), there[top : 2 * top], 2 * z, pair, cap
        )
        pick_all[j] = pick_j
        weight_all[j] = jnp.broadcast_to(weight_j, weight_all.shape[1:])

    pickbuf = r["pickbuf"]

    def take_raw(j, a):
        got = dot(pick_all[j], raw[a, source[j]])
        pickbuf[a, j] = (got * weight_all[j][:, 0:1] if a else got).astype(bf16)
        rows = block_rows(2 * source[j] + x)
        mine, other = pickbuf.at[a, j, own_half], pickbuf.at[a, j, other_half]
        here = full[a].at[rows, quarter]
        start(other, here, "x", (a, j), sx, q, keep=False)
        start(mine, here, "y", (a, j, 0), s, q_y, keep=False)
        start(mine, here, "c", (a, j, 0), s, q_core, keep=False)
        full[a][rows, quarter] = pickbuf[a, j, own_half]

    def arrive_raw(j, a):
        landed(raw.at[a, source[j]], "z", (a, source[j]))
        take_raw(j, a)

    def arrive_x(j, a):
        here = full[a].at[block_rows(2 * source[j] + 1 - x), quarter]
        landed(here, "x", (a, j))
        start(here, here, "y", (a, j, 1), s, q_y, keep=False)
        start(here, here, "c", (a, j, 1), s, q_core, keep=False)

    def arrive_y(j, a, i):
        here = full[a].at[block_rows(2 * source[j] + (x if i == 0 else 1 - x)), quarter_y]
        landed(here, "y", (a, j, i))
        start(here, here, "d", (a, j, i), s, q_core, keep=False)

    def complete(j, a):
        for i in range(2):
            rows = block_rows(2 * source[j] + (x if i == 0 else 1 - x))
            for key, owner in (("c", q_core), ("d", q_far)):
                landed(full[a].at[rows, aligned(owner * width, width)], key, (a, j, i))

    def arrive_own(a):
        for i, cols in enumerate((quarter, quarter_y)):
            here = full[a].at[block_rows(sx), cols]
            landed(here, "xo", (a, i))
            start(here, here, "xc", (a, i), s, q_core, keep=False)

    def complete_own(a):
        for i, owner in enumerate((q_core, q_far)):
            landed(full[a].at[block_rows(sx), aligned(owner * width, width)], "xc", (a, i))

    act_all, dg_all, du_all, part = r["act"], r["dg"], r["du"], r["part"]
    pre_gate_ref, pre_up_ref = r["pre_gate"], r["pre_up"]

    chunks = chunks_end

    def block_of(k, i):
        if chunks[k] is z:
            return s if i else sx
        return 2 * chunks[k] + i

    def chunk_of(k):
        return aligned(chunks[k] * pair, pair)

    def ready(k, a):
        if chunks[k] is z:
            complete_own(a)
        else:
            complete(k - 1 if chunks is chunks_end else k, a)

    def first_half(k):
        ready(k, 0)
        rows_in = full[0][chunk_of(k), :]
        pre_gate_ref[k] = dot(rows_in, wg[...])
        pre_up_ref[k] = dot(rows_in, wu[...])

    def second_half(k):
        ready(k, 1)
        rows = chunk_of(k)
        grad_act = dot(full[1][rows, :], wd[...], 1, 1)
        pre_gate, pre_up = pre_gate_ref[k], pre_up_ref[k]
        glu_part = jnp.minimum(pre_gate, clamp_limit)
        lin_part = jnp.clip(pre_up, -clamp_limit, clamp_limit)
        sig_glu = jax.nn.sigmoid(alpha_gate * glu_part)
        act_all[rows, :] = (glu_part * sig_glu * (lin_part + 1.0)).astype(bf16)
        slope = sig_glu + alpha_gate * glu_part * sig_glu * (1.0 - sig_glu)
        dg = jnp.where(
            pre_gate < clamp_limit, grad_act * (lin_part + 1.0) * slope, 0.0
        ).astype(bf16)
        du = jnp.where(
            jnp.abs(pre_up) < clamp_limit, grad_act * glu_part * sig_glu, 0.0
        ).astype(bf16)
        dg_all[rows, :] = dg
        du_all[rows, :] = du

    def input_grad(k, h):
        rows = chunk_of(k)
        half = y if h else 1 - y
        there = aligned(half * 2 * width, 2 * width)
        part[rows, there] = (
            dot(dg_all[rows, :], wg[there, :], 1, 1) + dot(du_all[rows, :], wu[there, :], 1, 1)
        ).astype(bf16)
        start(
            part.at[rows, aligned((2 * half + 1 - core) * width, width)],
            r["from_core"].at[h, rows], "rc", (k, h), s, q_core, keep=False,
        )

    def reduce_core(k, *parts):
        if 1 not in parts:
            landed(r["from_core"].at[0, chunk_of(k)], "rc", (k, 0))
        for i in parts or (0, 1):
            some = block_rows(block_of(k, i))
            r["to_y"][some, :] = (
                part[some, quarter_y].astype(f32) + r["from_core"][0, some, :].astype(f32)
            ).astype(bf16)
            start(
                r["to_y"].at[some], r["from_y"].at[some], "ry", (k, i), s, q_y, keep=False
            )

    ret = r["ret"]
    mine_slots = block_rows(s)

    def reduce_y(k):
        landed(r["from_core"].at[1, chunk_of(k)], "rc", (k, 1))
        for i in range(2):
            home = block_of(k, i)
            some = block_rows(home)
            landed(r["from_y"].at[some], "ry", (k, i))
            r["to_xz"][some, :] = (
                part[some, quarter].astype(f32)
                + r["from_core"][1, some, :].astype(f32)
                + r["from_y"][some, :].astype(f32)
            ).astype(bf16)
            if chunks[k] is z and i:
                ret[mine_slots, :] = r["to_xz"][mine_slots, :]
            else:
                send_home(home)

    def send_home(home):
        start(
            r["to_xz"].at[block_rows(home)], ret.at[mine_slots], "r", home, home, q, s, keep=False
        )

    hid_all = r["hid"]

    def hid_rows(block):
        return aligned(block * tokens, tokens)

    def send_hidden():
        here = hid_all.at[hid_rows(s)]
        start_if(z < nz - 1, here, here, "h", 0, s + 2, q, z)
        start_if(z > 0, here, here, "h", 1, s - 2, q, z)

    rim = r["rim_grad"].shape[0]

    def send_rim():
        for i, name in enumerate(("removed", "inverse")):
            start(r[name].at[0:rim], r["rim_" + name], "e", i, behind, q, keep=False)

    def relay_hidden(j):
        here = hid_all.at[hid_rows(2 * source[j] + x)]
        landed(here, "h", source[j])
        start(here, here, "h", j + 2, 2 * onward(j) + x, q, source[j], keep=False)

    def cross_hidden(k):
        here = hid_all.at[hid_rows(2 * chunks_end[k] + x)]
        start(here, here, "hx", k, sx, q, keep=False)

    def arrive_hidden(j):
        landed(hid_all.at[hid_rows(2 * source[j] + x)], "h", source[j])
        cross_hidden(j + 1)

    def weight_grad(left, right, out, by_left, part_of):
        tile = right.shape[1] if by_left else left.shape[1]
        steps = model_width // tile // 2

        def step(i, carry):
            there = aligned((part_of * steps + i) * tile, tile)
            if by_left:
                out[there, :] = dot(left[:, there], right[...], 0, 0).astype(bf16)
            else:
                out[:, there] = dot(left[...], right[:, there], 0, 0).astype(bf16)
            return carry

        lax.fori_loop(0, steps, step, 0)

    def grad_of(which, part_of):
        if which == "down":
            weight_grad(r["act"], r["cots"], r["gdown"], False, part_of)
        else:
            weight_grad(r["rows"], r["dg" if which == "gate" else "du"], r["g" + which], True, part_of)

    chan_sum, chan_sq = summed_stats(r["stat"], stat_waits)
    chan_mean = chan_sum / channel_total
    chan_var = chan_sq / channel_total - chan_mean * chan_mean
    inverse_deviation = lax.rsqrt(chan_var + norm_eps)
    mean_removed = (conv - chan_mean) * inverse_deviation
    gain = r["gain"][...]
    normed = mean_removed * gain
    sig = jax.nn.sigmoid(normed)
    hid_all[hid_rows(s), :] = (normed * sig).astype(bf16)
    r["slope"][...] = sig * (1.0 + normed * (1.0 - sig)) * gain
    r["removed"][...] = mean_removed
    r["inverse"][...] = jnp.broadcast_to(inverse_deviation, r["inverse"].shape)
    send_hidden()
    for name in ("wg", "wu", "wd"):
        loads[name].wait()

    def end_sequence():
        pick_for(0)
        arrive_raw(0, 0)
        send_own(1)
        arrive_own(0)
        pick_for(1)
        pick_for(2)
        arrive_raw(0, 1)
        arrive_x(0, 0)
        arrive_y(0, 0, 0)
        first_half(0)
        arrive_raw(1, 0)
        arrive_own(1)
        arrive_y(0, 1, 0)
        arrive_x(0, 1)
        arrive_y(0, 0, 1)
        arrive_raw(1, 1)
        second_half(0)
        arrive_x(1, 0)
        arrive_y(1, 0, 0)
        input_grad(0, 0)
        send_rim()
        arrive_y(0, 1, 1)
        arrive_raw(2, 0)
        first_half(1)
        arrive_x(1, 1)
        arrive_y(1, 1, 0)
        arrive_y(1, 0, 1)
        arrive_raw(2, 1)
        second_half(1)
        cross_hidden(0)
        arrive_x(2, 0)
        arrive_y(2, 0, 0)
        input_grad(1, 0)
        arrive_hidden(0)
        arrive_y(1, 1, 1)
        arrive_x(2, 1)
        first_half(2)
        arrive_y(2, 0, 1)
        arrive_y(2, 1, 0)
        reduce_core(1)
        second_half(2)
        input_grad(2, 0)
        input_grad(1, 1)
        reduce_core(2)
        arrive_y(2, 1, 1)
        first_half(3)
        second_half(3)
        input_grad(3, 0)
        reduce_y(1)
        arrive_hidden(1)
        input_grad(2, 1)
        reduce_core(3)
        reduce_core(0)
        reduce_y(2)
        input_grad(3, 1)
        grad_of("down", 0)
        input_grad(0, 1)
        reduce_y(3)
        grad_of("down", 1)
        reduce_y(0)
        arrive_hidden(2)

    def mid_sequence():
        pick_for(0)
        pick_for(1)
        relay_raw(0, 0)
        relay_raw(1, 0)
        take_raw(0, 0)
        take_raw(1, 0)
        pick_for(2)
        relay_raw(0, 1)
        relay_raw(1, 1)
        take_raw(0, 1)
        take_raw(1, 1)
        send_own(1)
        arrive_own(0)
        arrive_x(0, 0)
        arrive_x(1, 0)
        arrive_y(0, 0, 0)
        relay_raw(2, 0)
        take_raw(2, 0)
        arrive_y(1, 0, 0)
        arrive_x(0, 1)
        arrive_x(1, 1)
        arrive_y(0, 1, 0)
        relay_raw(2, 1)
        take_raw(2, 1)
        send_rim()
        arrive_y(1, 1, 0)
        arrive_y(0, 0, 1)
        relay_hidden(0)
        relay_hidden(1)
        arrive_x(2, 0)
        arrive_y(1, 0, 1)
        arrive_own(1)
        arrive_y(2, 0, 0)
        arrive_x(2, 1)
        first_half(0)
        first_half(1)
        arrive_y(0, 1, 1)
        cross_hidden(0)
        cross_hidden(1)
        cross_hidden(2)
        first_half(3)
        arrive_y(1, 1, 1)
        second_half(0)
        input_grad(0, 0)
        arrive_y(2, 1, 0)
        relay_hidden(2)
        cross_hidden(3)
        second_half(1)
        input_grad(1, 0)
        reduce_core(0)
        input_grad(0, 1)
        arrive_y(2, 0, 1)
        reduce_core(1)
        first_half(2)
        arrive_y(2, 1, 1)
        input_grad(1, 1)
        second_half(2)
        input_grad(2, 0)
        reduce_y(0)
        second_half(3)
        reduce_core(2)
        input_grad(2, 1)
        reduce_y(1)
        input_grad(3, 0)
        input_grad(3, 1)
        reduce_core(3)
        reduce_y(2)
        grad_of("down", 0)
        grad_of("down", 1)
        reduce_y(3)

    chunks = chunks_end
    pl.when(at_end)(end_sequence)
    chunks = chunks_mid
    pl.when(middle)(mid_sequence)
    grad_of("gate", 0)
    grad_of("gate", 1)

    for d in range(1, n):
        e = lax.rem(s + d, n)
        landed(ret.at[block_rows(e)], "r", e)
    gs_ref = r["gs"]
    combined = dot(r["pick"][...], ret[...], 0, 0) + cot[:, quarter].astype(f32)
    gs_ref[:, quarter] = combined.astype(bf16)
    mine_cols = gs_ref.at[:, quarter]
    by_core = start(mine_cols, mine_cols, "g", 0, s, q_core)
    by_y = start(mine_cols, mine_cols, "g", 1, s, q_y)
    col_all = r["col"]
    holder, relay = q == z, q_y == z
    for i in range(2):
        target = 2 * q + i
        start_if(
            target != s, gs_ref.at[:, aligned(target * icols, icols)], col_all.at[hid_rows(s)],
            "k", i, target, q, s,
        )
    blocks = [sx]
    for j in range(nz - 1):
        blocks += [2 * source[j] + x, 2 * source[j] + 1 - x]

    def pass_cols(block, where):
        there = col_all.at[hid_rows(block)]

        @pl.when(holder & where)
        def _():
            landed(there, "k", block)
            start(there, there, "fy", block, s, q_y, keep=False)
            start(there, there, "fc", block, s, q_core, keep=False)

    def relay_cols(block, where):
        there = col_all.at[hid_rows(block)]

        @pl.when(relay & where)
        def _():
            landed(there, "fy", block)
            start(there, there, "fc", block, s, q_core, keep=False)

    loads["proj"].wait()
    proj = r["proj"]

    def partial_of(owner):
        cols = aligned(owner * width, width)
        return dot(gs_ref[:, cols], proj[cols, :])

    grad_of("up", 0)
    grad_of("up", 1)
    for block in blocks[1:5]:
        pass_cols(block, at_end)
    grad_hidden = partial_of(q)
    by_y.wait_recv()
    y_cols = gs_ref.at[:, quarter_y]
    by_far = start(y_cols, y_cols, "g", 2, s, q_core)
    grad_hidden = grad_hidden + partial_of(q_y)
    by_core.wait_recv()
    grad_hidden = grad_hidden + partial_of(q_core)
    pass_cols(blocks[0], holder)
    by_far.wait_recv()
    grad_hidden = grad_hidden + partial_of(q_far)
    norm_grad = grad_hidden * r["slope"][...]
    mean_removed = r["removed"][...]
    inverse_deviation = r["inverse"][:, 0:1]
    norm_grad_ref = r["norm_grad"]
    norm_grad_ref[...] = norm_grad
    start(norm_grad_ref.at[0:rim], r["rim_grad"], "e", 2, behind, q)
    stat_waits = exchange_stats(
        r["stat2"],
        jnp.sum(norm_grad, axis=1, keepdims=True),
        jnp.sum(norm_grad * mean_removed, axis=1, keepdims=True),
        1,
    )
    rim_stat = r["rim_stat"]
    for p, peer in enumerate((q,) + peers):
        start(r["stat2"].at[3], rim_stat.at[q], "t", p, behind, peer, q)
    col_all[hid_rows(s), :] = gs_ref[:, aligned(s * icols, icols)]
    late_first = blocks[3:5] + blocks[1:3] + blocks[5:]
    for block in late_first:
        pass_cols(block, middle)
    for block in blocks[5:]:
        pass_cols(block, at_end)
    for block in blocks[1:5] + blocks[:1] + blocks[5:]:
        relay_cols(block, at_end)
    for block in blocks[:1] + late_first:
        relay_cols(block, middle)
    avg, cross = summed_stats(r["stat2"], stat_waits)
    ext = r["ext"]

    def conv_grad_of(inverse, grad, removed, avg, cross):
        return inverse * (grad - avg / channel_total - removed * (cross / channel_total))

    ext[0:tokens, :] = conv_grad_of(inverse_deviation, norm_grad, mean_removed, avg, cross)
    for i, name in enumerate(("removed", "inverse", "grad")):
        landed(r["rim_" + name], "e", i)
    for owner in range(1 + len(peers)):
        landed(rim_stat.at[owner], "t", owner)
    avg, cross = totals((rim_stat[0] + rim_stat[1]) + (rim_stat[2] + rim_stat[3]))
    edge = conv_grad_of(
        r["rim_inverse"][:, 0:1], r["rim_grad"][...], r["rim_removed"][...], avg[0:rim],
        cross[0:rim],
    )
    ext[tokens : tokens + rim, :] = jnp.where(s == n - 1, 0.0, edge)
    for name in ("taps", "gate", "value"):
        loads[name].wait()

    @pl.when(jnp.logical_not(holder | relay))
    def _():
        for block in blocks:
            landed(col_all.at[hid_rows(block)], "fc", block)

    for k in range(nz):
        landed(hid_all.at[hid_rows(2 * chunks_end[k] + 1 - x)], "hx", k)
    for copy in copies:
        copy.wait_send()
    piece, half_chunk = full[0].at[0:cap, 0:width], part.at[0:pair, 0:width]
    raw_piece, hid_piece = raw.at[0, 0], hid_all.at[hid_rows(0)]
    for a in range(2):
        for i in range(2):
            sent(piece, "xo", (a, i))
            sent(piece, "xc", (a, i))
        for j in range(nz - 1):
            sent(piece, "x", (a, j))
            for key in ("y", "c", "d"):
                for i in range(2):
                    sent(piece, key, (a, j, i))
    for k in range(nz):
        sent(hid_piece, "hx", k)
        for i in range(2):
            sent(half_chunk, "rc", (k, i))
            sent(piece, "ry", (k, i))
    for d in range(1, n):
        sent(piece, "r", lax.rem(s + d, n))
    for i, name in enumerate(("removed", "inverse")):
        sent(r["rim_" + name], "e", i)

    @pl.when(middle)
    def _():
        for j in range(nz - 1):
            sent(hid_piece, "h", j + 2)
            for a in range(2):
                sent(raw_piece, "z", (a, j + 2))

    for cond, copy in conditional:
        pl.when(cond)(copy.wait_send)
    block_cols = col_all.at[hid_rows(0)]
    for block in blocks:

        @pl.when(holder)
        def _():
            sent(block_cols, "fy", block)

        @pl.when(holder | relay)
        def _():
            sent(block_cols, "fc", block)


input_names = (
    "routes", "weights", "stream", "cot", "conv", "gain", "wg", "wu", "wd", "proj", "value",
    "gate", "taps",
)


def fused(
    routes, weights, stream, cot, wg, wu, wd, proj, value, gate, taps, conv, gain, n, cap, tp_count
):
    tokens, model_width = stream.shape
    hidden_width = wg.shape[1]
    width = model_width // tp_count
    channels = value.shape[0]
    icols = model_width // n
    slots = n * cap
    rim = -(-(taps.shape[0] - 1) // 8) * 8
    nz = n // 2
    V, dma = pltpu.VMEM, pltpu.SemaphoreType.DMA
    given = dict(
        routes=routes, weights=weights, stream=stream, cot=cot, conv=conv, gain=gain, wg=wg, wu=wu,
        wd=wd, proj=proj, value=value, gate=gate, taps=taps,
    )
    outs = dict(
        ggate=((model_width, hidden_width), bf16),
        gup=((model_width, hidden_width), bf16),
        gdown=((hidden_width, model_width), bf16),
        gs=((tokens, model_width), bf16),
        col=((n * tokens, icols), bf16),
        hid=((n * tokens, channels), bf16),
        ext=((tokens + rim, channels), f32),
        taps=(taps.shape, taps.dtype),
        gate=(gate.shape, gate.dtype),
        value=(value.shape, value.dtype),
    )
    scratch = {
        name: V(given[name].shape, given[name].dtype) for name in input_names if name not in outs
    }
    scratch.update(
        meta=V((nz, 8, tokens), f32),
        raw=V((2, nz, tokens, width), bf16),
        ownbuf=V((2, 2 * cap, model_width), bf16),
        pickbuf=V((2, nz - 1, 2 * cap, width), bf16),
        pick=V((slots, tokens), bf16),
        picks=V((nz - 1, 2 * cap, tokens), bf16),
        slot_weights=V((nz - 1, 2 * cap, tokens), f32),
        rows=V((slots, model_width), bf16),
        cots=V((slots, model_width), bf16),
        act=V((slots, hidden_width), bf16),
        dg=V((slots, hidden_width), bf16),
        du=V((slots, hidden_width), bf16),
        part=V((slots, model_width), bf16),
        pre_gate=V((nz, 2 * cap, hidden_width), f32),
        pre_up=V((nz, 2 * cap, hidden_width), f32),
        from_core=V((2, slots, width), bf16),
        to_y=V((slots, width), bf16),
        from_y=V((slots, width), bf16),
        to_xz=V((slots, width), bf16),
        ret=V((slots, width), bf16),
        slope=V((tokens, channels), f32),
        removed=V((tokens, channels), f32),
        inverse=V((tokens, tokens), f32),
        stat=V((4, 8, tokens), f32),
        stat2=V((4, 8, tokens), f32),
        norm_grad=V((tokens, channels), f32),
        rim_removed=V((rim, channels), f32),
        rim_inverse=V((rim, tokens), f32),
        rim_grad=V((rim, channels), f32),
        rim_stat=V((tp_count, 8, tokens), f32),
        load=dma((len(input_names),)),
    )
    sems = dict(
        m=(nz,), z=(2, nz + 1), xo=(2, 2), xc=(2, 2), x=(2, nz - 1), y=(2, nz - 1, 2),
        c=(2, nz - 1, 2), d=(2, nz - 1, 2), s=(2, 3), rc=(nz, 2), ry=(nz, 2), h=(nz + 1,),
        hx=(nz,), g=(3,), k=(n,), fy=(n,), fc=(n,), e=(3,), t=(tp_count,), r=(n,),
    )
    for key, shape in sems.items():
        scratch["send_" + key] = dma(shape)
        scratch["recv_" + key] = dma(shape)
    names = [name + "_h" for name in input_names] + list(outs) + list(scratch)
    return pl.pallas_call(
        functools.partial(fused_kernel, n, cap, channels * tp_count, tuple(names)),
        out_shape=tuple(V(*o) for o in outs.values()),
        in_specs=[pl.BlockSpec(memory_space=pltpu.HBM)] * len(input_names),
        out_specs=[pl.BlockSpec(memory_space=V)] * len(outs),
        scratch_shapes=list(scratch.values()),
        compiler_params=pltpu.CompilerParams(
            collective_id=0, has_side_effects=True, vmem_limit_bytes=48 << 20
        ),
        name="fused",
    )(*[pltpu.with_memory_space_constraint(given[name], pltpu.HBM) for name in input_names])


def finish_kernel(count, *refs):
    given, outs, scratch = refs[: count + 6], refs[count + 6 : 2 * count + 9], refs[2 * count + 9 :]
    col_ref, hid_ref, ext_ref, taps_ref, gate_ref, value_ref = given[count:]
    gproj_ref, gvalue_ref, ggin_ref, sem = scratch
    copies = []

    def put(src, i):
        copies.append(pltpu.make_async_copy(src, outs[i], sem.at[i]))
        copies[-1].start()

    for i in range(count):
        put(given[i], i)
    gproj_ref[...] = dot(col_ref[...], hid_ref[...], 0, 0)
    put(gproj_ref, count)
    tokens = gate_ref.shape[1]
    acc = jnp.zeros((tokens, ext_ref.shape[1]), f32)
    for tap in range(taps_ref.shape[0]):
        acc = acc + taps_ref[tap : tap + 1, :] * ext_ref[tap : tap + tokens, :]
    gated = acc.T
    gate_sig = jax.nn.sigmoid(gate_ref[...].astype(f32))
    gvalue_ref[...] = (gated * gate_sig).astype(bf16)
    put(gvalue_ref, count + 1)
    ggin_ref[...] = (
        gated * value_ref[...].astype(f32) * gate_sig * (1.0 - gate_sig)
    ).astype(bf16)
    put(ggin_ref, count + 2)
    for copy in copies:
        copy.wait()


def finish(*arrays):
    count = len(arrays) - 6
    col, hid, value = arrays[count], arrays[count + 1], arrays[-1]
    made = [((col.shape[1], hid.shape[1]), f32), (value.shape, bf16), (value.shape, bf16)]
    return pl.pallas_call(
        functools.partial(finish_kernel, count),
        out_shape=tuple(jax.ShapeDtypeStruct(a.shape, a.dtype) for a in arrays[:count])
        + tuple(jax.ShapeDtypeStruct(*m) for m in made),
        in_specs=[pl.BlockSpec(memory_space=pltpu.VMEM)] * len(arrays),
        out_specs=[pl.BlockSpec(memory_space=pltpu.HBM)] * (count + 3),
        scratch_shapes=[pltpu.VMEM(*m) for m in made]
        + [pltpu.SemaphoreType.DMA((count + 3,))],
        compiler_params=pltpu.CompilerParams(vmem_limit_bytes=6 << 20),
        name="finish",
    )(*arrays)


def body(
    stream_in, out_cot, route_experts, route_weights, w_gate, w_up, w_down, w_proj,
    conv_value, conv_gate, conv_taps, conv_result, channel_norm_gain,
):
    n = lax.axis_size("sp")
    tp_count = lax.axis_size("tp")
    experts = w_gate.shape[0] * n
    tokens, model_width = stream_in.shape
    cap = 2 * route_experts.shape[1] * tokens // experts
    outs = finish(
        *fused(
            route_experts.T, route_weights.T, stream_in, out_cot, w_gate[0], w_up[0], w_down[0],
            w_proj, conv_value, conv_gate, conv_taps, conv_result, channel_norm_gain[None, :],
            n, cap, tp_count,
        )
    )
    return (outs[0][None], outs[1][None], outs[2][None]) + tuple(outs[3:])


def from_behind(value, axis, steps):
    count = lax.axis_size(axis)
    leading, last = (max(0, -steps), min(count, count - steps))
    return lax.ppermute(value, axis, [(source, source + steps) for source in range(leading, last)])


def slot_tables(block_routes, experts_all, capacity):
    flat_routes = block_routes.reshape(-1)
    assigns = flat_routes.shape[0]
    onehot = (flat_routes[:, None] == jnp.arange(experts_all, dtype=jnp.int32)[None, :]).astype(
        jnp.int32
    )
    before = jnp.cumsum(onehot, axis=0) - onehot
    rank_in = jnp.sum(before * onehot, axis=1)
    slot_of = flat_routes * capacity + rank_in
    source_of = (
        jnp.full((experts_all * capacity,), -1, jnp.int32)
        .at[slot_of]
        .set(jnp.arange(assigns, dtype=jnp.int32))
    )
    return (slot_of, source_of)


def combine_routes(returned, slot_of, cot_cols, token_rows, top_count):
    feature_count = returned.shape[-1]
    flat_back = returned.reshape(-1, feature_count)
    per_route = flat_back[slot_of].astype(jnp.float32).reshape(token_rows, top_count, feature_count)
    return (cot_cols.astype(jnp.float32) + jnp.sum(per_route, axis=1)).astype(jnp.bfloat16)


def expert_terms_plain(rows_in, cot_in, w_gate, w_up, w_down):
    pre_gate = jnp.einsum("secd,edf->secf", rows_in, w_gate, preferred_element_type=jnp.float32)
    pre_up = jnp.einsum("secd,edf->secf", rows_in, w_up, preferred_element_type=jnp.float32)
    glu_part = jnp.minimum(pre_gate, clamp_limit)
    lin_part = jnp.clip(pre_up, -clamp_limit, clamp_limit)
    sig_glu = jax.nn.sigmoid(alpha_gate * glu_part)
    activated = (glu_part * sig_glu * (lin_part + 1.0)).astype(jnp.bfloat16)
    grad_act = jnp.einsum("secd,efd->secf", cot_in, w_down, preferred_element_type=jnp.float32)
    slope = sig_glu + alpha_gate * glu_part * sig_glu * (1.0 - sig_glu)
    grad_pre_gate = jnp.where(
        pre_gate < clamp_limit, grad_act * (lin_part + 1.0) * slope, 0.0
    ).astype(jnp.bfloat16)
    grad_pre_up = jnp.where(
        jnp.abs(pre_up) < clamp_limit, grad_act * glu_part * sig_glu, 0.0
    ).astype(jnp.bfloat16)
    grad_down = jnp.einsum(
        "secf,secd->efd", activated, cot_in, preferred_element_type=jnp.float32
    ).astype(jnp.bfloat16)
    grad_gate = jnp.einsum(
        "secd,secf->edf", rows_in, grad_pre_gate, preferred_element_type=jnp.float32
    ).astype(jnp.bfloat16)
    grad_up = jnp.einsum(
        "secd,secf->edf", rows_in, grad_pre_up, preferred_element_type=jnp.float32
    ).astype(jnp.bfloat16)
    input_part = jnp.einsum(
        "secf,edf->secd", grad_pre_gate, w_gate, preferred_element_type=jnp.float32
    )
    input_part = input_part + jnp.einsum(
        "secf,edf->secd", grad_pre_up, w_up, preferred_element_type=jnp.float32
    )
    return (grad_gate, grad_up, grad_down, input_part)


def body_plain(
    stream_in,
    out_cot,
    route_experts,
    route_weights,
    w_gate,
    w_up,
    w_down,
    w_proj,
    conv_value,
    conv_gate,
    conv_taps,
    conv_result,
    channel_norm_gain,
):
    sp_count = lax.axis_size("sp")
    tp_count = lax.axis_size("tp")
    local_experts = w_gate.shape[0]
    experts_all = local_experts * sp_count
    token_rows, model_width = stream_in.shape
    top_count = route_experts.shape[1]
    capacity = 2 * top_count * token_rows // experts_all
    slot_of, source_of = slot_tables(route_experts, experts_all, capacity)
    occupied = source_of >= 0
    source_safe = jnp.maximum(source_of, 0)
    token_of = source_safe // top_count
    slot_weight = jnp.where(occupied, route_weights.reshape(-1)[source_safe], 0.0)
    row_buffer = jnp.where(occupied[:, None], stream_in[token_of], jnp.zeros((), jnp.bfloat16))
    cot_buffer = (slot_weight[:, None] * out_cot[token_of].astype(jnp.float32)).astype(jnp.bfloat16)
    row_buffer = row_buffer.reshape(experts_all, capacity, model_width)
    cot_buffer = cot_buffer.reshape(experts_all, capacity, model_width)
    slice_width = model_width // tp_count
    slice_start = lax.axis_index("tp") * slice_width
    row_slice = lax.dynamic_slice_in_dim(row_buffer, slice_start, slice_width, 2)
    cot_slice = lax.dynamic_slice_in_dim(cot_buffer, slice_start, slice_width, 2)
    row_slice, cot_slice = (
        lax.all_to_all(row_slice, "sp", split_axis=0, concat_axis=0, tiled=True),
        lax.all_to_all(cot_slice, "sp", split_axis=0, concat_axis=0, tiled=True),
    )
    rows_in, cot_in = (
        lax.all_gather(row_slice, "tp", axis=2, tiled=True),
        lax.all_gather(cot_slice, "tp", axis=2, tiled=True),
    )
    rows_in = rows_in.reshape(sp_count, local_experts, capacity, model_width)
    cot_in = cot_in.reshape(sp_count, local_experts, capacity, model_width)
    grad_gate, grad_up, grad_down, input_part = expert_terms_plain(rows_in, cot_in, w_gate, w_up, w_down)
    shared = lax.psum_scatter(
        input_part.astype(jnp.bfloat16), "tp", scatter_dimension=3, tiled=True
    )
    returned = shared.reshape(experts_all, capacity, slice_width)
    returned = lax.all_to_all(returned, "sp", split_axis=0, concat_axis=0, tiled=True)
    cot_cols = lax.dynamic_slice_in_dim(out_cot, slice_start, slice_width, 1)
    stream_part = combine_routes(returned, slot_of, cot_cols, token_rows, top_count)
    grad_stream = lax.all_gather(stream_part, "tp", axis=1, tiled=True)
    channel_total = conv_result.shape[0] * tp_count
    positions = conv_result.shape[1]
    conv_float = conv_result.astype(jnp.float32)
    chan_sum, chan_sq = lax.psum(
        (jnp.sum(conv_float, axis=0), jnp.sum(conv_float * conv_float, axis=0)), "tp"
    )
    chan_mean = chan_sum / channel_total
    chan_var = chan_sq / channel_total - chan_mean * chan_mean
    inverse_deviation = lax.rsqrt(chan_var + norm_eps)
    mean_removed = (conv_float - chan_mean) * inverse_deviation
    normalized_rows = mean_removed * channel_norm_gain[:, None]
    sigmoid_of_norm = jax.nn.sigmoid(normalized_rows)
    hidden = (normalized_rows * sigmoid_of_norm).astype(jnp.bfloat16)
    grad_proj = lax.psum_scatter(
        lax.dot_general(
            grad_stream, hidden, (((0,), (1,)), ((), ())), preferred_element_type=jnp.float32
        ),
        "sp",
        scatter_dimension=0,
        tiled=True,
    )
    hidden_gradient = lax.dot_general(
        w_proj, grad_stream, (((0,), (1,)), ((), ())), preferred_element_type=jnp.float32
    )
    normed_input_gradient = (
        hidden_gradient
        * sigmoid_of_norm
        * (1.0 + normalized_rows * (1.0 - sigmoid_of_norm))
        * channel_norm_gain[:, None]
    )
    average_products, cross_products = lax.psum(
        (
            jnp.sum(normed_input_gradient, axis=0),
            jnp.sum(normed_input_gradient * mean_removed, axis=0),
        ),
        "tp",
    )
    conv_output_gradient = inverse_deviation * (
        normed_input_gradient
        - average_products / channel_total
        - mean_removed * (cross_products / channel_total)
    )
    taps_count = conv_taps.shape[0]
    next_rim = from_behind(conv_output_gradient[:, : taps_count - 1], "sp", -1)
    extended = jnp.concatenate([conv_output_gradient, next_rim], axis=1)
    grad_gated = jnp.zeros_like(conv_output_gradient)
    for tap_index in range(taps_count):
        grad_gated = (
            grad_gated
            + conv_taps[tap_index][:, None] * extended[:, tap_index : tap_index + positions]
        )
    gate_sig = jax.nn.sigmoid(conv_gate.astype(jnp.float32))
    grad_value = (grad_gated * gate_sig).astype(jnp.bfloat16)
    grad_gate_in = (
        grad_gated * conv_value.astype(jnp.float32) * gate_sig * (1.0 - gate_sig)
    ).astype(jnp.bfloat16)
    return (grad_gate, grad_up, grad_down, grad_stream, grad_proj, grad_value, grad_gate_in)


def solution(mesh):
    return jax.shard_map(
        body if (mesh.shape["sp"], mesh.shape["tp"]) == (8, 4) else body_plain,
        mesh=mesh,
        in_specs=(
            P("sp", None),
            P("sp", None),
            P("sp", None),
            P("sp", None),
            P("sp", None, "tp"),
            P("sp", None, "tp"),
            P("sp", "tp", None),
            P(None, "tp"),
            P("tp", "sp"),
            P("tp", "sp"),
            P(None, "tp"),
            P("tp", "sp"),
            P("tp"),
        ),
        out_specs=(
            P("sp", None, "tp"),
            P("sp", None, "tp"),
            P("sp", "tp", None),
            P("sp", None),
            P("sp", "tp"),
            P("tp", "sp"),
            P("tp", "sp"),
        ),
        check_vma=False,
    )
```

```python
import functools

import jax
import jax.numpy as jnp
from jax import lax
from jax.experimental import pallas as pl
from jax.experimental.pallas import tpu as pltpu
from jax.sharding import PartitionSpec as P

norm_eps = 1e-05
clamp_limit = 7.0
alpha_gate = 1.702
MESH = pl.DeviceIdType.MESH
f32 = jnp.float32
bf16 = jnp.bfloat16


def dot(a, b, ca=1, cb=0):
    return lax.dot_general(a, b, (((ca,), (cb,)), ((), ())), preferred_element_type=f32)


def aligned(start, size):
    return pl.ds(pl.multiple_of(start, size), size)


def greet(n, s, q, tp_peers, ahead):
    barrier = pltpu.get_barrier_semaphore()
    for d in range(1, n):
        pl.semaphore_signal(
            barrier, inc=1, device_id={"sp": lax.rem(s + d, n), "tp": q}, device_id_type=MESH
        )
    for peer in tp_peers:
        for sp in (s, ahead):
            pl.semaphore_signal(
                barrier, inc=1, device_id={"sp": sp, "tp": peer}, device_id_type=MESH
            )
    pl.semaphore_wait(barrier, n - 1 + 2 * len(tp_peers))


def remote(src, dst, send, recv, sp, tp):
    return pltpu.make_async_remote_copy(
        src_ref=src,
        dst_ref=dst,
        send_sem=send,
        recv_sem=recv,
        device_id={"sp": sp, "tp": tp},
        device_id_type=MESH,
    )


def partners(q):
    core, other = lax.rem(q, 2), q // 2
    return (2 * other + 1 - core, 2 * (1 - other) + core, 2 * (1 - other) + 1 - core)


def slot_pick(routes, weights, first, slots, cap):
    top, tokens = routes.shape
    local = routes - first
    expert_ids = lax.broadcasted_iota(jnp.int32, (8, tokens), 0)
    hits = [expert_ids == local[k : k + 1, :] for k in range(top)]
    count = sum(h.astype(f32) for h in hits)
    earlier = (
        lax.broadcasted_iota(jnp.int32, (tokens, tokens), 0)
        < lax.broadcasted_iota(jnp.int32, (tokens, tokens), 1)
    ).astype(f32)
    before = dot(count.astype(bf16), earlier.astype(bf16))
    slot_ids = lax.broadcasted_iota(jnp.int32, (slots, tokens), 0)
    pick = jnp.zeros((slots, tokens), f32)
    weighted = jnp.zeros((slots, tokens), f32)
    for k in range(top):
        rank = jnp.sum(jnp.where(hits[k], before, 0.0), axis=0, keepdims=True)
        here = slot_ids == local[k : k + 1, :] * cap + rank.astype(jnp.int32)
        pick = jnp.where(here, 1.0, pick)
        weighted = jnp.where(here, weights[k : k + 1, :], weighted)
    return pick.astype(bf16), jnp.sum(weighted, axis=1, keepdims=True)


def fused_kernel(n, cap, channel_total, names, *refs):
    r = dict(zip(names, refs))
    s, q = lax.axis_index("sp"), lax.axis_index("tp")
    q_core, q_y, q_far = partners(q)
    peers = (q_core, q_y, q_far)
    core, y = lax.rem(q, 2), q // 2
    z, x = s // 2, lax.rem(s, 2)
    sx = s + 1 - 2 * x
    nz = n // 2
    stream, cot = r["stream"], r["cot"]
    tokens, model_width = stream.shape
    width = r["ret"].shape[-1]
    top = r["routes"].shape[0]
    icols = r["col"].shape[1]
    pair = 2 * cap
    quarter, quarter_y = aligned(q * width, width), aligned(q_y * width, width)
    wg, wu, wd = r["wg"], r["wu"], r["wd"]
    full = (r["rows"], r["cots"])
    copies = []
    conditional = []

    loads = {}
    for i, name in enumerate(input_names):
        loads[name] = pltpu.make_async_copy(r[name + "_h"], r[name], r["load"].at[i])
        loads[name].start()

    def start(src, dst, key, index, sp, tp, recv=None, keep=True):
        send, arrive = r["send_" + key], r["recv_" + key]
        copy = remote(src, dst, send.at[index], arrive.at[index if recv is None else recv], sp, tp)
        copy.start()
        if keep:
            copies.append(copy)
        return copy

    def sent(like, key, index):
        remote(like, like, r["send_" + key].at[index], r["recv_" + key].at[index], s, q).wait_send()

    def start_if(cond, src, dst, key, index, sp, tp, recv):
        copy = remote(
            src, dst, r["send_" + key].at[index], r["recv_" + key].at[recv], sp, tp
        )
        pl.when(cond)(copy.start)
        conditional.append((cond, copy))

    def landed(dst, key, index):
        remote(dst, dst, r["send_" + key].at[index], r["recv_" + key].at[index], s, q).wait_recv()

    high = z // (nz // 2)
    folded = z + high * (nz - 1 - 2 * z)
    middle, at_end = folded == 1, folded == 0

    def unfold(f):
        return f + high * (nz - 1 - 2 * f)

    source = [
        unfold((1 - folded) * (j + 1) + folded * mid) for j, mid in enumerate((2, 0, 3))
    ]
    chunks_end = [z] + source
    chunks_mid = source + [z]

    def block_rows(block):
        return aligned(block * cap, cap)

    loads["routes"].wait()
    loads["weights"].wait()
    meta = r["meta"]
    routes_own, weights_own = r["routes"][...], r["weights"][...]
    meta[z] = jnp.concatenate(
        [routes_own.astype(f32), weights_own, jnp.zeros((8 - 2 * top, tokens), f32)], axis=0
    )
    behind, ahead = lax.rem(s + n - 1, n), lax.rem(s + 1, n)
    greet(n, s, q, peers, ahead)
    for d in range(1, nz):
        start(meta.at[z], meta.at[z], "m", d - 1, 2 * lax.rem(z + d, nz) + x, q, z)
    raw = r["raw"]
    values = (stream, cot)
    for a, name in enumerate(("stream", "cot")):
        loads[name].wait()
        src = values[a].at[:, quarter]
        start_if(z < nz - 1, src, raw.at[a, z], "z", (a, 0), s + 2, q, (a, z))
        start_if(z > 0, src, raw.at[a, z], "z", (a, 1), s - 2, q, (a, z))

    middle = (z > 0) & (z < nz - 1)

    def onward(j):
        return 2 * z - source[1] if j == 1 else source[1]

    def relay_raw(j, a):
        dst = raw.at[a, source[j]]
        landed(dst, "z", (a, source[j]))
        start(dst, dst, "z", (a, j + 2), 2 * onward(j) + x, q, (a, source[j]), keep=False)

    pick, slot_weight = slot_pick(routes_own, weights_own, 2 * z, pair, cap)
    ownbuf = r["ownbuf"]
    own_half, other_half = aligned(x * cap, cap), aligned((1 - x) * cap, cap)

    def send_own(a):
        got = dot(pick, values[a][...])
        ownbuf[a] = (got * slot_weight if a else got).astype(bf16)
        for i, cols in enumerate((quarter, quarter_y)):
            start(
                ownbuf.at[a, other_half, cols], full[a].at[block_rows(s), cols],
                "xo", (a, i), sx, q, keep=False,
            )
        full[a][block_rows(s), :] = ownbuf[a, own_half, :]

    send_own(0)
    r["pick"][...] = slot_pick(routes_own, weights_own, 0, n * cap, cap)[0]

    def exchange_stats(buffer, first, second, which):
        lanes = lax.broadcasted_iota(jnp.int32, (tokens, tokens), 1)
        packed = jnp.where(lanes == 0, first, jnp.where(lanes == 1, second, 0.0))
        buffer[3] = packed.T[0:8, :]
        return [
            start(buffer.at[3], buffer.at[p], "s", (which, p), s, peer)
            for p, peer in enumerate(peers)
        ]

    def totals(total):
        wide = jnp.concatenate([total, jnp.zeros((tokens - 8, tokens), f32)], axis=0).T
        return wide[:, 0:1], wide[:, 1:2]

    def summed_stats(buffer, waits):
        for w in waits:
            w.wait_recv()
        return totals((buffer[3] + buffer[0]) + (buffer[1] + buffer[2]))

    loads["conv"].wait()
    loads["gain"].wait()
    conv = r["conv"][...].astype(f32).T
    stat_waits = exchange_stats(
        r["stat"],
        jnp.sum(conv, axis=1, keepdims=True),
        jnp.sum(conv * conv, axis=1, keepdims=True),
        0,
    )
    pick_all, weight_all = r["picks"], r["slot_weights"]

    def pick_for(j):
        landed(meta.at[source[j]], "m", source[j])
        there = meta[source[j]]
        pick_j, weight_j = slot_pick(
            there[0:top].astype(jnp.int32), there[top : 2 * top], 2 * z, pair, cap
        )
        pick_all[j] = pick_j
        weight_all[j] = jnp.broadcast_to(weight_j, weight_all.shape[1:])

    pickbuf = r["pickbuf"]

    def take_raw(j, a):
        got = dot(pick_all[j], raw[a, source[j]])
        pickbuf[a, j] = (got * weight_all[j][:, 0:1] if a else got).astype(bf16)
        rows = block_rows(2 * source[j] + x)
        mine, other = pickbuf.at[a, j, own_half], pickbuf.at[a, j, other_half]
        here = full[a].at[rows, quarter]
        start(other, here, "x", (a, j), sx, q, keep=False)
        start(mine, here, "y", (a, j, 0), s, q_y, keep=False)
        start(mine, here, "c", (a, j, 0), s, q_core, keep=False)
        full[a][rows, quarter] = pickbuf[a, j, own_half]

    def arrive_raw(j, a):
        landed(raw.at[a, source[j]], "z", (a, source[j]))
        take_raw(j, a)

    def arrive_x(j, a):
        here = full[a].at[block_rows(2 * source[j] + 1 - x), quarter]
        landed(here, "x", (a, j))
        start(here, here, "y", (a, j, 1), s, q_y, keep=False)
        start(here, here, "c", (a, j, 1), s, q_core, keep=False)

    def arrive_y(j, a, i):
        here = full[a].at[block_rows(2 * source[j] + (x if i == 0 else 1 - x)), quarter_y]
        landed(here, "y", (a, j, i))
        start(here, here, "d", (a, j, i), s, q_core, keep=False)

    def complete(j, a):
        for i in range(2):
            rows = block_rows(2 * source[j] + (x if i == 0 else 1 - x))
            for key, owner in (("c", q_core), ("d", q_far)):
                landed(full[a].at[rows, aligned(owner * width, width)], key, (a, j, i))

    def arrive_own(a):
        for i, cols in enumerate((quarter, quarter_y)):
            here = full[a].at[block_rows(sx), cols]
            landed(here, "xo", (a, i))
            start(here, here, "xc", (a, i), s, q_core, keep=False)

    def complete_own(a):
        for i, owner in enumerate((q_core, q_far)):
            landed(full[a].at[block_rows(sx), aligned(owner * width, width)], "xc", (a, i))

    act_all, dg_all, du_all, part = r["act"], r["dg"], r["du"], r["part"]
    pre_gate_ref, pre_up_ref = r["pre_gate"], r["pre_up"]

    chunks = chunks_end

    def block_of(k, i):
        if chunks[k] is z:
            return s if i else sx
        return 2 * chunks[k] + i

    def chunk_of(k):
        return aligned(chunks[k] * pair, pair)

    def ready(k, a):
        if chunks[k] is z:
            complete_own(a)
        else:
            complete(k - 1 if chunks is chunks_end else k, a)

    def first_half(k):
        ready(k, 0)
        rows_in = full[0][chunk_of(k), :]
        pre_gate_ref[k] = dot(rows_in, wg[...])
        pre_up_ref[k] = dot(rows_in, wu[...])

    def second_half(k):
        ready(k, 1)
        rows = chunk_of(k)
        grad_act = dot(full[1][rows, :], wd[...], 1, 1)
        pre_gate, pre_up = pre_gate_ref[k], pre_up_ref[k]
        glu_part = jnp.minimum(pre_gate, clamp_limit)
        lin_part = jnp.clip(pre_up, -clamp_limit, clamp_limit)
        sig_glu = jax.nn.sigmoid(alpha_gate * glu_part)
        act_all[rows, :] = (glu_part * sig_glu * (lin_part + 1.0)).astype(bf16)
        slope = sig_glu + alpha_gate * glu_part * sig_glu * (1.0 - sig_glu)
        dg = jnp.where(
            pre_gate < clamp_limit, grad_act * (lin_part + 1.0) * slope, 0.0
        ).astype(bf16)
        du = jnp.where(
            jnp.abs(pre_up) < clamp_limit, grad_act * glu_part * sig_glu, 0.0
        ).astype(bf16)
        dg_all[rows, :] = dg
        du_all[rows, :] = du

    def input_grad(k, h):
        rows = chunk_of(k)
        half = y if h else 1 - y
        there = aligned(half * 2 * width, 2 * width)
        part[rows, there] = (
            dot(dg_all[rows, :], wg[there, :], 1, 1) + dot(du_all[rows, :], wu[there, :], 1, 1)
        ).astype(bf16)
        start(
            part.at[rows, aligned((2 * half + 1 - core) * width, width)],
            r["from_core"].at[h, rows], "rc", (k, h), s, q_core, keep=False,
        )

    def reduce_core(k, *parts):
        if 1 not in parts:
            landed(r["from_core"].at[0, chunk_of(k)], "rc", (k, 0))
        for i in parts or (0, 1):
            some = block_rows(block_of(k, i))
            r["to_y"][some, :] = (
                part[some, quarter_y].astype(f32) + r["from_core"][0, some, :].astype(f32)
            ).astype(bf16)
            start(
                r["to_y"].at[some], r["from_y"].at[some], "ry", (k, i), s, q_y, keep=False
            )

    ret = r["ret"]
    mine_slots = block_rows(s)

    def reduce_y(k):
        landed(r["from_core"].at[1, chunk_of(k)], "rc", (k, 1))
        for i in range(2):
            home = block_of(k, i)
            some = block_rows(home)
            landed(r["from_y"].at[some], "ry", (k, i))
            r["to_xz"][some, :] = (
                part[some, quarter].astype(f32)
                + r["from_core"][1, some, :].astype(f32)
                + r["from_y"][some, :].astype(f32)
            ).astype(bf16)
            if chunks[k] is z and i:
                ret[mine_slots, :] = r["to_xz"][mine_slots, :]
            else:
                send_home(home)

    def send_home(home):
        start(
            r["to_xz"].at[block_rows(home)], ret.at[mine_slots], "r", home, home, q, s, keep=False
        )

    hid_all = r["hid"]

    def hid_rows(block):
        return aligned(block * tokens, tokens)

    def send_hidden():
        here = hid_all.at[hid_rows(s)]
        start_if(z < nz - 1, here, here, "h", 0, s + 2, q, z)
        start_if(z > 0, here, here, "h", 1, s - 2, q, z)

    rim = r["rim_grad"].shape[0]

    def send_rim():
        for i, name in enumerate(("removed", "inverse")):
            start(r[name].at[0:rim], r["rim_" + name], "e", i, behind, q, keep=False)

    def relay_hidden(j):
        here = hid_all.at[hid_rows(2 * source[j] + x)]
        landed(here, "h", source[j])
        start(here, here, "h", j + 2, 2 * onward(j) + x, q, source[j], keep=False)

    def cross_hidden(k):
        here = hid_all.at[hid_rows(2 * chunks_end[k] + x)]
        start(here, here, "hx", k, sx, q, keep=False)

    def arrive_hidden(j):
        landed(hid_all.at[hid_rows(2 * source[j] + x)], "h", source[j])
        cross_hidden(j + 1)

    def weight_grad(left, right, out, by_left, part_of):
        tile = right.shape[1] if by_left else left.shape[1]
        steps = model_width // tile // 2

        def step(i, carry):
            there = aligned((part_of * steps + i) * tile, tile)
            if by_left:
                out[there, :] = dot(left[:, there], right[...], 0, 0).astype(bf16)
            else:
                out[:, there] = dot(left[...], right[:, there], 0, 0).astype(bf16)
            return carry

        lax.fori_loop(0, steps, step, 0)

    def grad_of(which, part_of):
        if which == "down":
            weight_grad(r["act"], r["cots"], r["gdown"], False, part_of)
        else:
            weight_grad(r["rows"], r["dg" if which == "gate" else "du"], r["g" + which], True, part_of)

    chan_sum, chan_sq = summed_stats(r["stat"], stat_waits)
    chan_mean = chan_sum / channel_total
    chan_var = chan_sq / channel_total - chan_mean * chan_mean
    inverse_deviation = lax.rsqrt(chan_var + norm_eps)
    mean_removed = (conv - chan_mean) * inverse_deviation
    gain = r["gain"][...]
    normed = mean_removed * gain
    sig = jax.nn.sigmoid(normed)
    hid_all[hid_rows(s), :] = (normed * sig).astype(bf16)
    r["slope"][...] = sig * (1.0 + normed * (1.0 - sig)) * gain
    r["removed"][...] = mean_removed
    r["inverse"][...] = jnp.broadcast_to(inverse_deviation, r["inverse"].shape)
    send_hidden()
    for name in ("wg", "wu", "wd"):
        loads[name].wait()

    def end_sequence():
        pick_for(0)
        arrive_raw(0, 0)
        send_own(1)
        arrive_own(0)
        pick_for(1)
        pick_for(2)
        arrive_raw(0, 1)
        arrive_x(0, 0)
        arrive_y(0, 0, 0)
        first_half(0)
        arrive_raw(1, 0)
        arrive_own(1)
        arrive_y(0, 1, 0)
        arrive_x(0, 1)
        arrive_y(0, 0, 1)
        arrive_raw(1, 1)
        second_half(0)
        arrive_x(1, 0)
        arrive_y(1, 0, 0)
        input_grad(0, 0)
        send_rim()
        arrive_y(0, 1, 1)
        arrive_raw(2, 0)
        first_half(1)
        arrive_x(1, 1)
        arrive_y(1, 1, 0)
        arrive_y(1, 0, 1)
        arrive_raw(2, 1)
        second_half(1)
        cross_hidden(0)
        arrive_x(2, 0)
        arrive_y(2, 0, 0)
        input_grad(1, 0)
        arrive_hidden(0)
        arrive_y(1, 1, 1)
        arrive_x(2, 1)
        first_half(2)
        arrive_y(2, 0, 1)
        arrive_y(2, 1, 0)
        reduce_core(1)
        second_half(2)
        input_grad(2, 0)
        input_grad(1, 1)
        reduce_core(2)
        arrive_y(2, 1, 1)
        first_half(3)
        second_half(3)
        input_grad(3, 0)
        reduce_y(1)
        arrive_hidden(1)
        input_grad(2, 1)
        reduce_core(3)
        reduce_core(0)
        reduce_y(2)
        input_grad(3, 1)
        grad_of("down", 0)
        input_grad(0, 1)
        reduce_y(3)
        grad_of("down", 1)
        reduce_y(0)
        arrive_hidden(2)

    def mid_sequence():
        pick_for(0)
        pick_for(1)
        relay_raw(0, 0)
        relay_raw(1, 0)
        take_raw(0, 0)
        take_raw(1, 0)
        pick_for(2)
        relay_raw(0, 1)
        relay_raw(1, 1)
        take_raw(0, 1)
        take_raw(1, 1)
        send_own(1)
        arrive_own(0)
        arrive_x(0, 0)
        arrive_x(1, 0)
        arrive_y(0, 0, 0)
        relay_raw(2, 0)
        take_raw(2, 0)
        arrive_y(1, 0, 0)
        arrive_x(0, 1)
        arrive_x(1, 1)
        arrive_y(0, 1, 0)
        relay_raw(2, 1)
        take_raw(2, 1)
        send_rim()
        arrive_y(1, 1, 0)
        arrive_y(0, 0, 1)
        relay_hidden(0)
        relay_hidden(1)
        arrive_x(2, 0)
        arrive_y(1, 0, 1)
        arrive_own(1)
        arrive_y(2, 0, 0)
        arrive_x(2, 1)
        first_half(0)
        first_half(1)
        arrive_y(0, 1, 1)
        cross_hidden(0)
        cross_hidden(1)
        cross_hidden(2)
        first_half(3)
        arrive_y(1, 1, 1)
        second_half(0)
        input_grad(0, 0)
        arrive_y(2, 1, 0)
        relay_hidden(2)
        cross_hidden(3)
        second_half(1)
        input_grad(1, 0)
        reduce_core(0)
        input_grad(0, 1)
        arrive_y(2, 0, 1)
        reduce_core(1)
        first_half(2)
        arrive_y(2, 1, 1)
        input_grad(1, 1)
        second_half(2)
        input_grad(2, 0)
        reduce_y(0)
        second_half(3)
        reduce_core(2)
        input_grad(2, 1)
        reduce_y(1)
        input_grad(3, 0)
        input_grad(3, 1)
        reduce_core(3)
        reduce_y(2)
        grad_of("down", 0)
        grad_of("down", 1)
        reduce_y(3)

    chunks = chunks_end
    pl.when(at_end)(end_sequence)
    chunks = chunks_mid
    pl.when(middle)(mid_sequence)
    grad_of("gate", 0)
    grad_of("gate", 1)

    for d in range(1, n):
        e = lax.rem(s + d, n)
        landed(ret.at[block_rows(e)], "r", e)
    gs_ref = r["gs"]
    combined = dot(r["pick"][...], ret[...], 0, 0) + cot[:, quarter].astype(f32)
    gs_ref[:, quarter] = combined.astype(bf16)
    mine_cols = gs_ref.at[:, quarter]
    by_core = start(mine_cols, mine_cols, "g", 0, s, q_core)
    by_y = start(mine_cols, mine_cols, "g", 1, s, q_y)
    col_all = r["col"]
    holder, relay = q == z, q_y == z
    for i in range(2):
        target = 2 * q + i
        start_if(
            target != s, gs_ref.at[:, aligned(target * icols, icols)], col_all.at[hid_rows(s)],
            "k", i, target, q, s,
        )
    blocks = [sx]
    for j in range(nz - 1):
        blocks += [2 * source[j] + x, 2 * source[j] + 1 - x]

    def crosses(i):
        return at_end if 3 <= i < 5 else i >= 5

    def pass_cols(i, where):
        there = col_all.at[hid_rows(blocks[i])]

        @pl.when(holder & where)
        def _():
            landed(there, "k", blocks[i])
            if crosses(i) is not False:
                copy = remote(
                    there, there, r["send_fy"].at[blocks[i]], r["recv_fy"].at[blocks[i]], s, q_y
                )
                if crosses(i) is True:
                    copy.start()
                else:
                    pl.when(crosses(i))(copy.start)
            start(there, there, "fc", blocks[i], s, q_core, keep=False)

    def relay_cols(block, where):
        there = col_all.at[hid_rows(block)]

        @pl.when(relay & where)
        def _():
            landed(there, "fy", block)
            start(there, there, "fc", block, s, q_core, keep=False)

    loads["proj"].wait()
    proj = r["proj"]

    def partial_of(owner):
        cols = aligned(owner * width, width)
        return dot(gs_ref[:, cols], proj[cols, :])

    grad_of("up", 0)
    grad_of("up", 1)
    for i in range(1, 5):
        pass_cols(i, at_end)
    grad_hidden = partial_of(q)
    by_y.wait_recv()
    near = (z - q_y) * (z - q_y) <= 1
    for i in range(2):
        target = 2 * q_y + i
        copy = remote(
            gs_ref.at[:, aligned(target * icols, icols)], col_all.at[hid_rows(s)],
            r["send_near"].at[i], r["recv_fy"].at[s], target, q,
        )
        go = near & (target != s)
        pl.when(go)(copy.start)
        conditional.append((go, copy))
    y_cols = gs_ref.at[:, quarter_y]
    by_far = start(y_cols, y_cols, "g", 2, s, q_core)
    grad_hidden = grad_hidden + partial_of(q_y)
    by_core.wait_recv()
    grad_hidden = grad_hidden + partial_of(q_core)
    pass_cols(0, holder)
    by_far.wait_recv()
    grad_hidden = grad_hidden + partial_of(q_far)
    norm_grad = grad_hidden * r["slope"][...]
    mean_removed = r["removed"][...]
    inverse_deviation = r["inverse"][:, 0:1]
    norm_grad_ref = r["norm_grad"]
    norm_grad_ref[...] = norm_grad
    start(norm_grad_ref.at[0:rim], r["rim_grad"], "e", 2, behind, q)
    stat_waits = exchange_stats(
        r["stat2"],
        jnp.sum(norm_grad, axis=1, keepdims=True),
        jnp.sum(norm_grad * mean_removed, axis=1, keepdims=True),
        1,
    )
    rim_stat = r["rim_stat"]
    for p, peer in enumerate((q,) + peers):
        start(r["stat2"].at[3], rim_stat.at[q], "t", p, behind, peer, q)
    col_all[hid_rows(s), :] = gs_ref[:, aligned(s * icols, icols)]
    for i in (3, 4, 1, 2, 5, 6):
        pass_cols(i, middle)
    for i in (5, 6):
        pass_cols(i, at_end)
    for i in (3, 4, 5, 6, 0, 1, 2):
        relay_cols(blocks[i], at_end)
    for i in (0, 1, 2, 5, 6, 3, 4):
        relay_cols(blocks[i], middle)
    avg, cross = summed_stats(r["stat2"], stat_waits)
    ext = r["ext"]

    def conv_grad_of(inverse, grad, removed, avg, cross):
        return inverse * (grad - avg / channel_total - removed * (cross / channel_total))

    ext[0:tokens, :] = conv_grad_of(inverse_deviation, norm_grad, mean_removed, avg, cross)
    for i, name in enumerate(("removed", "inverse", "grad")):
        landed(r["rim_" + name], "e", i)
    for owner in range(1 + len(peers)):
        landed(rim_stat.at[owner], "t", owner)
    avg, cross = totals((rim_stat[0] + rim_stat[1]) + (rim_stat[2] + rim_stat[3]))
    edge = conv_grad_of(
        r["rim_inverse"][:, 0:1], r["rim_grad"][...], r["rim_removed"][...], avg[0:rim],
        cross[0:rim],
    )
    ext[tokens : tokens + rim, :] = jnp.where(s == n - 1, 0.0, edge)
    for name in ("taps", "gate", "value"):
        loads[name].wait()

    @pl.when(jnp.logical_not(holder | relay))
    def _():
        for block in blocks:
            landed(col_all.at[hid_rows(block)], "fc", block)

    for k in range(nz):
        landed(hid_all.at[hid_rows(2 * chunks_end[k] + 1 - x)], "hx", k)
    for copy in copies:
        copy.wait_send()
    piece, half_chunk = full[0].at[0:cap, 0:width], part.at[0:pair, 0:width]
    raw_piece, hid_piece = raw.at[0, 0], hid_all.at[hid_rows(0)]
    for a in range(2):
        for i in range(2):
            sent(piece, "xo", (a, i))
            sent(piece, "xc", (a, i))
        for j in range(nz - 1):
            sent(piece, "x", (a, j))
            for key in ("y", "c", "d"):
                for i in range(2):
                    sent(piece, key, (a, j, i))
    for k in range(nz):
        sent(hid_piece, "hx", k)
        for i in range(2):
            sent(half_chunk, "rc", (k, i))
            sent(piece, "ry", (k, i))
    for d in range(1, n):
        sent(piece, "r", lax.rem(s + d, n))
    for i, name in enumerate(("removed", "inverse")):
        sent(r["rim_" + name], "e", i)

    @pl.when(middle)
    def _():
        for j in range(nz - 1):
            sent(hid_piece, "h", j + 2)
            for a in range(2):
                sent(raw_piece, "z", (a, j + 2))

    for cond, copy in conditional:
        pl.when(cond)(copy.wait_send)
    block_cols = col_all.at[hid_rows(0)]
    for i, block in enumerate(blocks):
        if crosses(i) is not False:

            @pl.when(holder & crosses(i))
            def _():
                sent(block_cols, "fy", block)

        @pl.when(holder | relay)
        def _():
            sent(block_cols, "fc", block)


input_names = (
    "routes", "weights", "stream", "cot", "conv", "gain", "wg", "wu", "wd", "proj", "value",
    "gate", "taps",
)


def fused(
    routes, weights, stream, cot, wg, wu, wd, proj, value, gate, taps, conv, gain, n, cap, tp_count
):
    tokens, model_width = stream.shape
    hidden_width = wg.shape[1]
    width = model_width // tp_count
    channels = value.shape[0]
    icols = model_width // n
    slots = n * cap
    rim = -(-(taps.shape[0] - 1) // 8) * 8
    nz = n // 2
    V, dma = pltpu.VMEM, pltpu.SemaphoreType.DMA
    given = dict(
        routes=routes, weights=weights, stream=stream, cot=cot, conv=conv, gain=gain, wg=wg, wu=wu,
        wd=wd, proj=proj, value=value, gate=gate, taps=taps,
    )
    outs = dict(
        ggate=((model_width, hidden_width), bf16),
        gup=((model_width, hidden_width), bf16),
        gdown=((hidden_width, model_width), bf16),
        gs=((tokens, model_width), bf16),
        col=((n * tokens, icols), bf16),
        hid=((n * tokens, channels), bf16),
        ext=((tokens + rim, channels), f32),
        taps=(taps.shape, taps.dtype),
        gate=(gate.shape, gate.dtype),
        value=(value.shape, value.dtype),
    )
    scratch = {
        name: V(given[name].shape, given[name].dtype) for name in input_names if name not in outs
    }
    scratch.update(
        meta=V((nz, 8, tokens), f32),
        raw=V((2, nz, tokens, width), bf16),
        ownbuf=V((2, 2 * cap, model_width), bf16),
        pickbuf=V((2, nz - 1, 2 * cap, width), bf16),
        pick=V((slots, tokens), bf16),
        picks=V((nz - 1, 2 * cap, tokens), bf16),
        slot_weights=V((nz - 1, 2 * cap, tokens), f32),
        rows=V((slots, model_width), bf16),
        cots=V((slots, model_width), bf16),
        act=V((slots, hidden_width), bf16),
        dg=V((slots, hidden_width), bf16),
        du=V((slots, hidden_width), bf16),
        part=V((slots, model_width), bf16),
        pre_gate=V((nz, 2 * cap, hidden_width), f32),
        pre_up=V((nz, 2 * cap, hidden_width), f32),
        from_core=V((2, slots, width), bf16),
        to_y=V((slots, width), bf16),
        from_y=V((slots, width), bf16),
        to_xz=V((slots, width), bf16),
        ret=V((slots, width), bf16),
        slope=V((tokens, channels), f32),
        removed=V((tokens, channels), f32),
        inverse=V((tokens, tokens), f32),
        stat=V((4, 8, tokens), f32),
        stat2=V((4, 8, tokens), f32),
        norm_grad=V((tokens, channels), f32),
        rim_removed=V((rim, channels), f32),
        rim_inverse=V((rim, tokens), f32),
        rim_grad=V((rim, channels), f32),
        rim_stat=V((tp_count, 8, tokens), f32),
        load=dma((len(input_names),)),
        send_near=dma((2,)),
    )
    sems = dict(
        m=(nz,), z=(2, nz + 1), xo=(2, 2), xc=(2, 2), x=(2, nz - 1), y=(2, nz - 1, 2),
        c=(2, nz - 1, 2), d=(2, nz - 1, 2), s=(2, 3), rc=(nz, 2), ry=(nz, 2), h=(nz + 1,),
        hx=(nz,), g=(3,), k=(n,), fy=(n,), fc=(n,), e=(3,), t=(tp_count,), r=(n,),
    )
    for key, shape in sems.items():
        scratch["send_" + key] = dma(shape)
        scratch["recv_" + key] = dma(shape)
    names = [name + "_h" for name in input_names] + list(outs) + list(scratch)
    return pl.pallas_call(
        functools.partial(fused_kernel, n, cap, channels * tp_count, tuple(names)),
        out_shape=tuple(V(*o) for o in outs.values()),
        in_specs=[pl.BlockSpec(memory_space=pltpu.HBM)] * len(input_names),
        out_specs=[pl.BlockSpec(memory_space=V)] * len(outs),
        scratch_shapes=list(scratch.values()),
        compiler_params=pltpu.CompilerParams(
            collective_id=0, has_side_effects=True, vmem_limit_bytes=48 << 20
        ),
        name="fused",
    )(*[pltpu.with_memory_space_constraint(given[name], pltpu.HBM) for name in input_names])


def finish_kernel(count, *refs):
    given, outs, scratch = refs[: count + 6], refs[count + 6 : 2 * count + 9], refs[2 * count + 9 :]
    col_ref, hid_ref, ext_ref, taps_ref, gate_ref, value_ref = given[count:]
    gproj_ref, gvalue_ref, ggin_ref, sem = scratch
    copies = []

    def put(src, i):
        copies.append(pltpu.make_async_copy(src, outs[i], sem.at[i]))
        copies[-1].start()

    for i in range(count):
        put(given[i], i)
    gproj_ref[...] = dot(col_ref[...], hid_ref[...], 0, 0)
    put(gproj_ref, count)
    tokens = gate_ref.shape[1]
    acc = jnp.zeros((tokens, ext_ref.shape[1]), f32)
    for tap in range(taps_ref.shape[0]):
        acc = acc + taps_ref[tap : tap + 1, :] * ext_ref[tap : tap + tokens, :]
    gated = acc.T
    gate_sig = jax.nn.sigmoid(gate_ref[...].astype(f32))
    gvalue_ref[...] = (gated * gate_sig).astype(bf16)
    put(gvalue_ref, count + 1)
    ggin_ref[...] = (
        gated * value_ref[...].astype(f32) * gate_sig * (1.0 - gate_sig)
    ).astype(bf16)
    put(ggin_ref, count + 2)
    for copy in copies:
        copy.wait()


def finish(*arrays):
    count = len(arrays) - 6
    col, hid, value = arrays[count], arrays[count + 1], arrays[-1]
    made = [((col.shape[1], hid.shape[1]), f32), (value.shape, bf16), (value.shape, bf16)]
    return pl.pallas_call(
        functools.partial(finish_kernel, count),
        out_shape=tuple(jax.ShapeDtypeStruct(a.shape, a.dtype) for a in arrays[:count])
        + tuple(jax.ShapeDtypeStruct(*m) for m in made),
        in_specs=[pl.BlockSpec(memory_space=pltpu.VMEM)] * len(arrays),
        out_specs=[pl.BlockSpec(memory_space=pltpu.HBM)] * (count + 3),
        scratch_shapes=[pltpu.VMEM(*m) for m in made]
        + [pltpu.SemaphoreType.DMA((count + 3,))],
        compiler_params=pltpu.CompilerParams(vmem_limit_bytes=6 << 20),
        name="finish",
    )(*arrays)


def body(
    stream_in, out_cot, route_experts, route_weights, w_gate, w_up, w_down, w_proj,
    conv_value, conv_gate, conv_taps, conv_result, channel_norm_gain,
):
    n = lax.axis_size("sp")
    tp_count = lax.axis_size("tp")
    experts = w_gate.shape[0] * n
    tokens, model_width = stream_in.shape
    cap = 2 * route_experts.shape[1] * tokens // experts
    outs = finish(
        *fused(
            route_experts.T, route_weights.T, stream_in, out_cot, w_gate[0], w_up[0], w_down[0],
            w_proj, conv_value, conv_gate, conv_taps, conv_result, channel_norm_gain[None, :],
            n, cap, tp_count,
        )
    )
    return (outs[0][None], outs[1][None], outs[2][None]) + tuple(outs[3:])


def from_behind(value, axis, steps):
    count = lax.axis_size(axis)
    leading, last = (max(0, -steps), min(count, count - steps))
    return lax.ppermute(value, axis, [(source, source + steps) for source in range(leading, last)])


def slot_tables(block_routes, experts_all, capacity):
    flat_routes = block_routes.reshape(-1)
    assigns = flat_routes.shape[0]
    onehot = (flat_routes[:, None] == jnp.arange(experts_all, dtype=jnp.int32)[None, :]).astype(
        jnp.int32
    )
    before = jnp.cumsum(onehot, axis=0) - onehot
    rank_in = jnp.sum(before * onehot, axis=1)
    slot_of = flat_routes * capacity + rank_in
    source_of = (
        jnp.full((experts_all * capacity,), -1, jnp.int32)
        .at[slot_of]
        .set(jnp.arange(assigns, dtype=jnp.int32))
    )
    return (slot_of, source_of)


def combine_routes(returned, slot_of, cot_cols, token_rows, top_count):
    feature_count = returned.shape[-1]
    flat_back = returned.reshape(-1, feature_count)
    per_route = flat_back[slot_of].astype(jnp.float32).reshape(token_rows, top_count, feature_count)
    return (cot_cols.astype(jnp.float32) + jnp.sum(per_route, axis=1)).astype(jnp.bfloat16)


def expert_terms_plain(rows_in, cot_in, w_gate, w_up, w_down):
    pre_gate = jnp.einsum("secd,edf->secf", rows_in, w_gate, preferred_element_type=jnp.float32)
    pre_up = jnp.einsum("secd,edf->secf", rows_in, w_up, preferred_element_type=jnp.float32)
    glu_part = jnp.minimum(pre_gate, clamp_limit)
    lin_part = jnp.clip(pre_up, -clamp_limit, clamp_limit)
    sig_glu = jax.nn.sigmoid(alpha_gate * glu_part)
    activated = (glu_part * sig_glu * (lin_part + 1.0)).astype(jnp.bfloat16)
    grad_act = jnp.einsum("secd,efd->secf", cot_in, w_down, preferred_element_type=jnp.float32)
    slope = sig_glu + alpha_gate * glu_part * sig_glu * (1.0 - sig_glu)
    grad_pre_gate = jnp.where(
        pre_gate < clamp_limit, grad_act * (lin_part + 1.0) * slope, 0.0
    ).astype(jnp.bfloat16)
    grad_pre_up = jnp.where(
        jnp.abs(pre_up) < clamp_limit, grad_act * glu_part * sig_glu, 0.0
    ).astype(jnp.bfloat16)
    grad_down = jnp.einsum(
        "secf,secd->efd", activated, cot_in, preferred_element_type=jnp.float32
    ).astype(jnp.bfloat16)
    grad_gate = jnp.einsum(
        "secd,secf->edf", rows_in, grad_pre_gate, preferred_element_type=jnp.float32
    ).astype(jnp.bfloat16)
    grad_up = jnp.einsum(
        "secd,secf->edf", rows_in, grad_pre_up, preferred_element_type=jnp.float32
    ).astype(jnp.bfloat16)
    input_part = jnp.einsum(
        "secf,edf->secd", grad_pre_gate, w_gate, preferred_element_type=jnp.float32
    )
    input_part = input_part + jnp.einsum(
        "secf,edf->secd", grad_pre_up, w_up, preferred_element_type=jnp.float32
    )
    return (grad_gate, grad_up, grad_down, input_part)


def body_plain(
    stream_in,
    out_cot,
    route_experts,
    route_weights,
    w_gate,
    w_up,
    w_down,
    w_proj,
    conv_value,
    conv_gate,
    conv_taps,
    conv_result,
    channel_norm_gain,
):
    sp_count = lax.axis_size("sp")
    tp_count = lax.axis_size("tp")
    local_experts = w_gate.shape[0]
    experts_all = local_experts * sp_count
    token_rows, model_width = stream_in.shape
    top_count = route_experts.shape[1]
    capacity = 2 * top_count * token_rows // experts_all
    slot_of, source_of = slot_tables(route_experts, experts_all, capacity)
    occupied = source_of >= 0
    source_safe = jnp.maximum(source_of, 0)
    token_of = source_safe // top_count
    slot_weight = jnp.where(occupied, route_weights.reshape(-1)[source_safe], 0.0)
    row_buffer = jnp.where(occupied[:, None], stream_in[token_of], jnp.zeros((), jnp.bfloat16))
    cot_buffer = (slot_weight[:, None] * out_cot[token_of].astype(jnp.float32)).astype(jnp.bfloat16)
    row_buffer = row_buffer.reshape(experts_all, capacity, model_width)
    cot_buffer = cot_buffer.reshape(experts_all, capacity, model_width)
    slice_width = model_width // tp_count
    slice_start = lax.axis_index("tp") * slice_width
    row_slice = lax.dynamic_slice_in_dim(row_buffer, slice_start, slice_width, 2)
    cot_slice = lax.dynamic_slice_in_dim(cot_buffer, slice_start, slice_width, 2)
    row_slice, cot_slice = (
        lax.all_to_all(row_slice, "sp", split_axis=0, concat_axis=0, tiled=True),
        lax.all_to_all(cot_slice, "sp", split_axis=0, concat_axis=0, tiled=True),
    )
    rows_in, cot_in = (
        lax.all_gather(row_slice, "tp", axis=2, tiled=True),
        lax.all_gather(cot_slice, "tp", axis=2, tiled=True),
    )
    rows_in = rows_in.reshape(sp_count, local_experts, capacity, model_width)
    cot_in = cot_in.reshape(sp_count, local_experts, capacity, model_width)
    grad_gate, grad_up, grad_down, input_part = expert_terms_plain(rows_in, cot_in, w_gate, w_up, w_down)
    shared = lax.psum_scatter(
        input_part.astype(jnp.bfloat16), "tp", scatter_dimension=3, tiled=True
    )
    returned = shared.reshape(experts_all, capacity, slice_width)
    returned = lax.all_to_all(returned, "sp", split_axis=0, concat_axis=0, tiled=True)
    cot_cols = lax.dynamic_slice_in_dim(out_cot, slice_start, slice_width, 1)
    stream_part = combine_routes(returned, slot_of, cot_cols, token_rows, top_count)
    grad_stream = lax.all_gather(stream_part, "tp", axis=1, tiled=True)
    channel_total = conv_result.shape[0] * tp_count
    positions = conv_result.shape[1]
    conv_float = conv_result.astype(jnp.float32)
    chan_sum, chan_sq = lax.psum(
        (jnp.sum(conv_float, axis=0), jnp.sum(conv_float * conv_float, axis=0)), "tp"
    )
    chan_mean = chan_sum / channel_total
    chan_var = chan_sq / channel_total - chan_mean * chan_mean
    inverse_deviation = lax.rsqrt(chan_var + norm_eps)
    mean_removed = (conv_float - chan_mean) * inverse_deviation
    normalized_rows = mean_removed * channel_norm_gain[:, None]
    sigmoid_of_norm = jax.nn.sigmoid(normalized_rows)
    hidden = (normalized_rows * sigmoid_of_norm).astype(jnp.bfloat16)
    grad_proj = lax.psum_scatter(
        lax.dot_general(
            grad_stream, hidden, (((0,), (1,)), ((), ())), preferred_element_type=jnp.float32
        ),
        "sp",
        scatter_dimension=0,
        tiled=True,
    )
    hidden_gradient = lax.dot_general(
        w_proj, grad_stream, (((0,), (1,)), ((), ())), preferred_element_type=jnp.float32
    )
    normed_input_gradient = (
        hidden_gradient
        * sigmoid_of_norm
        * (1.0 + normalized_rows * (1.0 - sigmoid_of_norm))
        * channel_norm_gain[:, None]
    )
    average_products, cross_products = lax.psum(
        (
            jnp.sum(normed_input_gradient, axis=0),
            jnp.sum(normed_input_gradient * mean_removed, axis=0),
        ),
        "tp",
    )
    conv_output_gradient = inverse_deviation * (
        normed_input_gradient
        - average_products / channel_total
        - mean_removed * (cross_products / channel_total)
    )
    taps_count = conv_taps.shape[0]
    next_rim = from_behind(conv_output_gradient[:, : taps_count - 1], "sp", -1)
    extended = jnp.concatenate([conv_output_gradient, next_rim], axis=1)
    grad_gated = jnp.zeros_like(conv_output_gradient)
    for tap_index in range(taps_count):
        grad_gated = (
            grad_gated
            + conv_taps[tap_index][:, None] * extended[:, tap_index : tap_index + positions]
        )
    gate_sig = jax.nn.sigmoid(conv_gate.astype(jnp.float32))
    grad_value = (grad_gated * gate_sig).astype(jnp.bfloat16)
    grad_gate_in = (
        grad_gated * conv_value.astype(jnp.float32) * gate_sig * (1.0 - gate_sig)
    ).astype(jnp.bfloat16)
    return (grad_gate, grad_up, grad_down, grad_stream, grad_proj, grad_value, grad_gate_in)


def solution(mesh):
    return jax.shard_map(
        body if (mesh.shape["sp"], mesh.shape["tp"]) == (8, 4) else body_plain,
        mesh=mesh,
        in_specs=(
            P("sp", None),
            P("sp", None),
            P("sp", None),
            P("sp", None),
            P("sp", None, "tp"),
            P("sp", None, "tp"),
            P("sp", "tp", None),
            P(None, "tp"),
            P("tp", "sp"),
            P("tp", "sp"),
            P(None, "tp"),
            P("tp", "sp"),
            P("tp"),
        ),
        out_specs=(
            P("sp", None, "tp"),
            P("sp", None, "tp"),
            P("sp", "tp", None),
            P("sp", None),
            P("sp", "tp"),
            P("tp", "sp"),
            P("tp", "sp"),
        ),
        check_vma=False,
    )
```
